256 devices in a mesh: sp: 32 (over z, x), tp: 8 (over y, core).
Axes of the slice: x: 4, y: 4, z: 8, core: 2. Of those that a mesh axis runs over, the one named last changes fastest.
Arguments:
- resid: bfloat16 [12288, 2048], P(('sp', 'tp')), may hold values from -6 to 6
- queries: bfloat16 [12288, 1024], P('sp', 'tp'), may hold values from -6 to 6
- keys: bfloat16 [12288, 1024], P('sp', 'tp'), may hold values from -6 to 6
- values: bfloat16 [12288, 1024], P('sp', 'tp'), may hold values from -6 to 6
- decay_input_part: bfloat16 [12288, 1024], P('sp', 'tp'), may hold values from -4 to 4
- decay_channel_offset: float32 [1024], P('tp'), may hold values from -16 to -2
- decay_head_extra: float32 [12288, 16], P('sp', 'tp'), may hold values from 0 to 0.7
- correction_rate_input: bfloat16 [12288, 1024], P('sp', 'tp'), may hold values from -6 to 6
- correction_rate_offset: float32 [1024], P('tp'), may hold values from -0.4 to 1
- head_norm_gain: float32 [1024], P('tp'), may hold values from 0.1 to 1.9
- mixer_output_weight: bfloat16 [1024, 2048], replicated, may hold values from -0.1875 to 0.1875
- feedforward_norm_gain: float32 [2048], replicated, may hold values from 0.1 to 1.9
- gate_weight: bfloat16 [2048, 5632], P('sp', 'tp'), may hold values from -0.125 to 0.125
- up_weight: bfloat16 [2048, 5632], P('sp', 'tp'), may hold values from -0.125 to 0.125
- down_weight: bfloat16 [5632, 2048], P('tp', 'sp'), may hold values from -0.078125 to 0.078125
Outputs:
- result: bfloat16 [12288, 2048], P(('sp', 'tp'))
The draws below stay inside these ranges and needn't reach their ends.
All inputs are finite; a program needn't handle non-finite values.
Results may differ from the reference program's by a relative error of at most 0.014.
Values may be sent and summed in bfloat16 or wider, within the bound.
No kernel may reach another device: no remote copies, remote signals or barrier semaphores. Data moves between devices by JAX's collectives and lax.ppermute only.
A program may use at most 64 MiB of HBM per device.

```python
import math
import jax
import jax.numpy as jnp
from jax import lax

D = 2048
HEADS = 16
HEAD = 64
FF = 5632
TOK_DEV = 384
HW = 1024
TOKENS = 12288
N_SP = 32
N_TP = 8


def head_kinds(key, share):
    chosen = jax.random.uniform(jax.random.fold_in(key, 11), (HEADS,))
    return jnp.repeat(chosen < share, HEAD)


def draw_keys(key, part):
    flips = jax.random.bernoulli(jax.random.fold_in(key, 21), 0.5, (HEADS, HEAD))
    sizes = jax.random.uniform(jax.random.fold_in(key, 22), (HEADS, HEAD), jnp.float32, 0.5, 1.5)
    direction = jnp.where(flips, 1.0, -1.0) * sizes
    turns = jax.random.bernoulli(jax.random.fold_in(key, 23), 0.5, (TOKENS, HEADS))
    amounts = jax.random.uniform(jax.random.fold_in(key, 24), (TOKENS, HEADS), jnp.float32, 1.5, 3.0)
    amplitude = jnp.where(turns, 1.0, -1.0) * amounts
    spread = math.sqrt(6.0 * HEAD / TOKENS)
    noise = spread * jax.random.normal(jax.random.fold_in(key, 25), (TOKENS, HEADS, HEAD), jnp.float32)
    rows = amplitude[:, :, None] * direction[None] + noise
    return jnp.clip(rows, -6.0, 6.0).reshape(TOKENS, HEADS * HEAD).astype(jnp.bfloat16)


def draw_decay_channel_offset(key, part):
    share = 0.5
    slow = head_kinds(key, share)
    jitter = jax.random.uniform(jax.random.fold_in(key, 12), (HEADS * HEAD,), jnp.float32, -0.4, 0.4)
    quick = jax.random.uniform(jax.random.fold_in(key, 18), (HEADS * HEAD,), jnp.float32, -5.6, -2.4)
    return jnp.where(slow, math.log(0.3 / TOKENS) + 0.5 + jitter, quick)


def draw_correction_rate_offset(key, part):
    share = 0.5
    slow = head_kinds(key, share)
    jitter = jax.random.uniform(jax.random.fold_in(key, 13), (HEADS * HEAD,), jnp.float32, -0.4, 0.4)
    strong = jax.random.uniform(jax.random.fold_in(key, 19), (HEADS * HEAD,), jnp.float32, 0.2, 1.0)
    return jnp.where(slow, strong, jitter)


def draw_decay_head_extra(key, part):
    places = jax.random.randint(jax.random.fold_in(key, 14), (3, HEADS), 0, TOKENS)
    losses = jax.random.uniform(jax.random.fold_in(key, 15), (3, HEADS), jnp.float32, 0.22, 0.69)
    positions = jnp.arange(TOKENS, dtype=jnp.int32)[:, None, None]
    return jnp.sum(jnp.where(positions == places[None], losses[None], 0.0), axis=1)


def draw_decay_input_part(key, part):
    noise = 0.5 * jax.random.normal(jax.random.fold_in(key, 16), (TOKENS, HEADS * HEAD), jnp.float32)
    offset = jax.random.uniform(jax.random.fold_in(key, 17), (TOKENS // TOK_DEV, HEADS * HEAD), jnp.float32, -0.7, 0.7)
    return jnp.clip(noise + jnp.repeat(offset, TOK_DEV, axis=0), -4.0, 4.0).astype(jnp.bfloat16)


def steps_of(own_key, shape, split, low, top_value):
    factor_of = 1.0
    for dim, parts in split:
        draws = jax.random.uniform(jax.random.fold_in(jax.random.fold_in(own_key, 6), dim), (parts,), jnp.float32, low / len(split), top_value / len(split))
        factor_of = factor_of * jnp.repeat(jnp.exp(draws), shape[dim] // parts).reshape((-1,) + (1,) * (len(shape) - 1 - dim))
    return factor_of


def gaussian(rng, dims, deviation, reach, pieces=(), held_as=jnp.bfloat16):
    factor_of = steps_of(rng, dims, pieces, -0.22, 0.18) if pieces else 1.0
    array = jax.random.normal(rng, dims, jnp.float32) * deviation * factor_of
    return jnp.minimum(jnp.maximum(array, -reach), reach).astype(held_as)


def setup_inputs(seed: int = 0) -> dict:
    key_of = jax.random.split(jax.random.key(seed), 16)
    resid = gaussian(key_of[0], (TOKENS, D), 1.0, 6.0, ((0, 256),))
    queries = gaussian(key_of[1], (TOKENS, HW), 1.0, 6.0, ((0, 32), (1, 8)))
    keys = draw_keys(jax.random.fold_in(key_of[15], 71), 0)
    values = gaussian(key_of[3], (TOKENS, HW), 1.0, 6.0, ((0, 32), (1, 8)))
    decay_input_part = draw_decay_input_part(jax.random.fold_in(key_of[15], 71), 0)
    decay_channel_offset = draw_decay_channel_offset(jax.random.fold_in(key_of[15], 71), 0)
    decay_head_extra = draw_decay_head_extra(jax.random.fold_in(key_of[15], 71), 0)
    correction_rate_input = gaussian(key_of[7], (TOKENS, HW), 1.0, 6.0, ((0, 32), (1, 8)))
    correction_rate_offset = draw_correction_rate_offset(jax.random.fold_in(key_of[15], 71), 0)
    head_norm_gain = jnp.clip(1.0 + 0.18 * jax.random.normal(key_of[9], (HW,), jnp.float32), 0.1, 1.9)
    mixer_output_weight = gaussian(key_of[10], (HW, D), HW ** -0.5, 0.1875)
    feedforward_norm_gain = jnp.clip(1.0 + 0.18 * jax.random.normal(key_of[11], (D,), jnp.float32), 0.1, 1.9)
    gate_weight = gaussian(key_of[12], (D, FF), D ** -0.5, 0.125, ((0, 32), (1, 8)))
    up_weight = gaussian(key_of[13], (D, FF), D ** -0.5, 0.125, ((0, 32), (1, 8)))
    down_weight = gaussian(key_of[14], (FF, D), FF ** -0.5, 0.078125, ((0, 8), (1, 32)))
    return {"resid": resid, "queries": queries, "keys": keys, "values": values, "decay_input_part": decay_input_part, "decay_channel_offset": decay_channel_offset, "decay_head_extra": decay_head_extra, "correction_rate_input": correction_rate_input, "correction_rate_offset": correction_rate_offset, "head_norm_gain": head_norm_gain, "mixer_output_weight": mixer_output_weight, "feedforward_norm_gain": feedforward_norm_gain, "gate_weight": gate_weight, "up_weight": up_weight, "down_weight": down_weight}


def recurrence(carry_state, inputs):
    query_t, decay_t, key_t, value_t, unit_t, lrate_t = inputs
    lifted = jnp.einsum('hvk,hk->hv', carry_state, -unit_t, precision=lax.Precision.HIGHEST)
    carry_state = carry_state * decay_t[:, None, :] + lifted[:, :, None] * (unit_t * lrate_t)[:, None, :] + value_t[:, :, None] * key_t[:, None, :]
    return (carry_state, jnp.einsum('hvk,hk->hv', carry_state, query_t, precision=lax.Precision.HIGHEST))

def reference(resid, queries, keys, values, decay_input_part, decay_channel_offset, decay_head_extra, correction_rate_input, correction_rate_offset, head_norm_gain, mixer_output_weight, feedforward_norm_gain, gate_weight, up_weight, down_weight):

    def head_count(arr):
        return arr.astype(jnp.float32).reshape(TOKENS, HEADS, HEAD)
    correction_rate = jnp.exp(-jax.nn.softplus(-(decay_channel_offset + decay_input_part.astype(jnp.float32))) - 0.5)
    decay_factor = jnp.exp(-head_count(correction_rate) - decay_head_extra[:, :, None])
    key_f = head_count(keys)
    unit_keys = key_f * lax.rsqrt(lax.optimization_barrier(jnp.sum(key_f * key_f, axis=-1, keepdims=True)) + 1e-06)
    lrate = head_count(jax.nn.sigmoid(correction_rate_offset + correction_rate_input.astype(jnp.float32)))
    start = jnp.zeros((HEADS, HEAD, HEAD), jnp.float32)
    _, mixer_out = lax.scan(recurrence, start, (head_count(queries), decay_factor, key_f, head_count(values), unit_keys, lrate))
    center = mixer_out - lax.optimization_barrier(jnp.mean(mixer_out, axis=-1, keepdims=True))
    spread = lax.optimization_barrier(jnp.mean(center * center, axis=-1, keepdims=True))
    mixed = (center * lax.rsqrt(spread + 1e-05) * head_norm_gain.reshape(HEADS, HEAD)).reshape(TOKENS, HW).astype(jnp.bfloat16)

    def layer_block(pair):
        mixed_rows, resid_rows = pair
        proj = jnp.dot(mixed_rows, mixer_output_weight, preferred_element_type=jnp.float32)
        resid_mid = (resid_rows.astype(jnp.float32) + proj).astype(jnp.bfloat16)
        mid_f = resid_mid.astype(jnp.float32)
        normed = (mid_f * lax.rsqrt(lax.optimization_barrier(jnp.mean(mid_f * mid_f, axis=-1, keepdims=True)) + 1e-06) * feedforward_norm_gain).astype(jnp.bfloat16)
        gate = jnp.dot(normed, gate_weight, preferred_element_type=jnp.float32)
        upper = jnp.dot(normed, up_weight, preferred_element_type=jnp.float32)
        hidden = (jax.nn.silu(gate) * upper).astype(jnp.bfloat16)
        hid_parts = hidden.reshape(TOK_DEV, N_TP, FF // N_TP).astype(jnp.float32)
        down_parts = down_weight.reshape(N_TP, FF // N_TP, D).astype(jnp.float32)
        partial_value = jnp.einsum('tnf,nfd->ntd', hid_parts, down_parts).astype(jnp.bfloat16)
        partial_value = lax.optimization_barrier(partial_value).astype(jnp.float32)
        down_sum = lax.optimization_barrier(jnp.sum(partial_value, axis=0))
        return (mid_f + 0.5 * down_sum).astype(jnp.bfloat16)
    result = lax.map(layer_block, (mixed.reshape(N_SP, TOK_DEV, HW), resid.reshape(N_SP, TOK_DEV, D)))
    return result.reshape(TOKENS, D)
```

```python
import jax
import jax.numpy as jnp
from jax import lax
from jax.experimental import pallas as pl
from jax.experimental.pallas import tpu as pltpu
from jax.sharding import Mesh
from jax.sharding import PartitionSpec as P

HEAD = 64
C = 64
SP = ("sp_0", "sp_1")
SP_TP = ("sp_0", "sp_1", "tp")
BF = jnp.bfloat16
F32 = jnp.float32


def split(x):
    hi = x.astype(BF)
    return hi, (x - hi.astype(F32)).astype(BF)


def dot(a, b):
    return lax.dot_general(a, b, (((1,), (0,)), ((), ())), preferred_element_type=F32)


def dot_t(a, b):
    return lax.dot_general(a, b, (((1,), (1,)), ((), ())), preferred_element_type=F32)


def mm(x, y, f=dot):
    return f(x[0], y[0]) + (f(x[0], y[1]) + f(x[1], y[0]))


def iota(shape, dim):
    return lax.broadcasted_iota(jnp.int32, shape, dim)


def head_masks(width=128):
    first = (iota((1, width), 1) & 127) < HEAD
    m0 = jnp.where(first, 1.0, 0.0)
    return m0.astype(BF), (1.0 - m0).astype(BF)


def stacked(y, masks):
    return tuple(jnp.concatenate([p * masks[0], p * masks[1]], axis=0) for p in y)


def local_scan(q, k, v, dx, lx, dco, lro, extra):
    tok = q.shape[0]
    first = iota((1, 128), 1) < HEAD
    masks, masks2 = head_masks(), head_masks(256)
    ext = jnp.where(first, extra[:, 0:1], extra[:, 1:2])
    log_decay = -0.6065306597126334 * (1.0 / (1.0 + jnp.exp(-(dco + dx)))) - ext
    lrate = 1.0 / (1.0 + jnp.exp(-(lro + lx)))
    same = (iota((128, 128), 0) < HEAD) == (iota((128, 128), 1) < HEAD)
    same_f = jnp.where(same, 1.0, 0.0)
    ones = same_f.astype(BF)
    kk = split(k * k)
    unit = k * lax.rsqrt(dot(kk[0], ones) + dot(kk[1], ones) + 1e-06)
    rate = lrate * unit
    row, col = iota((C, 128), 0), iota((C, 128), 1) & (C - 1)
    lower = row > col
    lower_eq = row >= col
    eye_packed = jnp.where(row == col, 1.0, 0.0)
    tri = jnp.where(iota((C, C), 0) >= iota((C, C), 1), 1.0, 0.0).astype(BF)
    eye = jnp.where(iota((128, 128), 0) == iota((128, 128), 1), 1.0, 0.0)
    levels = [
        ((row >> n) == (col >> n) + 1) & (((row >> n) & 1) == 1) for n in range(6)
    ]
    steps = []
    for c in range(tok // C):
        at = slice(c * C, (c + 1) * C)
        lw = log_decay[at]
        w0 = lw.astype(BF)
        w1, w2 = split(lw - w0.astype(F32))
        cum = dot(tri, w0) + (dot(tri, w1) + dot(tri, w2))
        mid, end = cum[C // 2 - 1 : C // 2], cum[C - 1 : C]
        grow = jnp.exp(cum - mid)
        fall = jnp.exp(mid - cum)
        pc = jnp.exp(cum - lw - mid) * unit[at]
        uc = grow * q[at]
        rc = fall * rate[at]
        gc = fall * k[at]
        left = split(jnp.concatenate([pc, uc], axis=0))
        rs, gs = stacked(split(rc), masks), stacked(split(gc), masks)
        right = tuple(jnp.concatenate([a, b], axis=0) for a, b in zip(rs, gs))
        pair = mm(left, right, dot_t)
        arp = jnp.where(lower, pair[:C, :128], 0.0)
        agp = jnp.where(lower, pair[:C, 128:], 0.0)
        bur = jnp.where(lower_eq, pair[C:, :128], 0.0)
        bug = jnp.where(lower_eq, pair[C:, 128:], 0.0)
        vs = stacked((v[at].astype(BF),), masks)[0]
        ab = split(jnp.concatenate([agp, bug], axis=0))
        abv = dot(ab[0], vs) + dot(ab[1], vs)
        inv = eye_packed - jnp.where(levels[0], arp, 0.0)
        for n in range(1, 6):
            s = split(inv)
            t = mm(split(jnp.where(levels[n], arp, 0.0)), stacked(s, masks))
            inv = inv - mm(s, stacked(split(t), masks))
        to_mid = jnp.exp(mid)
        rest = jnp.exp(end - mid)
        pt = jnp.concatenate([pc * to_mid, abv[:C]], axis=1)
        wy = mm(split(inv), stacked(split(pt), masks2))
        wys = split(wy)
        bwy = mm(split(bur), stacked(wys, masks2))
        ueff = uc * to_mid - bwy[:, :128]
        own = abv[C:] - bwy[:, 128:]
        r_end = (rc * rest).T
        g_end = (gc * rest).T
        rs_t = split(r_end)
        rwy = mm(rs_t, wys)
        gs_t = split(g_end)
        vb = v[at].astype(BF)
        gv = dot(gs_t[0], vb) + dot(gs_t[1], vb)
        trans = eye * jnp.exp(end) - same_f * rwy[:, :128]
        state = same_f * (gv - rwy[:, 128:])
        steps.append((ueff, own, trans, state))
    reads, owns = [], []
    both = jnp.concatenate([eye, jnp.zeros((128, 128), F32)], axis=1)
    for ueff, own, trans, state in steps:
        bs = split(both)
        out = mm(split(ueff), bs)
        reads.append(out[:, :128])
        owns.append(own + out[:, 128:])
        both = mm(split(trans), bs)
        both = jnp.concatenate([both[:, :128], both[:, 128:] + state], axis=1)
    total = jnp.concatenate(
        [both[:HEAD, :128] + both[HEAD:, :128], both[:HEAD, 128:] + both[HEAD:, 128:]], axis=0
    )
    return jnp.concatenate(reads, axis=0), jnp.concatenate(owns, axis=0), total


def local_kernel(q, k, v, dx, lx, dco, lro, extra, reads, owns, total):
    f = lambda r: r[...].astype(F32)
    a, b, t = local_scan(f(q), f(k), f(v), f(dx), f(lx), dco[...], lro[...], extra[...])
    reads[...] = a
    owns[...] = b
    total[...] = t.astype(BF)


def finish(reads, owns, state, gain):
    masks = head_masks()
    out = owns + mm(split(reads), stacked(split(state), masks))
    same = (iota((128, 128), 0) < HEAD) == (iota((128, 128), 1) < HEAD)
    mean = jnp.where(same, 1.0 / HEAD, 0.0).astype(BF)
    s = split(out)
    center = out - (dot(s[0], mean) + dot(s[1], mean))
    s = split(center * center)
    spread = dot(s[0], mean) + dot(s[1], mean)
    return (center * lax.rsqrt(spread + 1e-05) * gain).astype(BF)

def fold(level, masks2, exact):
    while len(level) > 1:
        nxt = []
        for i in range(0, len(level) - 1, 2):
            (t1, x1), (t2, x2) = level[i], level[i + 1]
            both = jnp.concatenate([t1, x1], axis=1)
            if exact:
                out = dot(t2.astype(BF), stacked((both.astype(BF),), masks2)[0])
            else:
                out = mm(split(t2), stacked(split(both), masks2))
            nxt.append((out[:, :128], out[:, 128:] + x2))
        if len(level) % 2:
            nxt.append(level[-1])
        level, exact = nxt, False
    return level[0]


def piece(pieces, d):
    p = pieces[d].astype(F32)
    return p[:HEAD], p[HEAD:]


def earlier(pieces, count, index, masks2):
    eye_packed = jnp.where(iota((HEAD, 128), 0) == (iota((HEAD, 128), 1) & (HEAD - 1)), 1.0, 0.0)
    level = []
    for d in range(count - 1):
        used = jnp.where(d < index, 1.0, 0.0)
        trans, state = piece(pieces, d)
        level.append((trans * used + eye_packed * (1.0 - used), state * used))
    return fold(level, masks2, True)


def group_kernel(index, pieces, total, inside):
    masks2 = head_masks(256)
    count = pieces.shape[0]
    t, x = fold([piece(pieces, d) for d in range(count)], masks2, True)
    total[...] = jnp.concatenate([t, x], axis=0).astype(BF)
    t, x = earlier(pieces, count, index[0], masks2)
    inside[...] = jnp.concatenate([t, x], axis=0)


def finish_kernel(index, pieces, inside, reads, owns, gain, mixed):
    _, x = earlier(pieces, pieces.shape[0], index[0], head_masks(256))
    t = inside[...]
    state = mm(split(t[:HEAD]), stacked(split(x), head_masks())) + t[HEAD:]
    mixed[...] = finish(reads[...], owns[...], state, gain[...])


def vmem(n):
    return [pl.BlockSpec(memory_space=pltpu.VMEM)] * n


SMEM = pl.BlockSpec(memory_space=pltpu.SMEM)


def from_everyone(array, axis):
    copies = jnp.broadcast_to(array, (lax.axis_size(axis), *array.shape))
    return lax.all_to_all(copies, axis, split_axis=0, concat_axis=0, tiled=True)


def per_device(
    resid,
    queries,
    keys,
    values,
    decay_input_part,
    decay_channel_offset,
    decay_head_extra,
    correction_rate_input,
    correction_rate_offset,
    head_norm_gain,
    mixer_output_weight,
    feedforward_norm_gain,
    gate_weight,
    up_weight,
    down_weight,
):
    tok = queries.shape[0]
    shape = jax.ShapeDtypeStruct
    cols = gate_weight.shape[1]
    weights = lax.all_gather(
        jnp.concatenate([gate_weight, up_weight, down_weight.T], axis=1), SP, axis=0, tiled=True
    )
    reads, owns, total = pl.pallas_call(
        local_kernel,
        out_shape=(shape((tok, 128), F32), shape((tok, 128), F32), shape((128, 128), BF)),
        in_specs=vmem(8),
        out_specs=tuple(vmem(3)),
        name="local",
    )(
        queries,
        keys,
        values,
        decay_input_part,
        correction_rate_input,
        decay_channel_offset[None],
        correction_rate_offset[None],
        decay_head_extra,
    )
    near = from_everyone(total, "sp_1")
    total, inside = pl.pallas_call(
        group_kernel,
        out_shape=(shape((128, 128), BF), shape((128, 128), F32)),
        in_specs=[SMEM] + vmem(1),
        out_specs=tuple(vmem(2)),
        name="group",
    )(lax.axis_index("sp_1")[None], near)
    far = from_everyone(total, "sp_0")
    mixed = pl.pallas_call(
        finish_kernel,
        out_shape=shape((tok, 128), BF),
        in_specs=[SMEM] + vmem(5),
        out_specs=vmem(1)[0],
        name="finish",
    )(lax.axis_index("sp_0")[None], far, inside, reads, owns, head_norm_gain[None])
    row_mixed = lax.all_to_all(mixed, "tp", split_axis=0, concat_axis=1, tiled=True)
    proj = jnp.dot(row_mixed, mixer_output_weight, preferred_element_type=F32)
    mid_f = (resid.astype(F32) + proj).astype(BF).astype(F32)
    normed = (
        mid_f
        * lax.rsqrt(jnp.mean(mid_f * mid_f, axis=-1, keepdims=True) + 1e-06)
        * feedforward_norm_gain
    ).astype(BF)
    rows = from_everyone(normed, "tp").reshape(tok, -1)
    both = jnp.dot(rows, weights[:, : 2 * cols], preferred_element_type=F32)
    hidden = (jax.nn.silu(both[:, :cols]) * both[:, cols:]).astype(BF)
    partial = lax.dot_general(
        hidden, weights[:, 2 * cols :], (((1,), (1,)), ((), ())), preferred_element_type=F32
    ).astype(BF)
    pieces = lax.all_to_all(
        partial.reshape(8, -1, partial.shape[1]), "tp", 0, 0, tiled=True
    )
    down_sum = jnp.sum(pieces.astype(F32), axis=0)
    return (mid_f + 0.5 * down_sum).astype(BF)


def solution(mesh):
    torus = Mesh(mesh.devices.reshape(8, 4, mesh.shape["tp"]), ("sp_0", "sp_1", "tp"))
    in_specs = (
        P(SP_TP, None),
        P(SP, "tp"),
        P(SP, "tp"),
        P(SP, "tp"),
        P(SP, "tp"),
        P("tp"),
        P(SP, "tp"),
        P(SP, "tp"),
        P("tp"),
        P("tp"),
        P(),
        P(),
        P(SP, "tp"),
        P(SP, "tp"),
        P("tp", SP),
    )
    return jax.shard_map(
        per_device, mesh=torus, in_specs=in_specs, out_specs=P(SP_TP, None), check_vma=False
    )
```

```python
import jax
import jax.numpy as jnp
from jax import lax
from jax.experimental import pallas as pl
from jax.experimental.pallas import tpu as pltpu
from jax.sharding import Mesh
from jax.sharding import PartitionSpec as P

HEAD = 64
C = 64
BF = jnp.bfloat16
F32 = jnp.float32


def split(x):
    hi = x.astype(BF)
    return hi, (x - hi.astype(F32)).astype(BF)


def dot(a, b):
    return lax.dot_general(a, b, (((1,), (0,)), ((), ())), preferred_element_type=F32)


def dot_t(a, b):
    return lax.dot_general(a, b, (((1,), (1,)), ((), ())), preferred_element_type=F32)


def mm(x, y, f=dot):
    return f(x[0], y[0]) + (f(x[0], y[1]) + f(x[1], y[0]))


def iota(shape, dim):
    return lax.broadcasted_iota(jnp.int32, shape, dim)


def head_masks(width=128):
    first = (iota((1, width), 1) & 127) < HEAD
    m0 = jnp.where(first, 1.0, 0.0)
    return m0.astype(BF), (1.0 - m0).astype(BF)


def stacked(y, masks):
    return tuple(jnp.concatenate([p * masks[0], p * masks[1]], axis=0) for p in y)


def local_scan(q, k, v, dx, lx, dco, lro, extra):
    tok = q.shape[0]
    first = iota((1, 128), 1) < HEAD
    masks, masks2 = head_masks(), head_masks(256)
    ext = jnp.where(first, extra[:, 0:1], extra[:, 1:2])
    log_decay = -0.6065306597126334 * (1.0 / (1.0 + jnp.exp(-(dco + dx)))) - ext
    lrate = 1.0 / (1.0 + jnp.exp(-(lro + lx)))
    same = (iota((128, 128), 0) < HEAD) == (iota((128, 128), 1) < HEAD)
    same_f = jnp.where(same, 1.0, 0.0)
    ones = same_f.astype(BF)
    kk = split(k * k)
    unit = k * lax.rsqrt(dot(kk[0], ones) + dot(kk[1], ones) + 1e-06)
    rate = lrate * unit
    row, col = iota((C, 128), 0), iota((C, 128), 1) & (C - 1)
    lower = row > col
    lower_eq = row >= col
    eye_packed = jnp.where(row == col, 1.0, 0.0)
    tri = jnp.where(iota((C, C), 0) >= iota((C, C), 1), 1.0, 0.0).astype(BF)
    eye = jnp.where(iota((128, 128), 0) == iota((128, 128), 1), 1.0, 0.0)
    levels = [
        ((row >> n) == (col >> n) + 1) & (((row >> n) & 1) == 1) for n in range(6)
    ]
    steps = []
    for c in range(tok // C):
        at = slice(c * C, (c + 1) * C)
        lw = log_decay[at]
        w0 = lw.astype(BF)
        w1, w2 = split(lw - w0.astype(F32))
        cum = dot(tri, w0) + (dot(tri, w1) + dot(tri, w2))
        mid, end = cum[C // 2 - 1 : C // 2], cum[C - 1 : C]
        grow = jnp.exp(cum - mid)
        fall = jnp.exp(mid - cum)
        pc = jnp.exp(cum - lw - mid) * unit[at]
        uc = grow * q[at]
        rc = fall * rate[at]
        gc = fall * k[at]
        left = split(jnp.concatenate([pc, uc], axis=0))
        rs, gs = stacked(split(rc), masks), stacked(split(gc), masks)
        right = tuple(jnp.concatenate([a, b], axis=0) for a, b in zip(rs, gs))
        pair = mm(left, right, dot_t)
        arp = jnp.where(lower, pair[:C, :128], 0.0)
        agp = jnp.where(lower, pair[:C, 128:], 0.0)
        bur = jnp.where(lower_eq, pair[C:, :128], 0.0)
        bug = jnp.where(lower_eq, pair[C:, 128:], 0.0)
        vs = stacked((v[at].astype(BF),), masks)[0]
        ab = split(jnp.concatenate([agp, bug], axis=0))
        abv = dot(ab[0], vs) + dot(ab[1], vs)
        inv = eye_packed - jnp.where(levels[0], arp, 0.0)
        for n in range(1, 6):
            s = split(inv)
            t = mm(split(jnp.where(levels[n], arp, 0.0)), stacked(s, masks))
            inv = inv - mm(s, stacked(split(t), masks))
        to_mid = jnp.exp(mid)
        rest = jnp.exp(end - mid)
        pt = jnp.concatenate([pc * to_mid, abv[:C]], axis=1)
        wy = mm(split(inv), stacked(split(pt), masks2))
        wys = split(wy)
        bwy = mm(split(bur), stacked(wys, masks2))
        ueff = uc * to_mid - bwy[:, :128]
        own = abv[C:] - bwy[:, 128:]
        r_end = (rc * rest).T
        g_end = (gc * rest).T
        rs_t = split(r_end)
        rwy = mm(rs_t, wys)
        gs_t = split(g_end)
        vb = v[at].astype(BF)
        gv = dot(gs_t[0], vb) + dot(gs_t[1], vb)
        trans = eye * jnp.exp(end) - same_f * rwy[:, :128]
        state = same_f * (gv - rwy[:, 128:])
        steps.append((ueff, own, trans, state))
    reads, owns = [], []
    both = jnp.concatenate([eye, jnp.zeros((128, 128), F32)], axis=1)
    for ueff, own, trans, state in steps:
        bs = split(both)
        out = mm(split(ueff), bs)
        reads.append(out[:, :128])
        owns.append(own + out[:, 128:])
        both = mm(split(trans), bs)
        both = jnp.concatenate([both[:, :128], both[:, 128:] + state], axis=1)
    total = jnp.concatenate(
        [both[:HEAD, :128] + both[HEAD:, :128], both[:HEAD, 128:] + both[HEAD:, 128:]], axis=0
    )
    return jnp.concatenate(reads, axis=0), jnp.concatenate(owns, axis=0), total


def local_kernel(q, k, v, dx, lx, dco, lro, extra, reads, owns, total):
    f = lambda r: r[...].astype(F32)
    a, b, t = local_scan(f(q), f(k), f(v), f(dx), f(lx), dco[...], lro[...], extra[...].T)
    reads[...] = a
    owns[...] = b
    out = sent(t[:HEAD], t[HEAD:])
    for d in range(total.shape[0]):
        total[d] = out


def finish(reads, owns, state, gain):
    masks = head_masks()
    out = owns + mm(split(reads), stacked(split(state), masks))
    same = (iota((128, 128), 0) < HEAD) == (iota((128, 128), 1) < HEAD)
    mean = jnp.where(same, 1.0 / HEAD, 0.0).astype(BF)
    s = split(out)
    center = out - (dot(s[0], mean) + dot(s[1], mean))
    s = split(center * center)
    spread = dot(s[0], mean) + dot(s[1], mean)
    return (center * lax.rsqrt(spread + 1e-05) * gain).astype(BF)

def fold(level, masks2, exact):
    while len(level) > 1:
        nxt = []
        for i in range(0, len(level) - 1, 2):
            (t1, x1), (t2, x2) = level[i], level[i + 1]
            both = jnp.concatenate([t1, x1], axis=1)
            out = mm(split(t2), stacked(split(both), masks2))
            nxt.append((out[:, :128], out[:, 128:] + x2))
        if len(level) % 2:
            nxt.append(level[-1])
        level = nxt
    return level[0]


def eye_packed():
    return jnp.where(iota((HEAD, 128), 0) == (iota((HEAD, 128), 1) & (HEAD - 1)), 1.0, 0.0)


def piece(pieces, d):
    p = pieces[d].astype(F32)
    return p[:HEAD], p[HEAD:]


def sent(trans, state):
    return jnp.concatenate([trans - eye_packed(), state], axis=0).astype(BF)


def earlier(pieces, count, index, masks2):
    level = []
    for d in range(count - 1):
        used = jnp.where(d < index, 1.0, 0.0)
        trans, state = piece(pieces, d)
        level.append((trans * used + eye_packed(), state * used))
    return fold(level, masks2, True)


def group_kernel(index, pieces, total, inside):
    masks2 = head_masks(256)
    count = pieces.shape[0]
    level = [piece(pieces, d) for d in range(count)]
    t, x = fold([(t + eye_packed(), x) for t, x in level], masks2, True)
    out = sent(t, x)
    for d in range(total.shape[0]):
        total[d] = out
    t, x = earlier(pieces, count, index[0], masks2)
    inside[...] = jnp.concatenate([t, x], axis=0)


def finish_kernel(index, pieces, inside, reads, owns, gain, mixed):
    _, x = earlier(pieces, pieces.shape[0], index[0], head_masks(256))
    t = inside[...]
    state = mm(split(t[:HEAD]), stacked(split(x), head_masks())) + t[HEAD:]
    out = finish(reads[...], owns[...], state, gain[...])
    rows = out.shape[0] // 8
    core = index[1]
    parts = [[out[(2 * y + c) * rows : (2 * y + c + 1) * rows] for y in range(4)] for c in range(2)]
    for d in range(4):
        for y in range(4):
            for c in range(2):
                at = y * rows + (c ^ core) * (4 * rows)
                mixed[d, pl.ds(pl.multiple_of(at, 16), rows)] = parts[c][y]


def proj_kernel(index, own, sib, resid_own, resid_sib, weight, gain, mid, normed):
    core = index[1]
    half = own.shape[1] // 2
    w = jnp.concatenate(
        [
            weight[pl.ds(pl.multiple_of((2 * y + (c ^ core)) * 128, 128), 128)]
            for c in range(2)
            for y in range(4)
        ],
        axis=0,
    )
    for n, resid in enumerate((resid_own, resid_sib)):
        left = jnp.concatenate(
            [own[y, n * half : (n + 1) * half] for y in range(4)]
            + [sib[y, (1 - n) * half : (2 - n) * half] for y in range(4)],
            axis=1,
        )
        rows = resid.shape[1]
        m = jnp.concatenate([resid[y] for y in range(4)], axis=0).astype(F32) + dot(left, w)
        m = m.astype(BF)
        if n == 0:
            for y in range(4):
                mid[y] = m[y * rows : (y + 1) * rows]
        m = m.astype(F32)
        scale = lax.rsqrt(jnp.mean(m * m, axis=-1, keepdims=True) + 1e-06)
        normed[n * half : (n + 1) * half] = (m * scale * gain[...]).astype(BF)


def ffn_kernel(index, normed, *refs):
    a, b, (keep, send, wa, wb, sems) = refs[:8], refs[8:12], refs[12:]
    z, x = index[2], index[3]
    copies_a, copies_b = [], []
    for r in range(8):
        copies_a.append(pltpu.make_async_copy(a[r], wa.at[(z + r) % 8], sems.at[r]))
    for s in range(4):
        for r in range(8):
            copies_b.append(
                pltpu.make_async_copy(
                    b[s].at[r], wb.at[(z + r) % 8, (x + 4 - s) % 4], sems.at[8 + 8 * s + r]
                )
            )
    for copy in copies_a + copies_b:
        copy.start()
    cols = wb.shape[3]
    for copy in copies_a:
        copy.wait()
    both = dot(normed[...], wa[...].reshape(-1, 2 * cols))
    gate = both[:, :cols]
    hidden = (gate * (1.0 / (1.0 + jnp.exp(-gate))) * both[:, cols:]).astype(BF)
    for copy in copies_b:
        copy.wait()
    half, rows = hidden.shape[0] // 2, hidden.shape[0] // 8
    for k in range(8):
        out = dot_t(hidden, wb[k].reshape(-1, cols)).astype(BF)
        for y in range(4):
            keep[y, k] = out[y * rows : (y + 1) * rows]
            send[y, k] = out[half + y * rows : half + (y + 1) * rows]


def final_kernel(index, pieces, mid, result):
    m = mid[index[4]].astype(F32)
    for k in range(8):
        total = pieces[0, k].astype(F32)
        for y in range(1, 4):
            total = total + pieces[y, k].astype(F32)
        at = slice(k * 256, (k + 1) * 256)
        result[:, at] = (m[:, at] + 0.5 * total).astype(BF)


def vmem(n):
    return [pl.BlockSpec(memory_space=pltpu.VMEM)] * n


SMEM = pl.BlockSpec(memory_space=pltpu.SMEM)
ANY = pl.BlockSpec(memory_space=pl.ANY)
shape = jax.ShapeDtypeStruct


def exchanged(array, axis):
    return lax.all_to_all(array, axis, split_axis=0, concat_axis=0, tiled=True)


def copies(array, axis):
    return jnp.broadcast_to(array, (lax.axis_size(axis), *array.shape))


def shifted(array, axis, by):
    n = lax.axis_size(axis)
    return lax.ppermute(array, axis, [(i, (i + by) % n) for i in range(n)])


def ring(array, axis):
    n = lax.axis_size(axis)
    found = {0: array}
    up = down = array
    for s in range(1, n // 2 + 1):
        up = shifted(up, axis, 1)
        found[n - s] = up
        if s < n - s:
            down = shifted(down, axis, -1)
            found[s] = down
    return [found[r] for r in range(n)]


def call(kernel, name, out, in_specs, us, mib=16, scratch=()):
    return pl.pallas_call(
        kernel,
        out_shape=out,
        in_specs=in_specs,
        out_specs=jax.tree.map(lambda _: vmem(1)[0], out),
        scratch_shapes=scratch,
        name=name,
        compiler_params=pltpu.CompilerParams(vmem_limit_bytes=mib << 20),
        cost_estimate=pl.CostEstimate(flops=int(us * FLOPS_US), bytes_accessed=0, transcendentals=0),
    )


FLOPS_US = 1e8


def per_device(
    resid,
    queries,
    keys,
    values,
    decay_input_part,
    decay_channel_offset,
    decay_head_extra,
    correction_rate_input,
    correction_rate_offset,
    head_norm_gain,
    mixer_output_weight,
    feedforward_norm_gain,
    gate_weight,
    up_weight,
    down_weight,
):
    tok = queries.shape[0]
    cols = gate_weight.shape[1]
    z, x, y, c = (lax.axis_index(a).astype(jnp.int32) for a in ("z", "x", "y", "c"))
    down = ring(down_weight.T, "z")
    first = exchanged(copies(jnp.concatenate([gate_weight, up_weight], axis=1), "x"), "x")
    pieces_a = ring(first, "z")
    resid_own = exchanged(copies(resid, "y"), "y")
    resid_sib = shifted(resid_own, "c", 1)
    stack = jnp.stack(down)
    pieces_b = [stack] + [shifted(stack, "x", s) for s in range(1, 4)]

    reads, owns, total = call(
        local_kernel,
        "local",
        (shape((tok, 128), F32), shape((tok, 128), F32), shape((4, 128, 128), BF)),
        vmem(8),
        18,
    )(
        queries,
        keys,
        values,
        decay_input_part,
        correction_rate_input,
        decay_channel_offset[None],
        correction_rate_offset[None],
        decay_head_extra.T,
    )
    near = exchanged(total, "x")
    total, inside = call(
        group_kernel,
        "group",
        (shape((8, 128, 128), BF), shape((128, 128), F32)),
        [SMEM] + vmem(1),
        2,
    )(jnp.stack([x]), near)
    far = exchanged(total, "z")
    index = jnp.stack([z, c, z, x, y])
    mixed = call(finish_kernel, "finish", shape((4, tok, 128), BF), [SMEM] + vmem(5), 3)(
        index, far, inside, reads, owns, head_norm_gain[None]
    )
    mixed_own = exchanged(mixed, "y")
    mixed_sib = shifted(mixed_own, "c", 1)
    mid, normed = call(
        proj_kernel,
        "proj",
        (shape((4, tok // 8, 2048), BF), shape((tok, 2048), BF)),
        [SMEM] + vmem(6),
        4,
        32,
    )(
        index,
        mixed_own,
        mixed_sib,
        resid_own,
        resid_sib,
        mixer_output_weight,
        feedforward_norm_gain[None],
    )
    part = shape((4, 8, tok // 8, 256), BF)
    keep, send = call(
        ffn_kernel,
        "ffn",
        (part, part),
        [SMEM] + vmem(1) + [ANY] * 12,
        8,
        40,
        [
            pltpu.VMEM((8, 4, 64, 2 * cols), BF),
            pltpu.VMEM((8, 4, 64, cols), BF),
            pltpu.SemaphoreType.DMA((40,)),
        ],
    )(index, normed, *pieces_a, *pieces_b)
    pair = (keep.astype(F32) + shifted(send, "c", 1).astype(F32)).astype(BF)
    return call(final_kernel, "final", shape((tok // 8, 2048), BF), [SMEM] + vmem(2), 1)(
        index, exchanged(pair, "y"), mid
    )


def solution(mesh):
    torus = Mesh(mesh.devices.reshape(8, 4, 4, 2), ("z", "x", "y", "c"))
    sp, tp = ("z", "x"), ("y", "c")
    in_specs = (
        P(sp + tp, None),
        P(sp, tp),
        P(sp, tp),
        P(sp, tp),
        P(sp, tp),
        P(tp),
        P(sp, tp),
        P(sp, tp),
        P(tp),
        P(tp),
        P(),
        P(),
        P(sp, tp),
        P(sp, tp),
        P(tp, sp),
    )
    return jax.shard_map(
        per_device, mesh=torus, in_specs=in_specs, out_specs=P(sp + tp, None), check_vma=False
    )
```

```python
import jax
import jax.numpy as jnp
from jax import lax
from jax.experimental import pallas as pl
from jax.experimental.pallas import tpu as pltpu
from jax.sharding import Mesh
from jax.sharding import PartitionSpec as P

HEAD = 64
C = 64
BF = jnp.bfloat16
F32 = jnp.float32


def split(x):
    hi = x.astype(BF)
    return hi, (x - hi.astype(F32)).astype(BF)


def dot(a, b):
    return lax.dot_general(a, b, (((1,), (0,)), ((), ())), preferred_element_type=F32)


def dot_t(a, b):
    return lax.dot_general(a, b, (((1,), (1,)), ((), ())), preferred_element_type=F32)


def mm(x, y, f=dot):
    return f(x[0], y[0]) + (f(x[0], y[1]) + f(x[1], y[0]))


def iota(shape, dim):
    return lax.broadcasted_iota(jnp.int32, shape, dim)


def head_masks(width=128):
    first = (iota((1, width), 1) & 127) < HEAD
    m0 = jnp.where(first, 1.0, 0.0)
    return m0.astype(BF), (1.0 - m0).astype(BF)


def stacked(y, masks):
    return tuple(jnp.concatenate([p * masks[0], p * masks[1]], axis=0) for p in y)


def local_scan(q, k, v, dx, lx, dco, lro, extra):
    chunks = range(q.shape[0] // C)
    first = iota((1, 128), 1) < HEAD
    masks, masks2 = head_masks(), head_masks(256)
    ext = jnp.where(first, extra[:, 0:1], extra[:, 1:2])
    log_decay = -0.6065306597126334 * (1.0 / (1.0 + jnp.exp(-(dco + dx)))) - ext
    lrate = 1.0 / (1.0 + jnp.exp(-(lro + lx)))
    same_f = jnp.where((iota((128, 128), 0) < HEAD) == (iota((128, 128), 1) < HEAD), 1.0, 0.0)
    ones = same_f.astype(BF)
    kk = split(k * k)
    unit = k * lax.rsqrt(dot(kk[0], ones) + dot(kk[1], ones) + 1e-06)
    rate = lrate * unit
    row, col = iota((C, 128), 0), iota((C, 128), 1) & (C - 1)
    lower = row > col
    lower_eq = row >= col
    unit_packed = jnp.where(row == col, 1.0, 0.0)
    tri = jnp.where(iota((C, C), 0) >= iota((C, C), 1), 1.0, 0.0).astype(BF)
    eye = jnp.where(iota((128, 128), 0) == iota((128, 128), 1), 1.0, 0.0)
    levels = [((row >> n) == (col >> n) + 1) & (((row >> n) & 1) == 1) for n in range(6)]
    at = [slice(c * C, (c + 1) * C) for c in chunks]

    def each(f, *lists):
        return [f(*args) for args in zip(*lists)]

    def summed(lw):
        w0 = lw.astype(BF)
        w1, w2 = split(lw - w0.astype(F32))
        return dot(tri, w0) + (dot(tri, w1) + dot(tri, w2))

    lws = [log_decay[a] for a in at]
    cums = each(summed, lws)
    mids = [cum[C // 2 - 1 : C // 2] for cum in cums]
    ends = [cum[C - 1 : C] for cum in cums]
    falls = each(lambda cum, mid: jnp.exp(mid - cum), cums, mids)
    pcs = each(lambda cum, lw, mid, a: jnp.exp(cum - lw - mid) * unit[a], cums, lws, mids, at)
    ucs = each(lambda cum, mid, a: jnp.exp(cum - mid) * q[a], cums, mids, at)
    rcs = each(lambda fall, a: fall * rate[a], falls, at)
    gcs = each(lambda fall, a: fall * k[a], falls, at)

    def pairs(pc, uc, rc, gc):
        left = split(jnp.concatenate([pc, uc], axis=0))
        rs, gs = stacked(split(rc), masks), stacked(split(gc), masks)
        right = tuple(jnp.concatenate([a, b], axis=0) for a, b in zip(rs, gs))
        return mm(left, right, dot_t)

    pair = each(pairs, pcs, ucs, rcs, gcs)
    arps = [jnp.where(lower, p[:C, :128], 0.0) for p in pair]
    burs = [jnp.where(lower_eq, p[C:, :128], 0.0) for p in pair]

    def values_read(p, a):
        ab = split(
            jnp.concatenate(
                [jnp.where(lower, p[:C, 128:], 0.0), jnp.where(lower_eq, p[C:, 128:], 0.0)], axis=0
            )
        )
        vs = stacked((v[a].astype(BF),), masks)[0]
        return dot(ab[0], vs) + dot(ab[1], vs)

    abvs = each(values_read, pair, at)
    invs = [unit_packed - jnp.where(levels[0], arp, 0.0) for arp in arps]
    for n in range(1, 6):
        ss = each(split, invs)
        ts = each(
            lambda arp, s: mm(split(jnp.where(levels[n], arp, 0.0)), stacked(s, masks)), arps, ss
        )
        invs = each(lambda inv, s, t: inv - mm(s, stacked(split(t), masks)), invs, ss, ts)
    to_mids = each(jnp.exp, mids)
    wys = each(
        lambda inv, pc, to_mid, abv: split(
            mm(
                split(inv),
                stacked(split(jnp.concatenate([pc * to_mid, abv[:C]], axis=1)), masks2),
            )
        ),
        invs,
        pcs,
        to_mids,
        abvs,
    )
    bwys = each(lambda bur, wy: mm(split(bur), stacked(wy, masks2)), burs, wys)
    ueffs = each(lambda uc, to_mid, bwy: split(uc * to_mid - bwy[:, :128]), ucs, to_mids, bwys)
    own = each(lambda abv, bwy: abv[C:] - bwy[:, 128:], abvs, bwys)

    def change(rc, gc, mid, end, wy, a):
        rest = jnp.exp(end - mid)
        rwy = mm(split((rc * rest).T), wy)
        gs = split((gc * rest).T)
        vb = v[a].astype(BF)
        gv = dot(gs[0], vb) + dot(gs[1], vb)
        return split(eye * jnp.exp(end) - same_f * rwy[:, :128]), same_f * (gv - rwy[:, 128:])

    changes = each(change, rcs, gcs, mids, ends, wys, at)
    reads, owns = [], []
    both = jnp.concatenate([eye, jnp.zeros((128, 128), F32)], axis=1)
    for c in chunks:
        bs = split(both)
        out = mm(ueffs[c], bs)
        reads.append(out[:, :128])
        owns.append(own[c] + out[:, 128:])
        trans, state = changes[c]
        both = mm(trans, bs)
        both = jnp.concatenate([both[:, :128], both[:, 128:] + state], axis=1)
    total = jnp.concatenate(
        [both[:HEAD, :128] + both[HEAD:, :128], both[:HEAD, 128:] + both[HEAD:, 128:]], axis=0
    )
    return jnp.concatenate(reads, axis=0), jnp.concatenate(owns, axis=0), total


def local_kernel(q, k, v, dx, lx, dco, lro, extra, reads_out, owns_out, total, reads, owns, sems):
    f = lambda r: r[...].astype(F32)
    a, b, t = local_scan(f(q), f(k), f(v), f(dx), f(lx), dco[...], lro[...], extra[...].T)
    reads[...] = a
    owns[...] = b
    stores = [
        pltpu.make_async_copy(reads, reads_out, sems.at[0]),
        pltpu.make_async_copy(owns, owns_out, sems.at[1]),
    ]
    for copy in stores:
        copy.start()
    total[...] = sent(t[:HEAD], t[HEAD:])
    for copy in stores:
        copy.wait()


def finish(reads, owns, state, gain):
    masks = head_masks()
    out = owns + mm(split(reads), stacked(split(state), masks))
    same = (iota((128, 128), 0) < HEAD) == (iota((128, 128), 1) < HEAD)
    mean = jnp.where(same, 1.0 / HEAD, 0.0).astype(BF)
    s = split(out)
    center = out - (dot(s[0], mean) + dot(s[1], mean))
    s = split(center * center)
    spread = dot(s[0], mean) + dot(s[1], mean)
    return (center * lax.rsqrt(spread + 1e-05) * gain).astype(BF)


def fold(level, masks2):
    while len(level) > 1:
        nxt = []
        for i in range(0, len(level) - 1, 2):
            (t1, x1), (t2, x2) = level[i], level[i + 1]
            both = jnp.concatenate([t1, x1], axis=1)
            out = mm(split(t2), stacked(split(both), masks2))
            nxt.append((out[:, :128], out[:, 128:] + x2))
        if len(level) % 2:
            nxt.append(level[-1])
        level = nxt
    return level[0]


def eye_packed():
    return jnp.where(iota((HEAD, 128), 0) == (iota((HEAD, 128), 1) & (HEAD - 1)), 1.0, 0.0)


def piece(pieces, d):
    p = pieces[d].astype(F32)
    return p[:HEAD], p[HEAD:]


def sent(trans, state):
    return jnp.concatenate([trans - eye_packed(), state], axis=0).astype(BF)


def earlier(pieces, count, index, masks2):
    level = []
    for d in range(count - 1):
        used = jnp.where(d < index, 1.0, 0.0)
        trans, state = piece(pieces, d)
        level.append((trans * used + eye_packed(), state * used))
    return fold(level, masks2)


def group_kernel(index, near0, near1, near2, near3, total, inside, pieces):
    masks2 = head_masks(256)
    for s, near in enumerate((near0, near1, near2, near3)):
        pieces[(index[0] + 4 - s) % 4] = near[...]
    level = [piece(pieces, d) for d in range(4)]
    t, x = fold([(t + eye_packed(), x) for t, x in level], masks2)
    out = sent(t, x)
    for d in range(total.shape[0]):
        total[d] = out
    t, x = earlier(pieces, 4, index[0], masks2)
    inside[...] = jnp.concatenate([t, x], axis=0)


def start_and_wait(loads):
    for copy in loads:
        copy.start()
    for copy in loads:
        copy.wait()


def pack_kernel(gate, up, down, a, b):
    cols = gate.shape[1]
    cut = a.shape[1] - cols
    a[:, :cols] = gate[...]
    a[:, cols:] = up[:, :cut]
    b[:, : cols - cut] = up[:, cut:]
    b[:, cols - cut :] = down[...]


def stack_kernel(index, near0, near1, near2, near3, own, sib, out, rows, sems):
    loads = [
        pltpu.make_async_copy(near, out.at[(index[3] + 4 - s) % 4], sems.at[s])
        for s, near in enumerate((near0, near1, near2, near3))
    ]
    loads.append(pltpu.make_async_copy(own, rows.at[0], sems.at[4]))
    loads.append(pltpu.make_async_copy(sib, rows.at[1], sems.at[5]))
    start_and_wait(loads)


def stackb_kernel(index, *refs):
    found, (out, sems) = refs[:8], refs[8:]
    start_and_wait(
        [
            pltpu.make_async_copy(found[r], out.at[(index[2] + r) % 8], sems.at[r])
            for r in range(8)
        ]
    )


def finish_kernel(index, pieces, inside, reads, owns, gain, mixed):
    _, x = earlier(pieces, pieces.shape[0], index[0], head_masks(256))
    t = inside[...]
    state = mm(split(t[:HEAD]), stacked(split(x), head_masks())) + t[HEAD:]
    out = finish(reads[...], owns[...], state, gain[...])
    rows = out.shape[0] // 8
    core = index[1]
    parts = [[out[(2 * y + c) * rows : (2 * y + c + 1) * rows] for y in range(4)] for c in range(2)]
    for d in range(4):
        for y in range(4):
            for c in range(2):
                at = y * rows + (c ^ core) * (4 * rows)
                mixed[d, pl.ds(pl.multiple_of(at, 16), rows)] = parts[c][y]


def proj_kernel(index, own, sib, r0, r1, r2, r3, weight, gain, mid, normed, resid, w, sems):
    core = index[1]
    loads = [
        pltpu.make_async_copy(
            weight.at[pl.ds(pl.multiple_of((2 * y + (c ^ core)) * 128, 128), 128)],
            w.at[pl.ds((4 * c + y) * 128, 128)],
            sems.at[4 * c + y],
        )
        for c in range(2)
        for y in range(4)
    ]
    for copy in loads:
        copy.start()
    for s, r in enumerate((r0, r1, r2, r3)):
        for n in range(2):
            resid[n, (index[4] + 4 - s) % 4] = r[n]
    half = own.shape[1] // 2
    sums = []
    for copy in loads[:4]:
        copy.wait()
    for n in range(2):
        left = jnp.concatenate([own[y, n * half : (n + 1) * half] for y in range(4)], axis=1)
        sums.append(dot(left, w[:512]))
    for copy in loads[4:]:
        copy.wait()
    for n in range(2):
        left = jnp.concatenate([sib[y, (1 - n) * half : (2 - n) * half] for y in range(4)], axis=1)
        rows = resid.shape[2]
        m = jnp.concatenate([resid[n, y] for y in range(4)], axis=0).astype(F32)
        m = m + (sums[n] + dot(left, w[512:]))
        m = m.astype(BF)
        if n == 0:
            for y in range(4):
                mid[y] = m[y * rows : (y + 1) * rows]
        m = m.astype(F32)
        scale = lax.rsqrt(jnp.mean(m * m, axis=-1, keepdims=True) + 1e-06)
        m = (m * scale * gain[...]).astype(BF)
        for k in range(8):
            normed[k, n * half : (n + 1) * half] = m[:, k * 256 : (k + 1) * 256]


def begin_kernel(index, normed, *refs):
    a, b, (acc, wa, wb, sems) = refs[:7], refs[7:11], refs[11:]
    z, x = index[2], index[3]
    order = (0, 1, 2, 3, 5, 6, 7)
    loads = [pltpu.make_async_copy(a[n], wa.at[n], sems.at[n]) for n in range(7)]
    loads += [
        pltpu.make_async_copy(
            b[s].at[:, :, 0 : wb.shape[3]], wb.at[:, (x + 4 - s) % 4], sems.at[7 + s]
        )
        for s in range(4)
    ]
    for copy in loads:
        copy.start()
    left = jnp.concatenate([normed[(z + r) % 8] for r in order], axis=1)
    na = wa.shape[3]
    for copy in loads[:7]:
        copy.wait()
    acc[:, :na] = dot(left, wa[...].reshape(-1, na))
    for copy in loads[7:]:
        copy.wait()
    left = jnp.concatenate([normed[k] for k in range(8)], axis=1)
    acc[:, na:] = dot(left, wb[...].reshape(-1, wb.shape[3]))


def end_kernel(index, normed, acc, *refs):
    a, b, (keep, send, wa, wb, sems) = refs[0], refs[1:5], refs[5:]
    z, x = index[2], index[3]
    cols = wb.shape[3]
    skip = b[0].shape[2] - cols
    first = pltpu.make_async_copy(a, wa, sems.at[0])
    loads = [
        pltpu.make_async_copy(
            b[s].at[:, :, skip : skip + cols], wb.at[:, (x + 4 - s) % 4], sems.at[1 + s]
        )
        for s in range(4)
    ]
    for copy in [first] + loads:
        copy.start()
    first.wait()
    na = wa.shape[2]
    both = acc[:, :na] + dot(normed[(z + 4) % 8], wa[...].reshape(-1, na))
    both = jnp.concatenate([both, acc[:, na:]], axis=1)
    gate = both[:, :cols]
    hidden = (gate * (1.0 / (1.0 + jnp.exp(-gate))) * both[:, cols:]).astype(BF)
    for copy in loads:
        copy.wait()
    half, rows = hidden.shape[0] // 2, hidden.shape[0] // 8
    for k in range(8):
        out = dot_t(hidden, wb[k].reshape(-1, cols)).astype(BF)
        for y in range(4):
            keep[y, k] = out[y * rows : (y + 1) * rows]
            send[y, k] = out[half + y * rows : half + (y + 1) * rows]


def final_kernel(index, pieces, mid, result):
    m = mid[index[4]].astype(F32)
    for k in range(8):
        total = pieces[0, k].astype(F32)
        for y in range(1, 4):
            total = total + pieces[y, k].astype(F32)
        at = slice(k * 256, (k + 1) * 256)
        result[:, at] = (m[:, at] + 0.5 * total).astype(BF)


def vmem(n):
    return [pl.BlockSpec(memory_space=pltpu.VMEM)] * n


SMEM = pl.BlockSpec(memory_space=pltpu.SMEM)
ANY = pl.BlockSpec(memory_space=pl.ANY)
HBM = pl.BlockSpec(memory_space=pltpu.MemorySpace.HBM)
shape = jax.ShapeDtypeStruct


def call(kernel, name, out, in_specs, us, mib=16, scratch=(), space=None):
    def run(*args):
        return pl.pallas_call(
            kernel,
            out_shape=out,
            in_specs=in_specs,
            out_specs=space
            if isinstance(space, tuple)
            else jax.tree.map(lambda _: space or vmem(1)[0], out),
            scratch_shapes=scratch,
            compiler_params=pltpu.CompilerParams(vmem_limit_bytes=LIMIT.get(name, mib << 20)),
            cost_estimate=pl.CostEstimate(
                flops=int(us * FLOPS_US), bytes_accessed=0, transcendentals=0
            ),
        )(*args)

    return run


FLOPS_US = 1e8
LIMIT = {"pack": None, "local": None}
NA = 1152


def per_device(
    resid,
    queries,
    keys,
    values,
    decay_input_part,
    decay_channel_offset,
    decay_head_extra,
    correction_rate_input,
    correction_rate_offset,
    head_norm_gain,
    mixer_output_weight,
    feedforward_norm_gain,
    gate_weight,
    up_weight,
    down_weight,
):
    tok, cols = queries.shape[0], gate_weight.shape[1]
    z, x, y, c = (lax.axis_index(a).astype(jnp.int32) for a in ("z", "x", "y", "c"))
    index = jnp.stack([z, c, z, x, y])

    def exchanged(array, axis):
        return lax.all_to_all(array, axis, split_axis=0, concat_axis=0, tiled=True)

    def shifted(array, axis, by):
        n = lax.axis_size(axis)
        return lax.ppermute(array, axis, [(i, (i + by) % n) for i in range(n)])

    part_a, part_b = call(
        pack_kernel,
        "pack",
        (shape((64, NA), BF), shape((64, 3 * cols - NA), BF)),
        vmem(3),
        1,
        8,
    )(gate_weight, up_weight, down_weight.T)
    down_up = down_dn = part_b
    found_b = {0: part_b}
    for s in range(1, 5):
        found_b[8 - s] = down_up = shifted(down_up, "z", 1)
        if s < 4:
            found_b[s] = down_dn = shifted(down_dn, "z", -1)
    near_a = [part_a] + [shifted(part_a, "x", s) for s in range(1, 4)]
    first, rows = call(
        stack_kernel,
        "stack",
        (shape((4, *part_a.shape), BF), shape((2, *resid.shape), BF)),
        [SMEM] + [ANY] * 6,
        1,
        8,
        [pltpu.SemaphoreType.DMA((6,))],
        ANY,
    )(index, *near_a, resid, shifted(resid, "c", 1))
    rows = [rows] + [shifted(rows, "y", s) for s in range(1, 4)]
    stack = call(
        stackb_kernel,
        "stackb",
        shape((8, *part_b.shape), BF),
        [SMEM] + [ANY] * 8,
        1,
        8,
        [pltpu.SemaphoreType.DMA((8,))],
        ANY,
    )(index, *[found_b[r] for r in range(8)])
    found = {0: first}
    up = down = first
    for s in range(1, 5):
        found[8 - s] = up = shifted(up, "z", 1)
        if s < 4:
            found[s] = down = shifted(down, "z", -1)
    pieces_b = [stack] + [shifted(stack, "x", s) for s in range(1, 4)]

    reads, owns, total = call(
        local_kernel,
        "local",
        (shape((tok, 128), F32), shape((tok, 128), F32), shape((128, 128), BF)),
        vmem(8),
        6,
        24,
        [
            pltpu.VMEM((tok, 128), F32),
            pltpu.VMEM((tok, 128), F32),
            pltpu.SemaphoreType.DMA((2,)),
        ],
        (HBM, HBM, vmem(1)[0]),
    )(
        queries,
        keys,
        values,
        decay_input_part,
        correction_rate_input,
        decay_channel_offset[None],
        correction_rate_offset[None],
        decay_head_extra.T,
    )
    near = [total] + [shifted(total, "x", s) for s in range(1, 4)]
    total, inside = call(
        group_kernel,
        "group",
        (shape((8, 128, 128), BF), shape((128, 128), F32)),
        [SMEM] + vmem(4),
        1,
        2,
        [pltpu.VMEM((4, 128, 128), BF)],
    )(x[None], *near)
    far = exchanged(total, "z")
    mixed = call(finish_kernel, "finish", shape((4, tok, 128), BF), [SMEM] + vmem(5), 3)(
        index, far, inside, reads, owns, head_norm_gain[None]
    )
    mixed_own = exchanged(mixed, "y")
    mixed_sib = shifted(mixed_own, "c", 1)
    mid, normed = call(
        proj_kernel,
        "proj",
        (shape((4, tok // 8, 2048), BF), shape((8, tok, 256), BF)),
        [SMEM] + vmem(6) + [ANY] + vmem(1),
        3,
        54,
        [
            pltpu.VMEM((2, 4, tok // 8, 2048), BF),
            pltpu.VMEM((1024, 2048), BF),
            pltpu.SemaphoreType.DMA((8,)),
        ],
    )(
        index,
        mixed_own,
        mixed_sib,
        *rows,
        mixer_output_weight,
        feedforward_norm_gain[None],
    )
    acc = call(
        begin_kernel,
        "begin",
        shape((tok, 2 * cols), F32),
        [SMEM] + vmem(1) + [ANY] * 11,
        5,
        24,
        [
            pltpu.VMEM((7, 4, 64, NA), BF),
            pltpu.VMEM((8, 4, 64, 2 * cols - NA), BF),
            pltpu.SemaphoreType.DMA((11,)),
        ],
    )(index, normed, *[found[r] for r in (0, 1, 2, 3, 5, 6, 7)], *pieces_b)
    part = shape((4, 8, tok // 8, 256), BF)
    keep, send = call(
        end_kernel,
        "end",
        (part, part),
        [SMEM] + vmem(2) + [ANY] * 5,
        4,
        24,
        [
            pltpu.VMEM((4, 64, NA), BF),
            pltpu.VMEM((8, 4, 64, cols), BF),
            pltpu.SemaphoreType.DMA((5,)),
        ],
    )(index, normed, acc, found[4], *pieces_b)
    pair = (keep.astype(F32) + shifted(send, "c", 1).astype(F32)).astype(BF)
    return call(final_kernel, "final", shape((tok // 8, 2048), BF), [SMEM] + vmem(2), 1)(
        index, exchanged(pair, "y"), mid
    )


def solution(mesh):
    torus = Mesh(mesh.devices.reshape(8, 4, 4, 2), ("z", "x", "y", "c"))
    sp, tp = ("z", "x"), ("y", "c")
    in_specs = (
        P(sp + tp, None),
        P(sp, tp),
        P(sp, tp),
        P(sp, tp),
        P(sp, tp),
        P(tp),
        P(sp, tp),
        P(sp, tp),
        P(tp),
        P(tp),
        P(),
        P(),
        P(sp, tp),
        P(sp, tp),
        P(tp, sp),
    )

    return jax.shard_map(
        per_device, mesh=torus, in_specs=in_specs, out_specs=P(sp + tp, None), check_vma=False
    )
```

```python
import jax
import jax.numpy as jnp
from jax import lax
from jax.experimental import pallas as pl
from jax.experimental.pallas import tpu as pltpu
from jax.sharding import Mesh
from jax.sharding import PartitionSpec as P

HEAD = 64
C = 64
BF = jnp.bfloat16
F32 = jnp.float32


def split(x):
    hi = x.astype(BF)
    return hi, (x - hi.astype(F32)).astype(BF)


def dot(a, b):
    return lax.dot_general(a, b, (((1,), (0,)), ((), ())), preferred_element_type=F32)


def dot_t(a, b):
    return lax.dot_general(a, b, (((1,), (1,)), ((), ())), preferred_element_type=F32)


def mm(x, y, f=dot):
    return f(x[0], y[0]) + (f(x[0], y[1]) + f(x[1], y[0]))


def iota(shape, dim):
    return lax.broadcasted_iota(jnp.int32, shape, dim)


def head_masks(width=128):
    first = (iota((1, width), 1) & 127) < HEAD
    m0 = jnp.where(first, 1.0, 0.0)
    return m0.astype(BF), (1.0 - m0).astype(BF)


def stacked(y, masks):
    return tuple(jnp.concatenate([p * masks[0], p * masks[1]], axis=0) for p in y)


def local_scan(q, k, v, dx, lx, dco, lro, extra):
    chunks = range(q.shape[0] // C)
    first = iota((1, 128), 1) < HEAD
    masks, masks2 = head_masks(), head_masks(256)
    ext = jnp.where(first, extra[:, 0:1], extra[:, 1:2])
    log_decay = -0.6065306597126334 * (1.0 / (1.0 + jnp.exp(-(dco + dx)))) - ext
    lrate = 1.0 / (1.0 + jnp.exp(-(lro + lx)))
    same_f = jnp.where((iota((128, 128), 0) < HEAD) == (iota((128, 128), 1) < HEAD), 1.0, 0.0)
    ones = same_f.astype(BF)
    kk = split(k * k)
    unit = k * lax.rsqrt(dot(kk[0], ones) + dot(kk[1], ones) + 1e-06)
    rate = lrate * unit
    row, col = iota((C, 128), 0), iota((C, 128), 1) & (C - 1)
    lower = row > col
    lower_eq = row >= col
    unit_packed = jnp.where(row == col, 1.0, 0.0)
    tri = jnp.where(iota((C, C), 0) >= iota((C, C), 1), 1.0, 0.0).astype(BF)
    eye = jnp.where(iota((128, 128), 0) == iota((128, 128), 1), 1.0, 0.0)
    levels = [((row >> n) == (col >> n) + 1) & (((row >> n) & 1) == 1) for n in range(6)]
    at = [slice(c * C, (c + 1) * C) for c in chunks]

    def each(f, *lists):
        return [f(*args) for args in zip(*lists)]

    def summed(lw):
        w0 = lw.astype(BF)
        w1, w2 = split(lw - w0.astype(F32))
        return dot(tri, w0) + (dot(tri, w1) + dot(tri, w2))

    lws = [log_decay[a] for a in at]
    cums = each(summed, lws)
    mids = [cum[C // 2 - 1 : C // 2] for cum in cums]
    ends = [cum[C - 1 : C] for cum in cums]
    falls = each(lambda cum, mid: jnp.exp(mid - cum), cums, mids)
    pcs = each(lambda cum, lw, mid, a: jnp.exp(cum - lw - mid) * unit[a], cums, lws, mids, at)
    ucs = each(lambda cum, mid, a: jnp.exp(cum - mid) * q[a], cums, mids, at)
    rcs = each(lambda fall, a: fall * rate[a], falls, at)
    gcs = each(lambda fall, a: fall * k[a], falls, at)

    def pairs(pc, uc, rc, gc):
        left = split(jnp.concatenate([pc, uc], axis=0))
        rs, gs = stacked(split(rc), masks), stacked(split(gc), masks)
        right = tuple(jnp.concatenate([a, b], axis=0) for a, b in zip(rs, gs))
        return mm(left, right, dot_t)

    pair = each(pairs, pcs, ucs, rcs, gcs)
    arps = [jnp.where(lower, p[:C, :128], 0.0) for p in pair]
    burs = [jnp.where(lower_eq, p[C:, :128], 0.0) for p in pair]

    def values_read(p, a):
        ab = split(
            jnp.concatenate(
                [jnp.where(lower, p[:C, 128:], 0.0), jnp.where(lower_eq, p[C:, 128:], 0.0)], axis=0
            )
        )
        vs = stacked((v[a].astype(BF),), masks)[0]
        return dot(ab[0], vs) + dot(ab[1], vs)

    abvs = each(values_read, pair, at)
    invs = [unit_packed - jnp.where(levels[0], arp, 0.0) for arp in arps]
    for n in range(1, 6):
        ss = each(split, invs)
        ts = each(
            lambda arp, s: mm(split(jnp.where(levels[n], arp, 0.0)), stacked(s, masks)), arps, ss
        )
        invs = each(lambda inv, s, t: inv - mm(s, stacked(split(t), masks)), invs, ss, ts)
    to_mids = each(jnp.exp, mids)
    wys = each(
        lambda inv, pc, to_mid, abv: split(
            mm(
                split(inv),
                stacked(split(jnp.concatenate([pc * to_mid, abv[:C]], axis=1)), masks2),
            )
        ),
        invs,
        pcs,
        to_mids,
        abvs,
    )
    bwys = each(lambda bur, wy: mm(split(bur), stacked(wy, masks2)), burs, wys)
    ueffs = each(lambda uc, to_mid, bwy: split(uc * to_mid - bwy[:, :128]), ucs, to_mids, bwys)
    own = each(lambda abv, bwy: abv[C:] - bwy[:, 128:], abvs, bwys)

    def change(rc, gc, mid, end, wy, a):
        rest = jnp.exp(end - mid)
        rwy = mm(split((rc * rest).T), wy)
        gs = split((gc * rest).T)
        vb = v[a].astype(BF)
        gv = dot(gs[0], vb) + dot(gs[1], vb)
        return split(eye * jnp.exp(end) - same_f * rwy[:, :128]), same_f * (gv - rwy[:, 128:])

    changes = each(change, rcs, gcs, mids, ends, wys, at)
    reads, owns = [], []
    both = jnp.concatenate([eye, jnp.zeros((128, 128), F32)], axis=1)
    for c in chunks:
        bs = split(both)
        out = mm(ueffs[c], bs)
        reads.append(out[:, :128])
        owns.append(own[c] + out[:, 128:])
        trans, state = changes[c]
        both = mm(trans, bs)
        both = jnp.concatenate([both[:, :128], both[:, 128:] + state], axis=1)
    total = jnp.concatenate(
        [both[:HEAD, :128] + both[HEAD:, :128], both[:HEAD, 128:] + both[HEAD:, 128:]], axis=0
    )
    return jnp.concatenate(reads, axis=0), jnp.concatenate(owns, axis=0), total


def local_kernel(q, k, v, dx, lx, dco, lro, extra, reads_out, owns_out, total, reads, owns, sems):
    f = lambda r: r[...].astype(F32)
    a, b, t = local_scan(f(q), f(k), f(v), f(dx), f(lx), dco[...], lro[...], extra[...].T)
    reads[...] = a
    owns[...] = b
    stores = [
        pltpu.make_async_copy(reads, reads_out, sems.at[0]),
        pltpu.make_async_copy(owns, owns_out, sems.at[1]),
    ]
    for copy in stores:
        copy.start()
    total[...] = sent(t[:HEAD], t[HEAD:])
    for copy in stores:
        copy.wait()


def finish(reads, owns, state, gain):
    masks = head_masks()
    out = owns + mm(split(reads), stacked(split(state), masks))
    same = (iota((128, 128), 0) < HEAD) == (iota((128, 128), 1) < HEAD)
    mean = jnp.where(same, 1.0 / HEAD, 0.0).astype(BF)
    s = split(out)
    center = out - (dot(s[0], mean) + dot(s[1], mean))
    s = split(center * center)
    spread = dot(s[0], mean) + dot(s[1], mean)
    return (center * lax.rsqrt(spread + 1e-05) * gain).astype(BF)


def fold(level, masks2):
    while len(level) > 1:
        nxt = []
        for i in range(0, len(level) - 1, 2):
            (t1, x1), (t2, x2) = level[i], level[i + 1]
            both = jnp.concatenate([t1, x1], axis=1)
            out = mm(split(t2), stacked(split(both), masks2))
            nxt.append((out[:, :128], out[:, 128:] + x2))
        if len(level) % 2:
            nxt.append(level[-1])
        level = nxt
    return level[0]


def eye_packed():
    return jnp.where(iota((HEAD, 128), 0) == (iota((HEAD, 128), 1) & (HEAD - 1)), 1.0, 0.0)


def piece(pieces, d):
    p = pieces[d].astype(F32)
    return p[:HEAD], p[HEAD:]


def sent(trans, state):
    return jnp.concatenate([trans - eye_packed(), state], axis=0).astype(BF)


def earlier(pieces, count, index, masks2):
    level = []
    for d in range(count - 1):
        used = jnp.where(d < index, 1.0, 0.0)
        trans, state = piece(pieces, d)
        level.append((trans * used + eye_packed(), state * used))
    return fold(level, masks2)


def group_kernel(index, near0, near1, near2, near3, total, inside, pieces):
    masks2 = head_masks(256)
    for s, near in enumerate((near0, near1, near2, near3)):
        pieces[(index[0] + 4 - s) % 4] = near[...]
    level = [piece(pieces, d) for d in range(4)]
    t, x = fold([(t + eye_packed(), x) for t, x in level], masks2)
    out = sent(t, x)
    for d in range(total.shape[0]):
        total[d] = out
    t, x = earlier(pieces, 4, index[0], masks2)
    inside[...] = jnp.concatenate([t, x], axis=0)


def pack_kernel(gate, up, down, a, b):
    cols = gate.shape[1]
    cut = a.shape[1] - cols
    a[:, :cols] = gate[...]
    a[:, cols:] = up[:, :cut]
    b[:, : cols - cut] = up[:, cut:]
    b[:, cols - cut :] = down[...]


def stack_kernel(index, near0, near1, near2, near3, own, sib, out, rows):
    for s, near in enumerate((near0, near1, near2, near3)):
        out[(index[3] + 4 - s) % 4] = near[...]
    rows[0] = own[...]
    rows[1] = sib[...]


def stackb_kernel(index, *refs):
    out = refs[8]
    for r in range(8):
        out[(index[2] + r) % 8] = refs[r][...]


def finish_kernel(index, pieces, inside, reads, owns, gain, mixed):
    _, x = earlier(pieces, pieces.shape[0], index[0], head_masks(256))
    t = inside[...]
    state = mm(split(t[:HEAD]), stacked(split(x), head_masks())) + t[HEAD:]
    out = finish(reads[...], owns[...], state, gain[...])
    rows = out.shape[0] // 8
    core = index[1]
    parts = [[out[(2 * y + c) * rows : (2 * y + c + 1) * rows] for y in range(4)] for c in range(2)]
    for d in range(4):
        for y in range(4):
            for c in range(2):
                at = y * rows + (c ^ core) * (4 * rows)
                mixed[d, pl.ds(pl.multiple_of(at, 16), rows)] = parts[c][y]


def proj_kernel(index, own, sib, r0, r1, r2, r3, weight, gain, mid, normed, resid, w, sems):
    core = index[1]
    loads = [
        pltpu.make_async_copy(
            weight.at[pl.ds(pl.multiple_of((2 * y + (c ^ core)) * 128, 128), 128)],
            w.at[pl.ds((4 * c + y) * 128, 128)],
            sems.at[4 * c + y],
        )
        for c in range(2)
        for y in range(4)
    ]
    for copy in loads:
        copy.start()
    for s, r in enumerate((r0, r1, r2, r3)):
        for n in range(2):
            resid[n, (index[4] + 4 - s) % 4] = r[n]
    half = own.shape[1] // 2
    sums = []
    for copy in loads[:4]:
        copy.wait()
    for n in range(2):
        left = jnp.concatenate([own[y, n * half : (n + 1) * half] for y in range(4)], axis=1)
        sums.append(dot(left, w[:512]))
    for copy in loads[4:]:
        copy.wait()
    for n in range(2):
        left = jnp.concatenate([sib[y, (1 - n) * half : (2 - n) * half] for y in range(4)], axis=1)
        rows = resid.shape[2]
        m = jnp.concatenate([resid[n, y] for y in range(4)], axis=0).astype(F32)
        m = m + (sums[n] + dot(left, w[512:]))
        m = m.astype(BF)
        if n == 0:
            for y in range(4):
                mid[y] = m[y * rows : (y + 1) * rows]
        m = m.astype(F32)
        scale = lax.rsqrt(jnp.mean(m * m, axis=-1, keepdims=True) + 1e-06)
        m = (m * scale * gain[...]).astype(BF)
        for k in range(8):
            normed[k, n * half : (n + 1) * half] = m[:, k * 256 : (k + 1) * 256]


def begin_kernel(index, normed, *refs):
    a, (acc, wa, sems) = refs[:7], refs[7:]
    loads = [pltpu.make_async_copy(a[n], wa.at[n], sems.at[n]) for n in range(7)]
    for copy in loads:
        copy.start()
    left = jnp.concatenate([normed[(index[2] + r) % 8] for r in (0, 1, 2, 3, 5, 6, 7)], axis=1)
    for copy in loads:
        copy.wait()
    acc[...] = dot(left, wa[...].reshape(-1, wa.shape[3]))


def end_kernel(index, normed, acc, *refs):
    a, b, (keep, send, wa, wb, sems) = refs[0], refs[1:5], refs[5:]
    z, x = index[2], index[3]
    na, nb = wa.shape[2], wb.shape[3]
    cols = (na + nb) // 3
    tail = 2 * cols - na
    first = pltpu.make_async_copy(a, wa, sems.at[0])
    loads = [
        pltpu.make_async_copy(b[s], wb.at[:, (x + 4 - s) % 4], sems.at[1 + s]) for s in range(4)
    ]
    for copy in [first] + loads:
        copy.start()
    first.wait()
    both = acc[...] + dot(normed[(z + 4) % 8], wa[...].reshape(-1, na))
    for copy in loads:
        copy.wait()
    left = jnp.concatenate([normed[k] for k in range(8)], axis=1)
    rest = dot(left, wb[:, :, :, :tail].reshape(-1, tail))
    both = jnp.concatenate([both, rest], axis=1)
    gate = both[:, :cols]
    hidden = (gate * (1.0 / (1.0 + jnp.exp(-gate))) * both[:, cols:]).astype(BF)
    half, rows = hidden.shape[0] // 2, hidden.shape[0] // 8
    for k in range(8):
        out = dot_t(hidden, wb[k, :, :, tail:].reshape(-1, cols)).astype(BF)
        for y in range(4):
            keep[y, k] = out[y * rows : (y + 1) * rows]
            send[y, k] = out[half + y * rows : half + (y + 1) * rows]


def final_kernel(index, pieces, mid, result):
    m = mid[index[4]].astype(F32)
    for k in range(8):
        total = pieces[0, k].astype(F32)
        for y in range(1, 4):
            total = total + pieces[y, k].astype(F32)
        at = slice(k * 256, (k + 1) * 256)
        result[:, at] = (m[:, at] + 0.5 * total).astype(BF)


def vmem(n):
    return [pl.BlockSpec(memory_space=pltpu.VMEM)] * n


SMEM = pl.BlockSpec(memory_space=pltpu.SMEM)
ANY = pl.BlockSpec(memory_space=pl.ANY)
HBM = pl.BlockSpec(memory_space=pltpu.MemorySpace.HBM)
shape = jax.ShapeDtypeStruct


def call(kernel, name, out, in_specs, us, mib=16, scratch=(), space=None):
    def run(*args):
        return pl.pallas_call(
            kernel,
            out_shape=out,
            in_specs=in_specs,
            out_specs=space
            if isinstance(space, tuple)
            else jax.tree.map(lambda _: space or vmem(1)[0], out),
            scratch_shapes=scratch,
            compiler_params=pltpu.CompilerParams(vmem_limit_bytes=LIMIT.get(name, mib << 20)),
            cost_estimate=pl.CostEstimate(
                flops=int(us * FLOPS_US), bytes_accessed=0, transcendentals=0
            ),
        )(*args)

    return run


FLOPS_US = 1e8
LIMIT = {"pack": None, "local": None}
NA = 1280


def per_device(
    resid,
    queries,
    keys,
    values,
    decay_input_part,
    decay_channel_offset,
    decay_head_extra,
    correction_rate_input,
    correction_rate_offset,
    head_norm_gain,
    mixer_output_weight,
    feedforward_norm_gain,
    gate_weight,
    up_weight,
    down_weight,
):
    tok, cols = queries.shape[0], gate_weight.shape[1]
    z, x, y, c = (lax.axis_index(a).astype(jnp.int32) for a in ("z", "x", "y", "c"))
    index = jnp.stack([z, c, z, x, y])

    def exchanged(array, axis):
        return lax.all_to_all(array, axis, split_axis=0, concat_axis=0, tiled=True)

    def shifted(array, axis, by):
        n = lax.axis_size(axis)
        return lax.ppermute(array, axis, [(i, (i + by) % n) for i in range(n)])

    part_a, part_b = call(
        pack_kernel,
        "pack",
        (shape((64, NA), BF), shape((64, 3 * cols - NA), BF)),
        vmem(3),
        1,
        8,
    )(gate_weight, up_weight, down_weight.T)
    down_up = down_dn = part_b
    found_b = {0: part_b}
    for s in range(1, 5):
        found_b[8 - s] = down_up = shifted(down_up, "z", 1)
        if s < 4:
            found_b[s] = down_dn = shifted(down_dn, "z", -1)
    near_a = [part_a] + [shifted(part_a, "x", s) for s in range(1, 4)]
    first, rows = call(
        stack_kernel,
        "stack",
        (shape((4, *part_a.shape), BF), shape((2, *resid.shape), BF)),
        [SMEM] + vmem(6),
        1,
        8,
    )(index, *near_a, resid, shifted(resid, "c", 1))
    rows = [rows] + [shifted(rows, "y", s) for s in range(1, 4)]
    stack = call(
        stackb_kernel,
        "stackb",
        shape((8, *part_b.shape), BF),
        [SMEM] + vmem(8),
        1,
        8,
    )(index, *[found_b[r] for r in range(8)])
    found = {0: first}
    up = down = first
    for s in range(1, 5):
        found[8 - s] = up = shifted(up, "z", 1)
        if s < 4:
            found[s] = down = shifted(down, "z", -1)
    pieces_b = [stack] + [shifted(stack, "x", s) for s in range(1, 4)]

    reads, owns, total = call(
        local_kernel,
        "local",
        (shape((tok, 128), F32), shape((tok, 128), F32), shape((128, 128), BF)),
        vmem(8),
        6,
        24,
        [
            pltpu.VMEM((tok, 128), F32),
            pltpu.VMEM((tok, 128), F32),
            pltpu.SemaphoreType.DMA((2,)),
        ],
        (HBM, HBM, vmem(1)[0]),
    )(
        queries,
        keys,
        values,
        decay_input_part,
        correction_rate_input,
        decay_channel_offset[None],
        correction_rate_offset[None],
        decay_head_extra.T,
    )
    near = [total] + [shifted(total, "x", s) for s in range(1, 4)]
    total, inside = call(
        group_kernel,
        "group",
        (shape((8, 128, 128), BF), shape((128, 128), F32)),
        [SMEM] + vmem(4),
        1,
        2,
        [pltpu.VMEM((4, 128, 128), BF)],
    )(x[None], *near)
    far = exchanged(total, "z")
    mixed = call(finish_kernel, "finish", shape((4, tok, 128), BF), [SMEM] + vmem(5), 3)(
        index, far, inside, reads, owns, head_norm_gain[None]
    )
    mixed_own = exchanged(mixed, "y")
    mixed_sib = shifted(mixed_own, "c", 1)
    mid, normed = call(
        proj_kernel,
        "proj",
        (shape((4, tok // 8, 2048), BF), shape((8, tok, 256), BF)),
        [SMEM] + vmem(6) + [ANY] + vmem(1),
        3,
        32,
        [
            pltpu.VMEM((2, 4, tok // 8, 2048), BF),
            pltpu.VMEM((1024, 2048), BF),
            pltpu.SemaphoreType.DMA((8,)),
        ],
    )(
        index,
        mixed_own,
        mixed_sib,
        *rows,
        mixer_output_weight,
        feedforward_norm_gain[None],
    )
    acc = call(
        begin_kernel,
        "begin",
        shape((tok, NA), F32),
        [SMEM] + vmem(1) + [ANY] * 7,
        5,
        24,
        [pltpu.VMEM((7, 4, 64, NA), BF), pltpu.SemaphoreType.DMA((7,))],
    )(index, normed, *[found[r] for r in (0, 1, 2, 3, 5, 6, 7)])
    part = shape((4, 8, tok // 8, 256), BF)
    keep, send = call(
        end_kernel,
        "end",
        (part, part),
        [SMEM] + vmem(2) + [ANY] * 5,
        4,
        24,
        [
            pltpu.VMEM((4, 64, NA), BF),
            pltpu.VMEM((8, 4, 64, 3 * cols - NA), BF),
            pltpu.SemaphoreType.DMA((5,)),
        ],
    )(index, normed, acc, found[4], *pieces_b)
    pair = (keep.astype(F32) + shifted(send, "c", 1).astype(F32)).astype(BF)
    return call(final_kernel, "final", shape((tok // 8, 2048), BF), [SMEM] + vmem(2), 1)(
        index, exchanged(pair, "y"), mid
    )


def solution(mesh):
    torus = Mesh(mesh.devices.reshape(8, 4, 4, 2), ("z", "x", "y", "c"))
    sp, tp = ("z", "x"), ("y", "c")
    in_specs = (
        P(sp + tp, None),
        P(sp, tp),
        P(sp, tp),
        P(sp, tp),
        P(sp, tp),
        P(tp),
        P(sp, tp),
        P(sp, tp),
        P(tp),
        P(tp),
        P(),
        P(),
        P(sp, tp),
        P(sp, tp),
        P(tp, sp),
    )

    return jax.shard_map(
        per_device, mesh=torus, in_specs=in_specs, out_specs=P(sp + tp, None), check_vma=False
    )
```

```python
import jax
import jax.numpy as jnp
from jax import lax
from jax.experimental import pallas as pl
from jax.experimental.pallas import tpu as pltpu
from jax.sharding import Mesh
from jax.sharding import PartitionSpec as P

HEAD = 64
C = 64
BF = jnp.bfloat16
F32 = jnp.float32


def split(x):
    hi = x.astype(BF)
    return hi, (x - hi.astype(F32)).astype(BF)


def dot(a, b):
    return lax.dot_general(a, b, (((1,), (0,)), ((), ())), preferred_element_type=F32)


def dot_t(a, b):
    return lax.dot_general(a, b, (((1,), (1,)), ((), ())), preferred_element_type=F32)


def mm(x, y, f=dot):
    return f(x[0], y[0]) + (f(x[0], y[1]) + f(x[1], y[0]))


def iota(shape, dim):
    return lax.broadcasted_iota(jnp.int32, shape, dim)


def head_masks(width=128):
    first = (iota((1, width), 1) & 127) < HEAD
    m0 = jnp.where(first, 1.0, 0.0)
    return m0.astype(BF), (1.0 - m0).astype(BF)


def stacked(y, masks):
    return tuple(jnp.concatenate([p * masks[0], p * masks[1]], axis=0) for p in y)


def local_scan(q, k, v, dx, lx, dco, lro, extra):
    chunks = range(q.shape[0] // C)
    first = iota((1, 128), 1) < HEAD
    masks, masks2 = head_masks(), head_masks(256)
    ext = jnp.where(first, extra[:, 0:1], extra[:, 1:2])
    log_decay = -0.6065306597126334 * (1.0 / (1.0 + jnp.exp(-(dco + dx)))) - ext
    lrate = 1.0 / (1.0 + jnp.exp(-(lro + lx)))
    same_f = jnp.where((iota((128, 128), 0) < HEAD) == (iota((128, 128), 1) < HEAD), 1.0, 0.0)
    ones = same_f.astype(BF)
    kk = split(k * k)
    unit = k * lax.rsqrt(dot(kk[0], ones) + dot(kk[1], ones) + 1e-06)
    rate = lrate * unit
    row, col = iota((C, 128), 0), iota((C, 128), 1) & (C - 1)
    lower = row > col
    lower_eq = row >= col
    unit_packed = jnp.where(row == col, 1.0, 0.0)
    tri = jnp.where(iota((C, C), 0) >= iota((C, C), 1), 1.0, 0.0).astype(BF)
    eye = jnp.where(iota((128, 128), 0) == iota((128, 128), 1), 1.0, 0.0)
    levels = [((row >> n) == (col >> n) + 1) & (((row >> n) & 1) == 1) for n in range(6)]
    at = [slice(c * C, (c + 1) * C) for c in chunks]

    def each(f, *lists):
        return [f(*args) for args in zip(*lists)]

    def summed(lw):
        w0 = lw.astype(BF)
        w1, w2 = split(lw - w0.astype(F32))
        return dot(tri, w0) + (dot(tri, w1) + dot(tri, w2))

    lws = [log_decay[a] for a in at]
    cums = each(summed, lws)
    mids = [cum[C // 2 - 1 : C // 2] for cum in cums]
    ends = [cum[C - 1 : C] for cum in cums]
    falls = each(lambda cum, mid: jnp.exp(mid - cum), cums, mids)
    pcs = each(lambda cum, lw, mid, a: jnp.exp(cum - lw - mid) * unit[a], cums, lws, mids, at)
    ucs = each(lambda cum, mid, a: jnp.exp(cum - mid) * q[a], cums, mids, at)
    rcs = each(lambda fall, a: fall * rate[a], falls, at)
    gcs = each(lambda fall, a: fall * k[a], falls, at)

    def pairs(pc, uc, rc, gc):
        left = split(jnp.concatenate([pc, uc], axis=0))
        rs, gs = stacked(split(rc), masks), stacked(split(gc), masks)
        right = tuple(jnp.concatenate([a, b], axis=0) for a, b in zip(rs, gs))
        return mm(left, right, dot_t)

    pair = each(pairs, pcs, ucs, rcs, gcs)
    arps = [jnp.where(lower, p[:C, :128], 0.0) for p in pair]
    burs = [jnp.where(lower_eq, p[C:, :128], 0.0) for p in pair]

    def values_read(p, a):
        ab = split(
            jnp.concatenate(
                [jnp.where(lower, p[:C, 128:], 0.0), jnp.where(lower_eq, p[C:, 128:], 0.0)], axis=0
            )
        )
        vs = stacked((v[a].astype(BF),), masks)[0]
        return dot(ab[0], vs) + dot(ab[1], vs)

    abvs = each(values_read, pair, at)
    invs = [unit_packed - jnp.where(levels[0], arp, 0.0) for arp in arps]
    for n in range(1, 6):
        ss = each(split, invs)
        ts = each(
            lambda arp, s: mm(split(jnp.where(levels[n], arp, 0.0)), stacked(s, masks)), arps, ss
        )
        invs = each(lambda inv, s, t: inv - mm(s, stacked(split(t), masks)), invs, ss, ts)
    to_mids = each(jnp.exp, mids)
    wys = each(
        lambda inv, pc, to_mid, abv: split(
            mm(
                split(inv),
                stacked(split(jnp.concatenate([pc * to_mid, abv[:C]], axis=1)), masks2),
            )
        ),
        invs,
        pcs,
        to_mids,
        abvs,
    )
    bwys = each(lambda bur, wy: mm(split(bur), stacked(wy, masks2)), burs, wys)
    ueffs = each(lambda uc, to_mid, bwy: split(uc * to_mid - bwy[:, :128]), ucs, to_mids, bwys)
    own = each(lambda abv, bwy: abv[C:] - bwy[:, 128:], abvs, bwys)

    def change(rc, gc, mid, end, wy, a):
        rest = jnp.exp(end - mid)
        rwy = mm(split((rc * rest).T), wy)
        gs = split((gc * rest).T)
        vb = v[a].astype(BF)
        gv = dot(gs[0], vb) + dot(gs[1], vb)
        return split(eye * jnp.exp(end) - same_f * rwy[:, :128]), same_f * (gv - rwy[:, 128:])

    changes = each(change, rcs, gcs, mids, ends, wys, at)
    reads, owns = [], []
    both = jnp.concatenate([eye, jnp.zeros((128, 128), F32)], axis=1)
    for c in chunks:
        bs = split(both)
        out = mm(ueffs[c], bs)
        reads.append(out[:, :128])
        owns.append(own[c] + out[:, 128:])
        trans, state = changes[c]
        both = mm(trans, bs)
        both = jnp.concatenate([both[:, :128], both[:, 128:] + state], axis=1)
    total = jnp.concatenate(
        [both[:HEAD, :128] + both[HEAD:, :128], both[:HEAD, 128:] + both[HEAD:, 128:]], axis=0
    )
    return jnp.concatenate(reads, axis=0), jnp.concatenate(owns, axis=0), total


def local_kernel(resid, core_rows, q, k, v, dx, lx, dco, lro, extra, *refs):
    reads_out, owns_out, rows, total, reads, owns, sems = refs
    moves = [
        pltpu.make_async_copy(resid, rows.at[0], sems.at[2]),
        pltpu.make_async_copy(core_rows, rows.at[1], sems.at[3]),
        pltpu.make_async_copy(reads, reads_out, sems.at[0]),
        pltpu.make_async_copy(owns, owns_out, sems.at[1]),
    ]
    for copy in moves[:2]:
        copy.start()
    f = lambda r: r[...].astype(F32)
    a, b, t = local_scan(f(q), f(k), f(v), f(dx), f(lx), dco[...], lro[...], extra[...].T)
    reads[...] = a
    owns[...] = b
    for copy in moves[2:]:
        copy.start()
    total[...] = sent(t[:HEAD], t[HEAD:])
    for copy in moves:
        copy.wait()


def finish(reads, owns, state, gain):
    masks = head_masks()
    out = owns + mm(split(reads), stacked(split(state), masks))
    same = (iota((128, 128), 0) < HEAD) == (iota((128, 128), 1) < HEAD)
    mean = jnp.where(same, 1.0 / HEAD, 0.0).astype(BF)
    s = split(out)
    center = out - (dot(s[0], mean) + dot(s[1], mean))
    s = split(center * center)
    spread = dot(s[0], mean) + dot(s[1], mean)
    return (center * lax.rsqrt(spread + 1e-05) * gain).astype(BF)


def fold(level, masks2):
    while len(level) > 1:
        nxt = []
        for i in range(0, len(level) - 1, 2):
            (t1, x1), (t2, x2) = level[i], level[i + 1]
            both = jnp.concatenate([t1, x1], axis=1)
            out = mm(split(t2), stacked(split(both), masks2))
            nxt.append((out[:, :128], out[:, 128:] + x2))
        if len(level) % 2:
            nxt.append(level[-1])
        level = nxt
    return level[0]


def eye_packed():
    return jnp.where(iota((HEAD, 128), 0) == (iota((HEAD, 128), 1) & (HEAD - 1)), 1.0, 0.0)


def piece(pieces, d):
    p = pieces[d].astype(F32)
    return p[:HEAD], p[HEAD:]


def sent(trans, state):
    return jnp.concatenate([trans - eye_packed(), state], axis=0).astype(BF)


def earlier(pieces, count, index, masks2):
    level = []
    for d in range(count - 1):
        used = jnp.where(d < index, 1.0, 0.0)
        trans, state = piece(pieces, d)
        level.append((trans * used + eye_packed(), state * used))
    return fold(level, masks2)


def group_kernel(index, near0, near1, near2, near3, total, inside, pieces):
    masks2 = head_masks(256)
    for s, near in enumerate((near0, near1, near2, near3)):
        pieces[(index[0] + 4 - s) % 4] = near[...]
    level = [piece(pieces, d) for d in range(4)]
    t, x = fold([(t + eye_packed(), x) for t, x in level], masks2)
    out = sent(t, x)
    for d in range(total.shape[0]):
        total[d] = out
    t, x = earlier(pieces, 4, index[0], masks2)
    inside[...] = jnp.concatenate([t, x], axis=0)


def pack_kernel(gate, up, down, a, b):
    cols = gate.shape[1]
    cut = a.shape[2] - cols
    for n in range(a.shape[0]):
        a[n, :, :cols] = gate[...]
        a[n, :, cols:] = up[:, :cut]
    b[:, : cols - cut] = up[:, cut:]
    b[:, cols - cut :] = down[...]


def stackb_kernel(index, *refs):
    out = refs[8]
    for r in range(8):
        out[(index[2] + r) % 8] = refs[r][...]


def finish_kernel(index, pieces, inside, reads, owns, gain, mixed):
    _, x = earlier(pieces, pieces.shape[0], index[0], head_masks(256))
    t = inside[...]
    state = mm(split(t[:HEAD]), stacked(split(x), head_masks())) + t[HEAD:]
    out = finish(reads[...], owns[...], state, gain[...])
    rows = out.shape[0] // 8
    core = index[1]
    parts = [[out[(2 * y + c) * rows : (2 * y + c + 1) * rows] for y in range(4)] for c in range(2)]
    for d in range(4):
        for y in range(4):
            for c in range(2):
                at = y * rows + (c ^ core) * (4 * rows)
                mixed[d, pl.ds(pl.multiple_of(at, 16), rows)] = parts[c][y]


def proj_kernel(index, own, sib, r0, r1, r2, r3, weight, gain, mid, normed, resid, w, sems):
    core = index[1]
    loads = [
        pltpu.make_async_copy(
            weight.at[pl.ds(pl.multiple_of((2 * y + (c ^ core)) * 128, 128), 128)],
            w.at[pl.ds((4 * c + y) * 128, 128)],
            sems.at[4 * c + y],
        )
        for c in range(2)
        for y in range(4)
    ]
    for copy in loads:
        copy.start()
    for s, r in enumerate((r0, r1, r2, r3)):
        for n in range(2):
            resid[n, (index[4] + 4 - s) % 4] = r[n]
    half = own.shape[1] // 2
    sums = []
    for copy in loads[:4]:
        copy.wait()
    for n in range(2):
        left = jnp.concatenate([own[y, n * half : (n + 1) * half] for y in range(4)], axis=1)
        sums.append(dot(left, w[:512]))
    for copy in loads[4:]:
        copy.wait()
    for n in range(2):
        left = jnp.concatenate([sib[y, (1 - n) * half : (2 - n) * half] for y in range(4)], axis=1)
        rows = resid.shape[2]
        m = jnp.concatenate([resid[n, y] for y in range(4)], axis=0).astype(F32)
        m = m + (sums[n] + dot(left, w[512:]))
        m = m.astype(BF)
        if n == 0:
            for y in range(4):
                mid[y] = m[y * rows : (y + 1) * rows]
        m = m.astype(F32)
        scale = lax.rsqrt(jnp.mean(m * m, axis=-1, keepdims=True) + 1e-06)
        m = (m * scale * gain[...]).astype(BF)
        for k in range(8):
            normed[k, n * half : (n + 1) * half] = m[:, k * 256 : (k + 1) * 256]


def begin_kernel(index, normed, *refs):
    a, (acc, wa, sems) = refs[:7], refs[7:]
    loads = [pltpu.make_async_copy(a[n], wa.at[n], sems.at[n]) for n in range(7)]
    for copy in loads:
        copy.start()
    left = jnp.concatenate([normed[(index[2] + r) % 8] for r in (0, 1, 2, 3, 5, 6, 7)], axis=1)
    for copy in loads:
        copy.wait()
    acc[...] = dot(left, wa[...].reshape(-1, wa.shape[3]))


def end_kernel(index, normed, acc, *refs):
    a, b, (keep, send, wa, wb, sems) = refs[0], refs[1:5], refs[5:]
    z, x = index[2], index[3]
    na, nb = wa.shape[2], wb.shape[3]
    cols = (na + nb) // 3
    tail = 2 * cols - na
    first = pltpu.make_async_copy(a, wa, sems.at[0])
    loads = [
        pltpu.make_async_copy(b[s], wb.at[:, (x + 4 - s) % 4], sems.at[1 + s]) for s in range(4)
    ]
    for copy in [first] + loads:
        copy.start()
    first.wait()
    both = acc[...] + dot(normed[(z + 4) % 8], wa[...].reshape(-1, na))
    for copy in loads:
        copy.wait()
    left = jnp.concatenate([normed[k] for k in range(8)], axis=1)
    rest = dot(left, wb[:, :, :, :tail].reshape(-1, tail))
    both = jnp.concatenate([both, rest], axis=1)
    gate = both[:, :cols]
    hidden = (gate * (1.0 / (1.0 + jnp.exp(-gate))) * both[:, cols:]).astype(BF)
    half, rows = hidden.shape[0] // 2, hidden.shape[0] // 8
    for k in range(8):
        out = dot_t(hidden, wb[k, :, :, tail:].reshape(-1, cols)).astype(BF)
        for y in range(4):
            keep[y, k] = out[y * rows : (y + 1) * rows]
            send[y, k] = out[half + y * rows : half + (y + 1) * rows]


def final_kernel(index, pieces, mid, result):
    m = mid[index[4]].astype(F32)
    for k in range(8):
        total = pieces[0, k].astype(F32)
        for y in range(1, 4):
            total = total + pieces[y, k].astype(F32)
        at = slice(k * 256, (k + 1) * 256)
        result[:, at] = (m[:, at] + 0.5 * total).astype(BF)


def vmem(n):
    return [pl.BlockSpec(memory_space=pltpu.VMEM)] * n


SMEM = pl.BlockSpec(memory_space=pltpu.SMEM)
ANY = pl.BlockSpec(memory_space=pl.ANY)
HBM = pl.BlockSpec(memory_space=pltpu.MemorySpace.HBM)
shape = jax.ShapeDtypeStruct


def call(kernel, name, out, in_specs, us, mib=16, scratch=(), space=None):
    def run(*args):
        return pl.pallas_call(
            kernel,
            out_shape=out,
            in_specs=in_specs,
            out_specs=space
            if isinstance(space, tuple)
            else jax.tree.map(lambda _: space or vmem(1)[0], out),
            scratch_shapes=scratch,
            compiler_params=pltpu.CompilerParams(vmem_limit_bytes=LIMIT.get(name, mib << 20)),
            cost_estimate=pl.CostEstimate(
                flops=int(us * FLOPS_US), bytes_accessed=0, transcendentals=0
            ),
        )(*args)

    return run


FLOPS_US = 1e8
LIMIT = {"pack": None, "local": None}
NA = 1152


def per_device(
    resid,
    queries,
    keys,
    values,
    decay_input_part,
    decay_channel_offset,
    decay_head_extra,
    correction_rate_input,
    correction_rate_offset,
    head_norm_gain,
    mixer_output_weight,
    feedforward_norm_gain,
    gate_weight,
    up_weight,
    down_weight,
):
    tok, cols = queries.shape[0], gate_weight.shape[1]
    z, x, y, c = (lax.axis_index(a).astype(jnp.int32) for a in ("z", "x", "y", "c"))
    index = jnp.stack([z, c, z, x, y])

    def exchanged(array, axis):
        return lax.all_to_all(array, axis, split_axis=0, concat_axis=0, tiled=True)

    def shifted(array, axis, by):
        n = lax.axis_size(axis)
        return lax.ppermute(array, axis, [(i, (i + by) % n) for i in range(n)])

    part_a, part_b = call(
        pack_kernel,
        "pack",
        (shape((4, 64, NA), BF), shape((64, 3 * cols - NA), BF)),
        vmem(3),
        1,
        8,
    )(gate_weight, up_weight, down_weight.T)
    down_up = down_dn = part_b
    found_b = {0: part_b}
    for s in range(1, 5):
        found_b[8 - s] = down_up = shifted(down_up, "z", 1)
        if s < 4:
            found_b[s] = down_dn = shifted(down_dn, "z", -1)
    first = exchanged(part_a, "x")
    core_rows = shifted(resid, "c", 1)
    stack = call(
        stackb_kernel,
        "stackb",
        shape((8, *part_b.shape), BF),
        [SMEM] + vmem(8),
        1,
        8,
    )(index, *[found_b[r] for r in range(8)])
    found = {0: first}
    up = down = first
    for s in range(1, 5):
        found[8 - s] = up = shifted(up, "z", 1)
        if s < 4:
            found[s] = down = shifted(down, "z", -1)
    pieces_b = [stack] + [shifted(stack, "x", s) for s in range(1, 4)]

    reads, owns, rows, total = call(
        local_kernel,
        "local",
        (
            shape((tok, 128), F32),
            shape((tok, 128), F32),
            shape((2, *resid.shape), BF),
            shape((128, 128), BF),
        ),
        [ANY] * 2 + vmem(8),
        6,
        24,
        [
            pltpu.VMEM((tok, 128), F32),
            pltpu.VMEM((tok, 128), F32),
            pltpu.SemaphoreType.DMA((4,)),
        ],
        (HBM, HBM, HBM, vmem(1)[0]),
    )(
        resid,
        core_rows,
        queries,
        keys,
        values,
        decay_input_part,
        correction_rate_input,
        decay_channel_offset[None],
        correction_rate_offset[None],
        decay_head_extra.T,
    )
    rows = [rows] + [shifted(rows, "y", s) for s in range(1, 4)]
    near = [total] + [shifted(total, "x", s) for s in range(1, 4)]
    total, inside = call(
        group_kernel,
        "group",
        (shape((8, 128, 128), BF), shape((128, 128), F32)),
        [SMEM] + vmem(4),
        1,
        2,
        [pltpu.VMEM((4, 128, 128), BF)],
    )(x[None], *near)
    far = exchanged(total, "z")
    mixed = call(finish_kernel, "finish", shape((4, tok, 128), BF), [SMEM] + vmem(5), 3)(
        index, far, inside, reads, owns, head_norm_gain[None]
    )
    mixed_own = exchanged(mixed, "y")
    mixed_sib = shifted(mixed_own, "c", 1)
    mid, normed = call(
        proj_kernel,
        "proj",
        (shape((4, tok // 8, 2048), BF), shape((8, tok, 256), BF)),
        [SMEM] + vmem(6) + [ANY] + vmem(1),
        3,
        32,
        [
            pltpu.VMEM((2, 4, tok // 8, 2048), BF),
            pltpu.VMEM((1024, 2048), BF),
            pltpu.SemaphoreType.DMA((8,)),
        ],
    )(
        index,
        mixed_own,
        mixed_sib,
        *rows,
        mixer_output_weight,
        feedforward_norm_gain[None],
    )
    acc = call(
        begin_kernel,
        "begin",
        shape((tok, NA), F32),
        [SMEM] + vmem(1) + [ANY] * 7,
        5,
        24,
        [pltpu.VMEM((7, 4, 64, NA), BF), pltpu.SemaphoreType.DMA((7,))],
    )(index, normed, *[found[r] for r in (0, 1, 2, 3, 5, 6, 7)])
    part = shape((4, 8, tok // 8, 256), BF)
    keep, send = call(
        end_kernel,
        "end",
        (part, part),
        [SMEM] + vmem(2) + [ANY] * 5,
        4,
        24,
        [
            pltpu.VMEM((4, 64, NA), BF),
            pltpu.VMEM((8, 4, 64, 3 * cols - NA), BF),
            pltpu.SemaphoreType.DMA((5,)),
        ],
    )(index, normed, acc, found[4], *pieces_b)
    pair = (keep.astype(F32) + shifted(send, "c", 1).astype(F32)).astype(BF)
    return call(final_kernel, "final", shape((tok // 8, 2048), BF), [SMEM] + vmem(2), 1)(
        index, exchanged(pair, "y"), mid
    )


def solution(mesh):
    torus = Mesh(mesh.devices.reshape(8, 4, 4, 2), ("z", "x", "y", "c"))
    sp, tp = ("z", "x"), ("y", "c")
    in_specs = (
        P(sp + tp, None),
        P(sp, tp),
        P(sp, tp),
        P(sp, tp),
        P(sp, tp),
        P(tp),
        P(sp, tp),
        P(sp, tp),
        P(tp),
        P(tp),
        P(),
        P(),
        P(sp, tp),
        P(sp, tp),
        P(tp, sp),
    )

    return jax.shard_map(
        per_device, mesh=torus, in_specs=in_specs, out_specs=P(sp + tp, None), check_vma=False
    )
```

```python
import jax
import jax.numpy as jnp
from jax import lax
from jax.experimental import pallas as pl
from jax.experimental.pallas import tpu as pltpu
from jax.sharding import Mesh
from jax.sharding import PartitionSpec as P

HEAD = 64
C = 64
BF = jnp.bfloat16
F32 = jnp.float32


def split(x):
    hi = x.astype(BF)
    return hi, (x - hi.astype(F32)).astype(BF)


def dot(a, b):
    return lax.dot_general(a, b, (((1,), (0,)), ((), ())), preferred_element_type=F32)


def dot_t(a, b):
    return lax.dot_general(a, b, (((1,), (1,)), ((), ())), preferred_element_type=F32)


def mm(x, y, f=dot):
    return f(x[0], y[0]) + (f(x[0], y[1]) + f(x[1], y[0]))


def iota(shape, dim):
    return lax.broadcasted_iota(jnp.int32, shape, dim)


def head_masks(width=128):
    first = (iota((1, width), 1) & 127) < HEAD
    m0 = jnp.where(first, 1.0, 0.0)
    return m0.astype(BF), (1.0 - m0).astype(BF)


def stacked(y, masks):
    return tuple(jnp.concatenate([p * masks[0], p * masks[1]], axis=0) for p in y)


def local_scan(q, k, v, dx, lx, dco, lro, extra):
    chunks = range(q.shape[0] // C)
    first = iota((1, 128), 1) < HEAD
    masks, masks2 = head_masks(), head_masks(256)
    ext = jnp.where(first, extra[:, 0:1], extra[:, 1:2])
    log_decay = -0.6065306597126334 * (1.0 / (1.0 + jnp.exp(-(dco + dx)))) - ext
    lrate = 1.0 / (1.0 + jnp.exp(-(lro + lx)))
    same_f = jnp.where((iota((128, 128), 0) < HEAD) == (iota((128, 128), 1) < HEAD), 1.0, 0.0)
    ones = same_f.astype(BF)
    kk = split(k * k)
    unit = k * lax.rsqrt(dot(kk[0], ones) + dot(kk[1], ones) + 1e-06)
    rate = lrate * unit
    row, col = iota((C, 128), 0), iota((C, 128), 1) & (C - 1)
    lower = row > col
    lower_eq = row >= col
    unit_packed = jnp.where(row == col, 1.0, 0.0)
    tri = jnp.where(iota((C, C), 0) >= iota((C, C), 1), 1.0, 0.0).astype(BF)
    eye = jnp.where(iota((128, 128), 0) == iota((128, 128), 1), 1.0, 0.0)
    levels = [((row >> n) == (col >> n) + 1) & (((row >> n) & 1) == 1) for n in range(6)]
    at = [slice(c * C, (c + 1) * C) for c in chunks]

    def each(f, *lists):
        return [f(*args) for args in zip(*lists)]

    def summed(lw):
        w0 = lw.astype(BF)
        w1, w2 = split(lw - w0.astype(F32))
        return dot(tri, w0) + (dot(tri, w1) + dot(tri, w2))

    lws = [log_decay[a] for a in at]
    cums = each(summed, lws)
    mids = [cum[C // 2 - 1 : C // 2] for cum in cums]
    ends = [cum[C - 1 : C] for cum in cums]
    falls = each(lambda cum, mid: jnp.exp(mid - cum), cums, mids)
    pcs = each(lambda cum, lw, mid, a: jnp.exp(cum - lw - mid) * unit[a], cums, lws, mids, at)
    ucs = each(lambda cum, mid, a: jnp.exp(cum - mid) * q[a], cums, mids, at)
    rcs = each(lambda fall, a: fall * rate[a], falls, at)
    gcs = each(lambda fall, a: fall * k[a], falls, at)

    def pairs(pc, uc, rc, gc):
        left = split(jnp.concatenate([pc, uc], axis=0))
        rs, gs = stacked(split(rc), masks), stacked(split(gc), masks)
        right = tuple(jnp.concatenate([a, b], axis=0) for a, b in zip(rs, gs))
        return mm(left, right, dot_t)

    pair = each(pairs, pcs, ucs, rcs, gcs)
    arps = [jnp.where(lower, p[:C, :128], 0.0) for p in pair]
    burs = [jnp.where(lower_eq, p[C:, :128], 0.0) for p in pair]

    def values_read(p, a):
        ab = split(
            jnp.concatenate(
                [jnp.where(lower, p[:C, 128:], 0.0), jnp.where(lower_eq, p[C:, 128:], 0.0)], axis=0
            )
        )
        vs = stacked((v[a].astype(BF),), masks)[0]
        return dot(ab[0], vs) + dot(ab[1], vs)

    abvs = each(values_read, pair, at)
    invs = [unit_packed - jnp.where(levels[0], arp, 0.0) for arp in arps]
    for n in range(1, 6):
        ss = each(split, invs)
        ts = each(
            lambda arp, s: mm(split(jnp.where(levels[n], arp, 0.0)), stacked(s, masks)), arps, ss
        )
        invs = each(lambda inv, s, t: inv - mm(s, stacked(split(t), masks)), invs, ss, ts)
    to_mids = each(jnp.exp, mids)
    wys = each(
        lambda inv, pc, to_mid, abv: split(
            mm(
                split(inv),
                stacked(split(jnp.concatenate([pc * to_mid, abv[:C]], axis=1)), masks2),
            )
        ),
        invs,
        pcs,
        to_mids,
        abvs,
    )
    bwys = each(lambda bur, wy: mm(split(bur), stacked(wy, masks2)), burs, wys)
    ueffs = each(lambda uc, to_mid, bwy: split(uc * to_mid - bwy[:, :128]), ucs, to_mids, bwys)
    own = each(lambda abv, bwy: abv[C:] - bwy[:, 128:], abvs, bwys)

    def change(rc, gc, mid, end, wy, a):
        rest = jnp.exp(end - mid)
        rwy = mm(split((rc * rest).T), wy)
        gs = split((gc * rest).T)
        vb = v[a].astype(BF)
        gv = dot(gs[0], vb) + dot(gs[1], vb)
        return split(eye * jnp.exp(end) - same_f * rwy[:, :128]), same_f * (gv - rwy[:, 128:])

    changes = each(change, rcs, gcs, mids, ends, wys, at)
    reads, owns = [], []
    both = jnp.concatenate([eye, jnp.zeros((128, 128), F32)], axis=1)
    for c in chunks:
        bs = split(both)
        out = mm(ueffs[c], bs)
        reads.append(out[:, :128])
        owns.append(own[c] + out[:, 128:])
        trans, state = changes[c]
        both = mm(trans, bs)
        both = jnp.concatenate([both[:, :128], both[:, 128:] + state], axis=1)
    total = jnp.concatenate(
        [both[:HEAD, :128] + both[HEAD:, :128], both[:HEAD, 128:] + both[HEAD:, 128:]], axis=0
    )
    return jnp.concatenate(reads, axis=0), jnp.concatenate(owns, axis=0), total


def local_kernel(resid, core_rows, q, k, v, dx, lx, dco, lro, extra, *refs):
    reads_out, owns_out, rows, total, reads, owns, sems = refs
    rows[0] = resid[...]
    rows[1] = core_rows[...]
    f = lambda r: r[...].astype(F32)
    a, b, t = local_scan(f(q), f(k), f(v), f(dx), f(lx), dco[...], lro[...], extra[...].T)
    reads[...] = a
    owns[...] = b
    stores = [
        pltpu.make_async_copy(reads, reads_out, sems.at[0]),
        pltpu.make_async_copy(owns, owns_out, sems.at[1]),
    ]
    for copy in stores:
        copy.start()
    total[...] = sent(t[:HEAD], t[HEAD:])
    for copy in stores:
        copy.wait()


def finish(reads, owns, state, gain):
    masks = head_masks()
    out = owns + mm(split(reads), stacked(split(state), masks))
    same = (iota((128, 128), 0) < HEAD) == (iota((128, 128), 1) < HEAD)
    mean = jnp.where(same, 1.0 / HEAD, 0.0).astype(BF)
    s = split(out)
    center = out - (dot(s[0], mean) + dot(s[1], mean))
    s = split(center * center)
    spread = dot(s[0], mean) + dot(s[1], mean)
    return (center * lax.rsqrt(spread + 1e-05) * gain).astype(BF)


def fold(level, masks2):
    while len(level) > 1:
        nxt = []
        for i in range(0, len(level) - 1, 2):
            (t1, x1), (t2, x2) = level[i], level[i + 1]
            both = jnp.concatenate([t1, x1], axis=1)
            out = mm(split(t2), stacked(split(both), masks2))
            nxt.append((out[:, :128], out[:, 128:] + x2))
        if len(level) % 2:
            nxt.append(level[-1])
        level = nxt
    return level[0]


def eye_packed():
    return jnp.where(iota((HEAD, 128), 0) == (iota((HEAD, 128), 1) & (HEAD - 1)), 1.0, 0.0)


def piece(pieces, d):
    p = pieces[d].astype(F32)
    return p[:HEAD], p[HEAD:]


def sent(trans, state):
    return jnp.concatenate([trans - eye_packed(), state], axis=0).astype(BF)


def earlier(pieces, count, index, masks2):
    level = []
    for d in range(count - 1):
        used = jnp.where(d < index, 1.0, 0.0)
        trans, state = piece(pieces, d)
        level.append((trans * used + eye_packed(), state * used))
    return fold(level, masks2)


def group_kernel(index, near0, near1, near2, near3, total, inside, pieces):
    masks2 = head_masks(256)
    for s, near in enumerate((near0, near1, near2, near3)):
        pieces[(index[0] + 4 - s) % 4] = near[...]
    level = [piece(pieces, d) for d in range(4)]
    t, x = fold([(t + eye_packed(), x) for t, x in level], masks2)
    out = sent(t, x)
    for d in range(total.shape[0]):
        total[d] = out
    t, x = earlier(pieces, 4, index[0], masks2)
    inside[...] = jnp.concatenate([t, x], axis=0)


def pack_kernel(gate, up, down, a, b):
    cols = gate.shape[1]
    cut = a.shape[2] - cols
    for n in range(a.shape[0]):
        a[n, :, :cols] = gate[...]
        a[n, :, cols:] = up[:, :cut]
    b[:, : cols - cut] = up[:, cut:]
    b[:, cols - cut :] = down[...]


def stackb_kernel(index, *refs):
    out = refs[8]
    for r in range(8):
        out[(index[2] + r) % 8] = refs[r][...]


def finish_kernel(index, pieces, inside, reads, owns, gain, mixed):
    _, x = earlier(pieces, pieces.shape[0], index[0], head_masks(256))
    t = inside[...]
    state = mm(split(t[:HEAD]), stacked(split(x), head_masks())) + t[HEAD:]
    out = finish(reads[...], owns[...], state, gain[...])
    rows = out.shape[0] // 8
    core = index[1]
    parts = [[out[(2 * y + c) * rows : (2 * y + c + 1) * rows] for y in range(4)] for c in range(2)]
    for d in range(4):
        for y in range(4):
            for c in range(2):
                at = y * rows + (c ^ core) * (4 * rows)
                mixed[d, pl.ds(pl.multiple_of(at, 16), rows)] = parts[c][y]


def proj_kernel(index, own, sib, r0, r1, r2, r3, weight, gain, mid, normed, resid, w, sems):
    core = index[1]
    loads = [
        pltpu.make_async_copy(
            weight.at[pl.ds(pl.multiple_of((2 * y + (c ^ core)) * 128, 128), 128)],
            w.at[pl.ds((4 * c + y) * 128, 128)],
            sems.at[4 * c + y],
        )
        for c in range(2)
        for y in range(4)
    ]
    for copy in loads:
        copy.start()
    for s, r in enumerate((r0, r1, r2, r3)):
        for n in range(2):
            resid[n, (index[4] + 4 - s) % 4] = r[n]
    half = own.shape[1] // 2
    sums = []
    for copy in loads[:4]:
        copy.wait()
    for n in range(2):
        left = jnp.concatenate([own[y, n * half : (n + 1) * half] for y in range(4)], axis=1)
        sums.append(dot(left, w[:512]))
    for copy in loads[4:]:
        copy.wait()
    for n in range(2):
        left = jnp.concatenate([sib[y, (1 - n) * half : (2 - n) * half] for y in range(4)], axis=1)
        rows = resid.shape[2]
        m = jnp.concatenate([resid[n, y] for y in range(4)], axis=0).astype(F32)
        m = m + (sums[n] + dot(left, w[512:]))
        m = m.astype(BF)
        if n == 0:
            for y in range(4):
                mid[y] = m[y * rows : (y + 1) * rows]
        m = m.astype(F32)
        scale = lax.rsqrt(jnp.mean(m * m, axis=-1, keepdims=True) + 1e-06)
        m = (m * scale * gain[...]).astype(BF)
        for k in range(8):
            normed[k, n * half : (n + 1) * half] = m[:, k * 256 : (k + 1) * 256]


def begin_kernel(index, normed, *refs):
    a, (acc, wa, sems) = refs[:7], refs[7:]
    loads = [pltpu.make_async_copy(a[n], wa.at[n], sems.at[n]) for n in range(7)]
    for copy in loads:
        copy.start()
    left = jnp.concatenate([normed[(index[2] + r) % 8] for r in (0, 1, 2, 3, 5, 6, 7)], axis=1)
    for copy in loads:
        copy.wait()
    acc[...] = dot(left, wa[...].reshape(-1, wa.shape[3]))


def end_kernel(index, normed, acc, *refs):
    a, b, (keep, send, wa, wb, sems) = refs[0], refs[1:5], refs[5:]
    z, x = index[2], index[3]
    na, nb = wa.shape[2], wb.shape[3]
    cols = (na + nb) // 3
    tail = 2 * cols - na
    first = pltpu.make_async_copy(a, wa, sems.at[0])
    loads = [
        pltpu.make_async_copy(b[s], wb.at[:, (x + 4 - s) % 4], sems.at[1 + s]) for s in range(4)
    ]
    for copy in [first] + loads:
        copy.start()
    first.wait()
    both = acc[...] + dot(normed[(z + 4) % 8], wa[...].reshape(-1, na))
    for copy in loads:
        copy.wait()
    left = jnp.concatenate([normed[k] for k in range(8)], axis=1)
    rest = dot(left, wb[:, :, :, :tail].reshape(-1, tail))
    both = jnp.concatenate([both, rest], axis=1)
    gate = both[:, :cols]
    hidden = (gate * (1.0 / (1.0 + jnp.exp(-gate))) * both[:, cols:]).astype(BF)
    half, rows = hidden.shape[0] // 2, hidden.shape[0] // 8
    for k in range(8):
        out = dot_t(hidden, wb[k, :, :, tail:].reshape(-1, cols)).astype(BF)
        for y in range(4):
            keep[y, k] = out[y * rows : (y + 1) * rows]
            send[y, k] = out[half + y * rows : half + (y + 1) * rows]


def final_kernel(index, pieces, mid, result):
    m = mid[index[4]].astype(F32)
    for k in range(8):
        total = pieces[0, k].astype(F32)
        for y in range(1, 4):
            total = total + pieces[y, k].astype(F32)
        at = slice(k * 256, (k + 1) * 256)
        result[:, at] = (m[:, at] + 0.5 * total).astype(BF)


def vmem(n):
    return [pl.BlockSpec(memory_space=pltpu.VMEM)] * n


SMEM = pl.BlockSpec(memory_space=pltpu.SMEM)
ANY = pl.BlockSpec(memory_space=pl.ANY)
HBM = pl.BlockSpec(memory_space=pltpu.MemorySpace.HBM)
shape = jax.ShapeDtypeStruct


def call(kernel, name, out, in_specs, us, mib=16, scratch=(), space=None):
    def run(*args):
        return pl.pallas_call(
            kernel,
            out_shape=out,
            in_specs=in_specs,
            out_specs=space
            if isinstance(space, tuple)
            else jax.tree.map(lambda _: space or vmem(1)[0], out),
            scratch_shapes=scratch,
            compiler_params=pltpu.CompilerParams(vmem_limit_bytes=LIMIT.get(name, mib << 20)),
            cost_estimate=pl.CostEstimate(
                flops=int(us * FLOPS_US), bytes_accessed=0, transcendentals=0
            ),
        )(*args)

    return run


FLOPS_US = 1e8
LIMIT = {"pack": None, "local": None, "finish": 56 << 20, "group": 16 << 20}
NA = 1152


def per_device(
    resid,
    queries,
    keys,
    values,
    decay_input_part,
    decay_channel_offset,
    decay_head_extra,
    correction_rate_input,
    correction_rate_offset,
    head_norm_gain,
    mixer_output_weight,
    feedforward_norm_gain,
    gate_weight,
    up_weight,
    down_weight,
):
    tok, cols = queries.shape[0], gate_weight.shape[1]
    z, x, y, c = (lax.axis_index(a).astype(jnp.int32) for a in ("z", "x", "y", "c"))
    index = jnp.stack([z, c, z, x, y])

    def exchanged(array, axis):
        return lax.all_to_all(array, axis, split_axis=0, concat_axis=0, tiled=True)

    def shifted(array, axis, by):
        n = lax.axis_size(axis)
        return lax.ppermute(array, axis, [(i, (i + by) % n) for i in range(n)])

    part_a, part_b = call(
        pack_kernel,
        "pack",
        (shape((4, 64, NA), BF), shape((64, 3 * cols - NA), BF)),
        vmem(3),
        1,
        8,
    )(gate_weight, up_weight, down_weight.T)
    down_up = down_dn = part_b
    found_b = {0: part_b}
    for s in range(1, 5):
        found_b[8 - s] = down_up = shifted(down_up, "z", 1)
        if s < 4:
            found_b[s] = down_dn = shifted(down_dn, "z", -1)
    first = exchanged(part_a, "x")
    core_rows = shifted(resid, "c", 1)
    stack = call(
        stackb_kernel,
        "stackb",
        shape((8, *part_b.shape), BF),
        [SMEM] + vmem(8),
        1,
        8,
    )(index, *[found_b[r] for r in range(8)])
    found = {0: first}
    up = down = first
    for s in range(1, 5):
        found[8 - s] = up = shifted(up, "z", 1)
        if s < 4:
            found[s] = down = shifted(down, "z", -1)
    pieces_b = [stack] + [shifted(stack, "x", s) for s in range(1, 4)]

    reads, owns, rows, total = call(
        local_kernel,
        "local",
        (
            shape((tok, 128), F32),
            shape((tok, 128), F32),
            shape((2, *resid.shape), BF),
            shape((128, 128), BF),
        ),
        vmem(10),
        6,
        24,
        [
            pltpu.VMEM((tok, 128), F32),
            pltpu.VMEM((tok, 128), F32),
            pltpu.SemaphoreType.DMA((2,)),
        ],
        (HBM, HBM, vmem(1)[0], vmem(1)[0]),
    )(
        resid,
        core_rows,
        queries,
        keys,
        values,
        decay_input_part,
        correction_rate_input,
        decay_channel_offset[None],
        correction_rate_offset[None],
        decay_head_extra.T,
    )
    rows = [rows] + [shifted(rows, "y", s) for s in range(1, 4)]
    near = [total] + [shifted(total, "x", s) for s in range(1, 4)]
    total, inside = call(
        group_kernel,
        "group",
        (shape((8, 128, 128), BF), shape((128, 128), F32)),
        [SMEM] + vmem(4),
        1,
        2,
        [pltpu.VMEM((4, 128, 128), BF)],
    )(x[None], *near)
    far = exchanged(total, "z")
    mixed = call(finish_kernel, "finish", shape((4, tok, 128), BF), [SMEM] + vmem(5), 3)(
        index, far, inside, reads, owns, head_norm_gain[None]
    )
    mixed_own = exchanged(mixed, "y")
    mixed_sib = shifted(mixed_own, "c", 1)
    mid, normed = call(
        proj_kernel,
        "proj",
        (shape((4, tok // 8, 2048), BF), shape((8, tok, 256), BF)),
        [SMEM] + vmem(6) + [ANY] + vmem(1),
        3,
        48,
        [
            pltpu.VMEM((2, 4, tok // 8, 2048), BF),
            pltpu.VMEM((1024, 2048), BF),
            pltpu.SemaphoreType.DMA((8,)),
        ],
    )(
        index,
        mixed_own,
        mixed_sib,
        *rows,
        mixer_output_weight,
        feedforward_norm_gain[None],
    )
    acc = call(
        begin_kernel,
        "begin",
        shape((tok, NA), F32),
        [SMEM] + vmem(1) + [ANY] * 7,
        5,
        24,
        [pltpu.VMEM((7, 4, 64, NA), BF), pltpu.SemaphoreType.DMA((7,))],
    )(index, normed, *[found[r] for r in (0, 1, 2, 3, 5, 6, 7)])
    part = shape((4, 8, tok // 8, 256), BF)
    keep, send = call(
        end_kernel,
        "end",
        (part, part),
        [SMEM] + vmem(2) + [ANY] * 5,
        4,
        24,
        [
            pltpu.VMEM((4, 64, NA), BF),
            pltpu.VMEM((8, 4, 64, 3 * cols - NA), BF),
            pltpu.SemaphoreType.DMA((5,)),
        ],
    )(index, normed, acc, found[4], *pieces_b)
    pair = (keep.astype(F32) + shifted(send, "c", 1).astype(F32)).astype(BF)
    return call(final_kernel, "final", shape((tok // 8, 2048), BF), [SMEM] + vmem(2), 1)(
        index, exchanged(pair, "y"), mid
    )


def solution(mesh):
    torus = Mesh(mesh.devices.reshape(8, 4, 4, 2), ("z", "x", "y", "c"))
    sp, tp = ("z", "x"), ("y", "c")
    in_specs = (
        P(sp + tp, None),
        P(sp, tp),
        P(sp, tp),
        P(sp, tp),
        P(sp, tp),
        P(tp),
        P(sp, tp),
        P(sp, tp),
        P(tp),
        P(tp),
        P(),
        P(),
        P(sp, tp),
        P(sp, tp),
        P(tp, sp),
    )

    return jax.shard_map(
        per_device, mesh=torus, in_specs=in_specs, out_specs=P(sp + tp, None), check_vma=False
    )
```

```python
import jax
import jax.numpy as jnp
from jax import lax
from jax.experimental import pallas as pl
from jax.experimental.pallas import tpu as pltpu
from jax.sharding import Mesh
from jax.sharding import PartitionSpec as P

HEAD = 64
C = 64
BF = jnp.bfloat16
F32 = jnp.float32


def split(x):
    hi = x.astype(BF)
    return hi, (x - hi.astype(F32)).astype(BF)


def dot(a, b):
    return lax.dot_general(a, b, (((1,), (0,)), ((), ())), preferred_element_type=F32)


def dot_t(a, b):
    return lax.dot_general(a, b, (((1,), (1,)), ((), ())), preferred_element_type=F32)


def mm(x, y, f=dot):
    return f(x[0], y[0]) + (f(x[0], y[1]) + f(x[1], y[0]))


def iota(shape, dim):
    return lax.broadcasted_iota(jnp.int32, shape, dim)


def head_masks(width=128):
    first = (iota((1, width), 1) & 127) < HEAD
    m0 = jnp.where(first, 1.0, 0.0)
    return m0.astype(BF), (1.0 - m0).astype(BF)


def stacked(y, masks):
    return tuple(jnp.concatenate([p * masks[0], p * masks[1]], axis=0) for p in y)


def local_scan(q, k, v, dx, lx, dco, lro, extra):
    chunks = range(q.shape[0] // C)
    first = iota((1, 128), 1) < HEAD
    masks, masks2 = head_masks(), head_masks(256)
    ext = jnp.where(first, extra[:, 0:1], extra[:, 1:2])
    log_decay = -0.6065306597126334 * (1.0 / (1.0 + jnp.exp(-(dco + dx)))) - ext
    lrate = 1.0 / (1.0 + jnp.exp(-(lro + lx)))
    same_f = jnp.where((iota((128, 128), 0) < HEAD) == (iota((128, 128), 1) < HEAD), 1.0, 0.0)
    ones = same_f.astype(BF)
    kk = split(k * k)
    unit = k * lax.rsqrt(dot(kk[0], ones) + dot(kk[1], ones) + 1e-06)
    rate = lrate * unit
    row, col = iota((C, 128), 0), iota((C, 128), 1) & (C - 1)
    lower = row > col
    lower_eq = row >= col
    unit_packed = jnp.where(row == col, 1.0, 0.0)
    tri = jnp.where(iota((C, C), 0) >= iota((C, C), 1), 1.0, 0.0).astype(BF)
    eye = jnp.where(iota((128, 128), 0) == iota((128, 128), 1), 1.0, 0.0)
    levels = [((row >> n) == (col >> n) + 1) & (((row >> n) & 1) == 1) for n in range(6)]
    at = [slice(c * C, (c + 1) * C) for c in chunks]

    def each(f, *lists):
        return [f(*args) for args in zip(*lists)]

    def summed(lw):
        w0 = lw.astype(BF)
        w1, w2 = split(lw - w0.astype(F32))
        return dot(tri, w0) + (dot(tri, w1) + dot(tri, w2))

    lws = [log_decay[a] for a in at]
    cums = each(summed, lws)
    mids = [cum[C // 2 - 1 : C // 2] for cum in cums]
    ends = [cum[C - 1 : C] for cum in cums]
    falls = each(lambda cum, mid: jnp.exp(mid - cum), cums, mids)
    pcs = each(lambda cum, lw, mid, a: jnp.exp(cum - lw - mid) * unit[a], cums, lws, mids, at)
    ucs = each(lambda cum, mid, a: jnp.exp(cum - mid) * q[a], cums, mids, at)
    rcs = each(lambda fall, a: fall * rate[a], falls, at)
    gcs = each(lambda fall, a: fall * k[a], falls, at)

    def pairs(pc, uc, rc, gc):
        left = split(jnp.concatenate([pc, uc], axis=0))
        rs, gs = stacked(split(rc), masks), stacked(split(gc), masks)
        right = tuple(jnp.concatenate([a, b], axis=0) for a, b in zip(rs, gs))
        return mm(left, right, dot_t)

    pair = each(pairs, pcs, ucs, rcs, gcs)
    arps = [jnp.where(lower, p[:C, :128], 0.0) for p in pair]
    burs = [jnp.where(lower_eq, p[C:, :128], 0.0) for p in pair]

    def values_read(p, a):
        ab = split(
            jnp.concatenate(
                [jnp.where(lower, p[:C, 128:], 0.0), jnp.where(lower_eq, p[C:, 128:], 0.0)], axis=0
            )
        )
        vs = stacked((v[a].astype(BF),), masks)[0]
        return dot(ab[0], vs) + dot(ab[1], vs)

    abvs = each(values_read, pair, at)
    invs = [unit_packed - jnp.where(levels[0], arp, 0.0) for arp in arps]
    for n in range(1, 6):
        ss = each(split, invs)
        ts = each(
            lambda arp, s: mm(split(jnp.where(levels[n], arp, 0.0)), stacked(s, masks)), arps, ss
        )
        invs = each(lambda inv, s, t: inv - mm(s, stacked(split(t), masks)), invs, ss, ts)
    to_mids = each(jnp.exp, mids)
    wys = each(
        lambda inv, pc, to_mid, abv: split(
            mm(
                split(inv),
                stacked(split(jnp.concatenate([pc * to_mid, abv[:C]], axis=1)), masks2),
            )
        ),
        invs,
        pcs,
        to_mids,
        abvs,
    )
    bwys = each(lambda bur, wy: mm(split(bur), stacked(wy, masks2)), burs, wys)
    ueffs = each(lambda uc, to_mid, bwy: split(uc * to_mid - bwy[:, :128]), ucs, to_mids, bwys)
    own = each(lambda abv, bwy: abv[C:] - bwy[:, 128:], abvs, bwys)

    def change(rc, gc, mid, end, wy, a):
        rest = jnp.exp(end - mid)
        rwy = mm(split((rc * rest).T), wy)
        gs = split((gc * rest).T)
        vb = v[a].astype(BF)
        gv = dot(gs[0], vb) + dot(gs[1], vb)
        return split(eye * jnp.exp(end) - same_f * rwy[:, :128]), same_f * (gv - rwy[:, 128:])

    changes = each(change, rcs, gcs, mids, ends, wys, at)
    reads, owns = [], []
    both = jnp.concatenate([eye, jnp.zeros((128, 128), F32)], axis=1)
    for c in chunks:
        bs = split(both)
        out = mm(ueffs[c], bs)
        reads.append(out[:, :128])
        owns.append(own[c] + out[:, 128:])
        trans, state = changes[c]
        both = mm(trans, bs)
        both = jnp.concatenate([both[:, :128], both[:, 128:] + state], axis=1)
    total = jnp.concatenate(
        [both[:HEAD, :128] + both[HEAD:, :128], both[:HEAD, 128:] + both[HEAD:, 128:]], axis=0
    )
    return jnp.concatenate(reads, axis=0), jnp.concatenate(owns, axis=0), total


def local_kernel(resid, core_rows, q, k, v, dx, lx, dco, lro, extra, *refs):
    reads_out, owns_out, rows, total, reads, owns, sems = refs
    rows[0] = resid[...]
    rows[1] = core_rows[...]
    f = lambda r: r[...].astype(F32)
    a, b, t = local_scan(f(q), f(k), f(v), f(dx), f(lx), dco[...], lro[...], extra[...].T)
    reads[...] = a
    owns[...] = b
    stores = [
        pltpu.make_async_copy(reads, reads_out, sems.at[0]),
        pltpu.make_async_copy(owns, owns_out, sems.at[1]),
    ]
    for copy in stores:
        copy.start()
    out = sent(t[:HEAD], t[HEAD:])
    for d in range(total.shape[0]):
        total[d] = out
    for copy in stores:
        copy.wait()


def finish(reads, owns, state, gain):
    masks = head_masks()
    out = owns + mm(split(reads), stacked(split(state), masks))
    same = (iota((128, 128), 0) < HEAD) == (iota((128, 128), 1) < HEAD)
    mean = jnp.where(same, 1.0 / HEAD, 0.0).astype(BF)
    s = split(out)
    center = out - (dot(s[0], mean) + dot(s[1], mean))
    s = split(center * center)
    spread = dot(s[0], mean) + dot(s[1], mean)
    return (center * lax.rsqrt(spread + 1e-05) * gain).astype(BF)


def fold(level, masks2):
    while len(level) > 1:
        nxt = []
        for i in range(0, len(level) - 1, 2):
            (t1, x1), (t2, x2) = level[i], level[i + 1]
            both = jnp.concatenate([t1, x1], axis=1)
            out = mm(split(t2), stacked(split(both), masks2))
            nxt.append((out[:, :128], out[:, 128:] + x2))
        if len(level) % 2:
            nxt.append(level[-1])
        level = nxt
    return level[0]


def eye_packed():
    return jnp.where(iota((HEAD, 128), 0) == (iota((HEAD, 128), 1) & (HEAD - 1)), 1.0, 0.0)


def piece(pieces, d):
    p = pieces[d].astype(F32)
    return p[:HEAD], p[HEAD:]


def sent(trans, state):
    return jnp.concatenate([trans - eye_packed(), state], axis=0).astype(BF)


def earlier(pieces, count, index, masks2):
    level = []
    for d in range(count - 1):
        used = jnp.where(d < index, 1.0, 0.0)
        trans, state = piece(pieces, d)
        level.append((trans * used + eye_packed(), state * used))
    return fold(level, masks2)


def group_kernel(index, pieces, total, inside):
    masks2 = head_masks(256)
    level = [piece(pieces, d) for d in range(4)]
    t, x = fold([(t + eye_packed(), x) for t, x in level], masks2)
    out = sent(t, x)
    for d in range(total.shape[0]):
        total[d] = out
    t, x = earlier(pieces, 4, index[0], masks2)
    inside[...] = jnp.concatenate([t, x], axis=0)


def pack_kernel(gate, up, down, a, b):
    cols = gate.shape[1]
    cut = a.shape[2] - cols
    for n in range(a.shape[0]):
        a[n, :, :cols] = gate[...]
        a[n, :, cols:] = up[:, :cut]
    b[:, : cols - cut] = up[:, cut:]
    b[:, cols - cut :] = down[...]


def stackb_kernel(index, *refs):
    out = refs[8]
    for r in range(8):
        out[(index[2] + r) % 8] = refs[r][...]


def finish_kernel(index, pieces, inside, reads, owns, gain, mixed):
    _, x = earlier(pieces, pieces.shape[0], index[0], head_masks(256))
    t = inside[...]
    state = mm(split(t[:HEAD]), stacked(split(x), head_masks())) + t[HEAD:]
    out = finish(reads[...], owns[...], state, gain[...])
    rows = out.shape[0] // 8
    core = index[1]
    parts = [[out[(2 * y + c) * rows : (2 * y + c + 1) * rows] for y in range(4)] for c in range(2)]
    for d in range(4):
        for y in range(4):
            for c in range(2):
                at = y * rows + (c ^ core) * (4 * rows)
                mixed[d, pl.ds(pl.multiple_of(at, 16), rows)] = parts[c][y]


def proj_kernel(index, own, sib, r0, r1, r2, r3, weight, gain, mid, normed, resid, w, sems):
    core = index[1]
    loads = [
        pltpu.make_async_copy(
            weight.at[pl.ds(pl.multiple_of((2 * y + (c ^ core)) * 128, 128), 128)],
            w.at[pl.ds((4 * c + y) * 128, 128)],
            sems.at[4 * c + y],
        )
        for c in range(2)
        for y in range(4)
    ]
    for copy in loads:
        copy.start()
    for s, r in enumerate((r0, r1, r2, r3)):
        for n in range(2):
            resid[n, (index[4] + 4 - s) % 4] = r[n]
    half = own.shape[1] // 2
    sums = []
    for copy in loads[:4]:
        copy.wait()
    for n in range(2):
        left = jnp.concatenate([own[y, n * half : (n + 1) * half] for y in range(4)], axis=1)
        sums.append(dot(left, w[:512]))
    for copy in loads[4:]:
        copy.wait()
    for n in range(2):
        left = jnp.concatenate([sib[y, (1 - n) * half : (2 - n) * half] for y in range(4)], axis=1)
        rows = resid.shape[2]
        m = jnp.concatenate([resid[n, y] for y in range(4)], axis=0).astype(F32)
        m = m + (sums[n] + dot(left, w[512:]))
        m = m.astype(BF)
        if n == 0:
            for y in range(4):
                mid[y] = m[y * rows : (y + 1) * rows]
        m = m.astype(F32)
        scale = lax.rsqrt(jnp.mean(m * m, axis=-1, keepdims=True) + 1e-06)
        m = (m * scale * gain[...]).astype(BF)
        for k in range(8):
            normed[k, n * half : (n + 1) * half] = m[:, k * 256 : (k + 1) * 256]


def ffn_kernel(index, normed, *refs):
    a, b, (keep, send, wa, wb, sems) = refs[:8], refs[8:12], refs[12:]
    z, x = index[2], index[3]
    na, nb = wa.shape[3], wb.shape[3]
    cols = (na + nb) // 3
    tail = 2 * cols - na
    order = (0, 1, 7, 2, 6, 3, 5, 4)
    loads = [pltpu.make_async_copy(a[r], wa.at[n], sems.at[n]) for n, r in enumerate(order)]
    later = [
        pltpu.make_async_copy(b[s], wb.at[:, (x + 4 - s) % 4], sems.at[8 + s]) for s in range(4)
    ]
    for copy in loads + later:
        copy.start()
    both = None
    for first, last in ((0, 3), (3, 6), (6, 8)):
        for copy in loads[first:last]:
            copy.wait()
        left = jnp.concatenate([normed[(z + r) % 8] for r in order[first:last]], axis=1)
        part = dot(left, wa[first:last].reshape(-1, na))
        both = part if both is None else both + part
    for copy in later:
        copy.wait()
    left = jnp.concatenate([normed[k] for k in range(8)], axis=1)
    rest = dot(left, wb[:, :, :, :tail].reshape(-1, tail))
    both = jnp.concatenate([both, rest], axis=1)
    gate = both[:, :cols]
    hidden = (gate * (1.0 / (1.0 + jnp.exp(-gate))) * both[:, cols:]).astype(BF)
    half, rows = hidden.shape[0] // 2, hidden.shape[0] // 8
    for k in range(8):
        out = dot_t(hidden, wb[k, :, :, tail:].reshape(-1, cols)).astype(BF)
        for y in range(4):
            keep[y, k] = out[y * rows : (y + 1) * rows]
            send[y, k] = out[half + y * rows : half + (y + 1) * rows]


def final_kernel(index, pieces, mid, result):
    m = mid[index[4]].astype(F32)
    for k in range(8):
        total = pieces[0, k].astype(F32)
        for y in range(1, 4):
            total = total + pieces[y, k].astype(F32)
        at = slice(k * 256, (k + 1) * 256)
        result[:, at] = (m[:, at] + 0.5 * total).astype(BF)


def vmem(n):
    return [pl.BlockSpec(memory_space=pltpu.VMEM)] * n


SMEM = pl.BlockSpec(memory_space=pltpu.SMEM)
ANY = pl.BlockSpec(memory_space=pl.ANY)
HBM = pl.BlockSpec(memory_space=pltpu.MemorySpace.HBM)
shape = jax.ShapeDtypeStruct


def call(kernel, name, out, in_specs, us, mib=16, scratch=(), space=None):
    def run(*args):
        return pl.pallas_call(
            kernel,
            out_shape=out,
            in_specs=in_specs,
            out_specs=space
            if isinstance(space, tuple)
            else jax.tree.map(lambda _: space or vmem(1)[0], out),
            scratch_shapes=scratch,
            compiler_params=pltpu.CompilerParams(vmem_limit_bytes=LIMIT.get(name, mib << 20)),
            cost_estimate=pl.CostEstimate(
                flops=int(us * FLOPS_US), bytes_accessed=0, transcendentals=0
            ),
        )(*args)

    return run


FLOPS_US = 1e8
LIMIT = {"pack": None, "local": None, "finish": 56 << 20, "group": 16 << 20}
NA = 1152


def per_device(
    resid,
    queries,
    keys,
    values,
    decay_input_part,
    decay_channel_offset,
    decay_head_extra,
    correction_rate_input,
    correction_rate_offset,
    head_norm_gain,
    mixer_output_weight,
    feedforward_norm_gain,
    gate_weight,
    up_weight,
    down_weight,
):
    tok, cols = queries.shape[0], gate_weight.shape[1]
    z, x, y, c = (lax.axis_index(a).astype(jnp.int32) for a in ("z", "x", "y", "c"))
    index = jnp.stack([z, c, z, x, y])

    def exchanged(array, axis):
        return lax.all_to_all(array, axis, split_axis=0, concat_axis=0, tiled=True)

    def shifted(array, axis, by):
        n = lax.axis_size(axis)
        return lax.ppermute(array, axis, [(i, (i + by) % n) for i in range(n)])

    part_a, part_b = call(
        pack_kernel,
        "pack",
        (shape((4, 64, NA), BF), shape((64, 3 * cols - NA), BF)),
        vmem(3),
        1,
        8,
    )(gate_weight, up_weight, down_weight.T)
    down_up = down_dn = part_b
    found_b = {0: part_b}
    for s in range(1, 5):
        found_b[8 - s] = down_up = shifted(down_up, "z", 1)
        if s < 4:
            found_b[s] = down_dn = shifted(down_dn, "z", -1)
    first = exchanged(part_a, "x")
    core_rows = shifted(resid, "c", 1)
    stack = call(
        stackb_kernel,
        "stackb",
        shape((8, *part_b.shape), BF),
        [SMEM] + vmem(8),
        1,
        8,
    )(index, *[found_b[r] for r in range(8)])
    found = {0: first}
    up = down = first
    for s in range(1, 5):
        found[8 - s] = up = shifted(up, "z", 1)
        if s < 4:
            found[s] = down = shifted(down, "z", -1)
    pieces_b = [stack] + [shifted(stack, "x", s) for s in range(1, 4)]

    reads, owns, rows, total = call(
        local_kernel,
        "local",
        (
            shape((tok, 128), F32),
            shape((tok, 128), F32),
            shape((2, *resid.shape), BF),
            shape((4, 128, 128), BF),
        ),
        vmem(10),
        6,
        24,
        [
            pltpu.VMEM((tok, 128), F32),
            pltpu.VMEM((tok, 128), F32),
            pltpu.SemaphoreType.DMA((2,)),
        ],
        (HBM, HBM, vmem(1)[0], vmem(1)[0]),
    )(
        resid,
        core_rows,
        queries,
        keys,
        values,
        decay_input_part,
        correction_rate_input,
        decay_channel_offset[None],
        correction_rate_offset[None],
        decay_head_extra.T,
    )
    rows = [rows] + [shifted(rows, "y", s) for s in range(1, 4)]
    near = exchanged(total, "x")
    total, inside = call(
        group_kernel,
        "group",
        (shape((8, 128, 128), BF), shape((128, 128), F32)),
        [SMEM] + vmem(1),
        1,
    )(x[None], near)
    far = exchanged(total, "z")
    mixed = call(finish_kernel, "finish", shape((4, tok, 128), BF), [SMEM] + vmem(5), 3)(
        jnp.stack([z, c]), far, inside, reads, owns, head_norm_gain[None]
    )
    mixed_own = exchanged(mixed, "y")
    mixed_sib = shifted(mixed_own, "c", 1)
    mid, normed = call(
        proj_kernel,
        "proj",
        (shape((4, tok // 8, 2048), BF), shape((8, tok, 256), BF)),
        [SMEM] + vmem(6) + [ANY] + vmem(1),
        3,
        48,
        [
            pltpu.VMEM((2, 4, tok // 8, 2048), BF),
            pltpu.VMEM((1024, 2048), BF),
            pltpu.SemaphoreType.DMA((8,)),
        ],
    )(
        index,
        mixed_own,
        mixed_sib,
        *rows,
        mixer_output_weight,
        feedforward_norm_gain[None],
    )
    part = shape((4, 8, tok // 8, 256), BF)
    keep, send = call(
        ffn_kernel,
        "ffn",
        (part, part),
        [SMEM] + vmem(1) + [ANY] * 12,
        7,
        32,
        [
            pltpu.VMEM((8, 4, 64, NA), BF),
            pltpu.VMEM((8, 4, 64, 3 * cols - NA), BF),
            pltpu.SemaphoreType.DMA((12,)),
        ],
    )(index, normed, *[found[r] for r in range(8)], *pieces_b)
    pair = (keep.astype(F32) + shifted(send, "c", 1).astype(F32)).astype(BF)
    return call(final_kernel, "final", shape((tok // 8, 2048), BF), [SMEM] + vmem(2), 1)(
        index, exchanged(pair, "y"), mid
    )


def solution(mesh):
    torus = Mesh(mesh.devices.reshape(8, 4, 4, 2), ("z", "x", "y", "c"))
    sp, tp = ("z", "x"), ("y", "c")
    in_specs = (
        P(sp + tp, None),
        P(sp, tp),
        P(sp, tp),
        P(sp, tp),
        P(sp, tp),
        P(tp),
        P(sp, tp),
        P(sp, tp),
        P(tp),
        P(tp),
        P(),
        P(),
        P(sp, tp),
        P(sp, tp),
        P(tp, sp),
    )

    return jax.shard_map(
        per_device, mesh=torus, in_specs=in_specs, out_specs=P(sp + tp, None), check_vma=False
    )
```

```python
import jax
import jax.numpy as jnp
from jax import lax
from jax.experimental import pallas as pl
from jax.experimental.pallas import tpu as pltpu
from jax.sharding import Mesh
from jax.sharding import PartitionSpec as P

HEAD = 64
C = 64
BF = jnp.bfloat16
F32 = jnp.float32


def split(x):
    hi = x.astype(BF)
    return hi, (x - hi.astype(F32)).astype(BF)


def dot(a, b):
    return lax.dot_general(a, b, (((1,), (0,)), ((), ())), preferred_element_type=F32)


def dot_t(a, b):
    return lax.dot_general(a, b, (((1,), (1,)), ((), ())), preferred_element_type=F32)


def mm(x, y, f=dot):
    return f(x[0], y[0]) + (f(x[0], y[1]) + f(x[1], y[0]))


def iota(shape, dim):
    return lax.broadcasted_iota(jnp.int32, shape, dim)


def head_masks(width=128):
    first = (iota((1, width), 1) & 127) < HEAD
    m0 = jnp.where(first, 1.0, 0.0)
    return m0.astype(BF), (1.0 - m0).astype(BF)


def stacked(y, masks):
    return tuple(jnp.concatenate([p * masks[0], p * masks[1]], axis=0) for p in y)


def local_scan(q, k, v, dx, lx, dco, lro, extra):
    chunks = range(q.shape[0] // C)
    first = iota((1, 128), 1) < HEAD
    masks, masks2 = head_masks(), head_masks(256)
    ext = jnp.where(first, extra[:, 0:1], extra[:, 1:2])
    log_decay = -0.6065306597126334 * (1.0 / (1.0 + jnp.exp(-(dco + dx)))) - ext
    lrate = 1.0 / (1.0 + jnp.exp(-(lro + lx)))
    same_f = jnp.where((iota((128, 128), 0) < HEAD) == (iota((128, 128), 1) < HEAD), 1.0, 0.0)
    ones = same_f.astype(BF)
    kk = split(k * k)
    unit = k * lax.rsqrt(dot(kk[0], ones) + dot(kk[1], ones) + 1e-06)
    rate = lrate * unit
    row, col = iota((C, 128), 0), iota((C, 128), 1) & (C - 1)
    lower = row > col
    lower_eq = row >= col
    unit_packed = jnp.where(row == col, 1.0, 0.0)
    tri = jnp.where(iota((C, C), 0) >= iota((C, C), 1), 1.0, 0.0).astype(BF)
    eye = jnp.where(iota((128, 128), 0) == iota((128, 128), 1), 1.0, 0.0)
    levels = [((row >> n) == (col >> n) + 1) & (((row >> n) & 1) == 1) for n in range(6)]
    at = [slice(c * C, (c + 1) * C) for c in chunks]

    def each(f, *lists):
        return [f(*args) for args in zip(*lists)]

    def summed(lw):
        w0 = lw.astype(BF)
        w1, w2 = split(lw - w0.astype(F32))
        return dot(tri, w0) + (dot(tri, w1) + dot(tri, w2))

    lws = [log_decay[a] for a in at]
    cums = each(summed, lws)
    mids = [cum[C // 2 - 1 : C // 2] for cum in cums]
    ends = [cum[C - 1 : C] for cum in cums]
    falls = each(lambda cum, mid: jnp.exp(mid - cum), cums, mids)
    pcs = each(lambda cum, lw, mid, a: jnp.exp(cum - lw - mid) * unit[a], cums, lws, mids, at)
    ucs = each(lambda cum, mid, a: jnp.exp(cum - mid) * q[a], cums, mids, at)
    rcs = each(lambda fall, a: fall * rate[a], falls, at)
    gcs = each(lambda fall, a: fall * k[a], falls, at)

    def pairs(pc, uc, rc, gc):
        left = split(jnp.concatenate([pc, uc], axis=0))
        rs, gs = stacked(split(rc), masks), stacked(split(gc), masks)
        right = tuple(jnp.concatenate([a, b], axis=0) for a, b in zip(rs, gs))
        return mm(left, right, dot_t)

    pair = each(pairs, pcs, ucs, rcs, gcs)
    arps = [jnp.where(lower, p[:C, :128], 0.0) for p in pair]
    burs = [jnp.where(lower_eq, p[C:, :128], 0.0) for p in pair]

    def values_read(p, a):
        ab = split(
            jnp.concatenate(
                [jnp.where(lower, p[:C, 128:], 0.0), jnp.where(lower_eq, p[C:, 128:], 0.0)], axis=0
            )
        )
        vs = stacked((v[a].astype(BF),), masks)[0]
        return dot(ab[0], vs) + dot(ab[1], vs)

    abvs = each(values_read, pair, at)
    invs = [unit_packed - jnp.where(levels[0], arp, 0.0) for arp in arps]
    for n in range(1, 6):
        ss = each(split, invs)
        ts = each(
            lambda arp, s: mm(split(jnp.where(levels[n], arp, 0.0)), stacked(s, masks)), arps, ss
        )
        invs = each(lambda inv, s, t: inv - mm(s, stacked(split(t), masks)), invs, ss, ts)
    to_mids = each(jnp.exp, mids)
    wys = each(
        lambda inv, pc, to_mid, abv: split(
            mm(
                split(inv),
                stacked(split(jnp.concatenate([pc * to_mid, abv[:C]], axis=1)), masks2),
            )
        ),
        invs,
        pcs,
        to_mids,
        abvs,
    )
    bwys = each(lambda bur, wy: mm(split(bur), stacked(wy, masks2)), burs, wys)
    ueffs = each(lambda uc, to_mid, bwy: split(uc * to_mid - bwy[:, :128]), ucs, to_mids, bwys)
    own = each(lambda abv, bwy: abv[C:] - bwy[:, 128:], abvs, bwys)

    def change(rc, gc, mid, end, wy, a):
        rest = jnp.exp(end - mid)
        rwy = mm(split((rc * rest).T), wy)
        gs = split((gc * rest).T)
        vb = v[a].astype(BF)
        gv = dot(gs[0], vb) + dot(gs[1], vb)
        return split(eye * jnp.exp(end) - same_f * rwy[:, :128]), same_f * (gv - rwy[:, 128:])

    changes = each(change, rcs, gcs, mids, ends, wys, at)
    reads, owns = [], []
    both = jnp.concatenate([eye, jnp.zeros((128, 128), F32)], axis=1)
    for c in chunks:
        bs = split(both)
        out = mm(ueffs[c], bs)
        reads.append(out[:, :128])
        owns.append(own[c] + out[:, 128:])
        trans, state = changes[c]
        both = mm(trans, bs)
        both = jnp.concatenate([both[:, :128], both[:, 128:] + state], axis=1)
    total = jnp.concatenate(
        [both[:HEAD, :128] + both[HEAD:, :128], both[:HEAD, 128:] + both[HEAD:, 128:]], axis=0
    )
    return jnp.concatenate(reads, axis=0), jnp.concatenate(owns, axis=0), total


def local_kernel(resid, core_rows, q, k, v, dx, lx, dco, lro, extra, *refs):
    reads_out, owns_out, rows, total, reads, owns, sems = refs
    rows[0] = resid[...]
    rows[1] = core_rows[...]
    f = lambda r: r[...].astype(F32)
    a, b, t = local_scan(f(q), f(k), f(v), f(dx), f(lx), dco[...], lro[...], extra[...].T)
    reads[...] = a
    owns[...] = b
    stores = [
        pltpu.make_async_copy(reads, reads_out, sems.at[0]),
        pltpu.make_async_copy(owns, owns_out, sems.at[1]),
    ]
    for copy in stores:
        copy.start()
    out = sent(t[:HEAD], t[HEAD:])
    for d in range(total.shape[0]):
        total[d] = out
    for copy in stores:
        copy.wait()


def finish(reads, owns, state, gain):
    masks = head_masks()
    out = owns + mm(split(reads), stacked(split(state), masks))
    same = (iota((128, 128), 0) < HEAD) == (iota((128, 128), 1) < HEAD)
    mean = jnp.where(same, 1.0 / HEAD, 0.0).astype(BF)
    s = split(out)
    center = out - (dot(s[0], mean) + dot(s[1], mean))
    s = split(center * center)
    spread = dot(s[0], mean) + dot(s[1], mean)
    return (center * lax.rsqrt(spread + 1e-05) * gain).astype(BF)


def fold(level, masks2):
    while len(level) > 1:
        nxt = []
        for i in range(0, len(level) - 1, 2):
            (t1, x1), (t2, x2) = level[i], level[i + 1]
            both = jnp.concatenate([t1, x1], axis=1)
            out = mm(split(t2), stacked(split(both), masks2))
            nxt.append((out[:, :128], out[:, 128:] + x2))
        if len(level) % 2:
            nxt.append(level[-1])
        level = nxt
    return level[0]


def eye_packed():
    return jnp.where(iota((HEAD, 128), 0) == (iota((HEAD, 128), 1) & (HEAD - 1)), 1.0, 0.0)


def piece(pieces, d):
    p = pieces[d].astype(F32)
    return p[:HEAD], p[HEAD:]


def sent(trans, state):
    return jnp.concatenate([trans - eye_packed(), state], axis=0).astype(BF)


def earlier(pieces, count, index, masks2):
    level = []
    for d in range(count - 1):
        used = jnp.where(d < index, 1.0, 0.0)
        trans, state = piece(pieces, d)
        level.append((trans * used + eye_packed(), state * used))
    return fold(level, masks2)


def group_kernel(index, pieces, total, inside):
    masks2 = head_masks(256)
    level = [piece(pieces, d) for d in range(4)]
    t, x = fold([(t + eye_packed(), x) for t, x in level], masks2)
    out = sent(t, x)
    for d in range(total.shape[0]):
        total[d] = out
    t, x = earlier(pieces, 4, index[0], masks2)
    inside[...] = jnp.concatenate([t, x], axis=0)


def pack_kernel(gate, up, down, a, b):
    cols = gate.shape[1]
    cut = a.shape[2] - cols
    for n in range(a.shape[0]):
        a[n, :, :cols] = gate[...]
        a[n, :, cols:] = up[:, :cut]
    b[:, : cols - cut] = up[:, cut:]
    b[:, cols - cut :] = down[...]


def stackb_kernel(index, *refs):
    out = refs[8]
    for r in range(8):
        out[(index[2] + r) % 8] = refs[r][...]


def finish_kernel(index, pieces, inside, reads, owns, gain, mixed):
    _, x = earlier(pieces, pieces.shape[0], index[0], head_masks(256))
    t = inside[...]
    state = mm(split(t[:HEAD]), stacked(split(x), head_masks())) + t[HEAD:]
    out = finish(reads[...], owns[...], state, gain[...])
    rows = out.shape[0] // 8
    core = index[1]
    parts = [[out[(2 * y + c) * rows : (2 * y + c + 1) * rows] for y in range(4)] for c in range(2)]
    for d in range(4):
        for y in range(4):
            for c in range(2):
                at = y * rows + (c ^ core) * (4 * rows)
                mixed[d, pl.ds(pl.multiple_of(at, 16), rows)] = parts[c][y]


def proj_kernel(index, own, sib, r0, r1, r2, r3, weight, gain, mid, normed, resid, w, sems):
    core = index[1]
    loads = [
        pltpu.make_async_copy(
            weight.at[pl.ds(pl.multiple_of((2 * y + (c ^ core)) * 128, 128), 128)],
            w.at[pl.ds((4 * c + y) * 128, 128)],
            sems.at[4 * c + y],
        )
        for c in range(2)
        for y in range(4)
    ]
    for copy in loads:
        copy.start()
    for s, r in enumerate((r0, r1, r2, r3)):
        for n in range(2):
            resid[n, (index[4] + 4 - s) % 4] = r[n]
    half = own.shape[1] // 2
    sums = []
    for copy in loads[:4]:
        copy.wait()
    for n in range(2):
        left = jnp.concatenate([own[y, n * half : (n + 1) * half] for y in range(4)], axis=1)
        sums.append(dot(left, w[:512]))
    for copy in loads[4:]:
        copy.wait()
    for n in range(2):
        left = jnp.concatenate([sib[y, (1 - n) * half : (2 - n) * half] for y in range(4)], axis=1)
        rows = resid.shape[2]
        m = jnp.concatenate([resid[n, y] for y in range(4)], axis=0).astype(F32)
        m = m + (sums[n] + dot(left, w[512:]))
        m = m.astype(BF)
        if n == 0:
            for y in range(4):
                mid[y] = m[y * rows : (y + 1) * rows]
        m = m.astype(F32)
        scale = lax.rsqrt(jnp.mean(m * m, axis=-1, keepdims=True) + 1e-06)
        m = (m * scale * gain[...]).astype(BF)
        for k in range(8):
            normed[k, n * half : (n + 1) * half] = m[:, k * 256 : (k + 1) * 256]


def ffn_kernel(index, normed, *refs):
    a, b, (keep, send, wa, wb, sems) = refs[:8], refs[8:12], refs[12:]
    z, x = index[2], index[3]
    na, nb = wa.shape[3], wb.shape[3]
    cols = (na + nb) // 3
    tail = 2 * cols - na
    order = (0, 1, 7, 2, 6, 3, 5, 4)
    loads = [pltpu.make_async_copy(a[r], wa.at[n], sems.at[n]) for n, r in enumerate(order)]
    later = [
        pltpu.make_async_copy(b[s], wb.at[:, (x + 4 - s) % 4], sems.at[8 + s]) for s in range(4)
    ]
    for copy in loads + later:
        copy.start()
    both = None
    for first, last in ((0, 3), (3, 6), (6, 8)):
        for copy in loads[first:last]:
            copy.wait()
        left = jnp.concatenate([normed[(z + r) % 8] for r in order[first:last]], axis=1)
        part = dot(left, wa[first:last].reshape(-1, na))
        both = part if both is None else both + part
    for copy in later:
        copy.wait()
    left = jnp.concatenate([normed[k] for k in range(8)], axis=1)
    rest = dot(left, wb[:, :, :, :tail].reshape(-1, tail))
    both = jnp.concatenate([both, rest], axis=1)
    gate = both[:, :cols]
    hidden = (gate * (1.0 / (1.0 + jnp.exp(-gate))) * both[:, cols:]).astype(BF)
    half, rows = hidden.shape[0] // 2, hidden.shape[0] // 8
    for k in range(8):
        out = dot_t(hidden, wb[k, :, :, tail:].reshape(-1, cols)).astype(BF)
        for y in range(4):
            keep[y, k] = out[y * rows : (y + 1) * rows]
            send[y, k] = out[half + y * rows : half + (y + 1) * rows]


def pair_kernel(index, keep, other, out0, out1, out2, out3):
    for d, out in enumerate((out0, out1, out2, out3)):
        at = (index[4] + d) % 4
        out[...] = (keep[at].astype(F32) + other[at].astype(F32)).astype(out.dtype)


def final_kernel(index, own, near1, near2, near3, mid, result):
    m = mid[index[4]].astype(F32)
    for k in range(8):
        total = own[k] + (near1[k].astype(F32) + near2[k].astype(F32)) + near3[k].astype(F32)
        at = slice(k * 256, (k + 1) * 256)
        result[:, at] = (m[:, at] + 0.5 * total).astype(BF)


def vmem(n):
    return [pl.BlockSpec(memory_space=pltpu.VMEM)] * n


SMEM = pl.BlockSpec(memory_space=pltpu.SMEM)
ANY = pl.BlockSpec(memory_space=pl.ANY)
HBM = pl.BlockSpec(memory_space=pltpu.MemorySpace.HBM)
shape = jax.ShapeDtypeStruct


def call(kernel, name, out, in_specs, us, mib=16, scratch=(), space=None):
    def run(*args):
        return pl.pallas_call(
            kernel,
            out_shape=out,
            in_specs=in_specs,
            out_specs=space
            if isinstance(space, tuple)
            else jax.tree.map(lambda _: space or vmem(1)[0], out),
            scratch_shapes=scratch,
            compiler_params=pltpu.CompilerParams(vmem_limit_bytes=LIMIT.get(name, mib << 20)),
            cost_estimate=pl.CostEstimate(
                flops=int(us * FLOPS_US), bytes_accessed=0, transcendentals=0
            ),
        )(*args)

    return run


FLOPS_US = 1e8
LIMIT = {"pack": None, "local": None, "finish": 56 << 20, "group": 16 << 20}
NA = 1280


def per_device(
    resid,
    queries,
    keys,
    values,
    decay_input_part,
    decay_channel_offset,
    decay_head_extra,
    correction_rate_input,
    correction_rate_offset,
    head_norm_gain,
    mixer_output_weight,
    feedforward_norm_gain,
    gate_weight,
    up_weight,
    down_weight,
):
    tok, cols = queries.shape[0], gate_weight.shape[1]
    z, x, y, c = (lax.axis_index(a).astype(jnp.int32) for a in ("z", "x", "y", "c"))
    index = jnp.stack([z, c, z, x, y])

    def exchanged(array, axis):
        return lax.all_to_all(array, axis, split_axis=0, concat_axis=0, tiled=True)

    def shifted(array, axis, by):
        n = lax.axis_size(axis)
        return lax.ppermute(array, axis, [(i, (i + by) % n) for i in range(n)])

    part_a, part_b = call(
        pack_kernel,
        "pack",
        (shape((4, 64, NA), BF), shape((64, 3 * cols - NA), BF)),
        vmem(3),
        1,
        8,
    )(gate_weight, up_weight, down_weight.T)
    down_up = down_dn = part_b
    found_b = {0: part_b}
    for s in range(1, 5):
        found_b[8 - s] = down_up = shifted(down_up, "z", 1)
        if s < 4:
            found_b[s] = down_dn = shifted(down_dn, "z", -1)
    first = exchanged(part_a, "x")
    core_rows = shifted(resid, "c", 1)
    stack = call(
        stackb_kernel,
        "stackb",
        shape((8, *part_b.shape), BF),
        [SMEM] + vmem(8),
        1,
        8,
    )(index, *[found_b[r] for r in range(8)])
    found = {0: first}
    up = down = first
    for s in range(1, 5):
        found[8 - s] = up = shifted(up, "z", 1)
        if s < 4:
            found[s] = down = shifted(down, "z", -1)
    pieces_b = [stack] + [shifted(stack, "x", s) for s in range(1, 4)]

    reads, owns, rows, total = call(
        local_kernel,
        "local",
        (
            shape((tok, 128), F32),
            shape((tok, 128), F32),
            shape((2, *resid.shape), BF),
            shape((4, 128, 128), BF),
        ),
        vmem(10),
        6,
        24,
        [
            pltpu.VMEM((tok, 128), F32),
            pltpu.VMEM((tok, 128), F32),
            pltpu.SemaphoreType.DMA((2,)),
        ],
        (HBM, HBM, vmem(1)[0], vmem(1)[0]),
    )(
        resid,
        core_rows,
        queries,
        keys,
        values,
        decay_input_part,
        correction_rate_input,
        decay_channel_offset[None],
        correction_rate_offset[None],
        decay_head_extra.T,
    )
    rows = [rows] + [shifted(rows, "y", s) for s in range(1, 4)]
    near = exchanged(total, "x")
    total, inside = call(
        group_kernel,
        "group",
        (shape((8, 128, 128), BF), shape((128, 128), F32)),
        [SMEM] + vmem(1),
        1,
    )(x[None], near)
    far = exchanged(total, "z")
    mixed = call(finish_kernel, "finish", shape((4, tok, 128), BF), [SMEM] + vmem(5), 3)(
        jnp.stack([z, c]), far, inside, reads, owns, head_norm_gain[None]
    )
    mixed_own = exchanged(mixed, "y")
    mixed_sib = shifted(mixed_own, "c", 1)
    mid, normed = call(
        proj_kernel,
        "proj",
        (shape((4, tok // 8, 2048), BF), shape((8, tok, 256), BF)),
        [SMEM] + vmem(6) + [ANY] + vmem(1),
        3,
        48,
        [
            pltpu.VMEM((2, 4, tok // 8, 2048), BF),
            pltpu.VMEM((1024, 2048), BF),
            pltpu.SemaphoreType.DMA((8,)),
        ],
    )(
        index,
        mixed_own,
        mixed_sib,
        *rows,
        mixer_output_weight,
        feedforward_norm_gain[None],
    )
    part = shape((4, 8, tok // 8, 256), BF)
    keep, send = call(
        ffn_kernel,
        "ffn",
        (part, part),
        [SMEM] + vmem(1) + [ANY] * 12,
        7,
        32,
        [
            pltpu.VMEM((8, 4, 64, NA), BF),
            pltpu.VMEM((8, 4, 64, 3 * cols - NA), BF),
            pltpu.SemaphoreType.DMA((12,)),
        ],
    )(index, normed, *[found[r] for r in range(8)], *pieces_b)
    block = (8, tok // 8, 256)
    pairs = call(
        pair_kernel,
        "pair",
        (shape(block, F32), shape(block, BF), shape(block, BF), shape(block, BF)),
        [SMEM] + vmem(2),
        1,
    )(index, keep, shifted(send, "c", 1))
    near = [shifted(pairs[d], "y", d) for d in (1, 2, 3)]
    return call(final_kernel, "final", shape((tok // 8, 2048), BF), [SMEM] + vmem(5), 1)(
        index, pairs[0], *near, mid
    )


def solution(mesh):
    torus = Mesh(mesh.devices.reshape(8, 4, 4, 2), ("z", "x", "y", "c"))
    sp, tp = ("z", "x"), ("y", "c")
    in_specs = (
        P(sp + tp, None),
        P(sp, tp),
        P(sp, tp),
        P(sp, tp),
        P(sp, tp),
        P(tp),
        P(sp, tp),
        P(sp, tp),
        P(tp),
        P(tp),
        P(),
        P(),
        P(sp, tp),
        P(sp, tp),
        P(tp, sp),
    )

    return jax.shard_map(
        per_device, mesh=torus, in_specs=in_specs, out_specs=P(sp + tp, None), check_vma=False
    )
```

```python
import jax
import jax.numpy as jnp
from jax import lax
from jax.experimental import pallas as pl
from jax.experimental.pallas import tpu as pltpu
from jax.sharding import Mesh
from jax.sharding import PartitionSpec as P

HEAD = 64
C = 64
BF = jnp.bfloat16
F32 = jnp.float32


def split(x):
    hi = x.astype(BF)
    return hi, (x - hi.astype(F32)).astype(BF)


def dot(a, b):
    return lax.dot_general(a, b, (((1,), (0,)), ((), ())), preferred_element_type=F32)


def dot_t(a, b):
    return lax.dot_general(a, b, (((1,), (1,)), ((), ())), preferred_element_type=F32)


def mm(x, y, f=dot):
    return f(x[0], y[0]) + (f(x[0], y[1]) + f(x[1], y[0]))


def iota(shape, dim):
    return lax.broadcasted_iota(jnp.int32, shape, dim)


def head_masks(width=128):
    first = (iota((1, width), 1) & 127) < HEAD
    m0 = jnp.where(first, 1.0, 0.0)
    return m0.astype(BF), (1.0 - m0).astype(BF)


def stacked(y, masks):
    return tuple(jnp.concatenate([p * masks[0], p * masks[1]], axis=0) for p in y)


def local_scan(q, k, v, dx, lx, dco, lro, extra):
    chunks = range(q.shape[0] // C)
    first = iota((1, 128), 1) < HEAD
    masks, masks2 = head_masks(), head_masks(256)
    ext = jnp.where(first, extra[:, 0:1], extra[:, 1:2])
    log_decay = -0.6065306597126334 * (1.0 / (1.0 + jnp.exp(-(dco + dx)))) - ext
    lrate = 1.0 / (1.0 + jnp.exp(-(lro + lx)))
    same_f = jnp.where((iota((128, 128), 0) < HEAD) == (iota((128, 128), 1) < HEAD), 1.0, 0.0)
    ones = same_f.astype(BF)
    kk = split(k * k)
    unit = k * lax.rsqrt(dot(kk[0], ones) + dot(kk[1], ones) + 1e-06)
    rate = lrate * unit
    row, col = iota((C, 128), 0), iota((C, 128), 1) & (C - 1)
    lower = row > col
    lower_eq = row >= col
    unit_packed = jnp.where(row == col, 1.0, 0.0)
    tri = jnp.where(iota((C, C), 0) >= iota((C, C), 1), 1.0, 0.0).astype(BF)
    eye = jnp.where(iota((128, 128), 0) == iota((128, 128), 1), 1.0, 0.0)
    levels = [((row >> n) == (col >> n) + 1) & (((row >> n) & 1) == 1) for n in range(6)]
    at = [slice(c * C, (c + 1) * C) for c in chunks]

    def each(f, *lists):
        return [f(*args) for args in zip(*lists)]

    def summed(lw):
        w0 = lw.astype(BF)
        w1, w2 = split(lw - w0.astype(F32))
        return dot(tri, w0) + (dot(tri, w1) + dot(tri, w2))

    lws = [log_decay[a] for a in at]
    cums = each(summed, lws)
    mids = [cum[C // 2 - 1 : C // 2] for cum in cums]
    ends = [cum[C - 1 : C] for cum in cums]
    falls = each(lambda cum, mid: jnp.exp(mid - cum), cums, mids)
    pcs = each(lambda cum, lw, mid, a: jnp.exp(cum - lw - mid) * unit[a], cums, lws, mids, at)
    ucs = each(lambda cum, mid, a: jnp.exp(cum - mid) * q[a], cums, mids, at)
    rcs = each(lambda fall, a: fall * rate[a], falls, at)
    gcs = each(lambda fall, a: fall * k[a], falls, at)

    def pairs(pc, uc, rc, gc):
        left = split(jnp.concatenate([pc, uc], axis=0))
        rs, gs = stacked(split(rc), masks), stacked(split(gc), masks)
        right = tuple(jnp.concatenate([a, b], axis=0) for a, b in zip(rs, gs))
        return mm(left, right, dot_t)

    pair = each(pairs, pcs, ucs, rcs, gcs)
    arps = [jnp.where(lower, p[:C, :128], 0.0) for p in pair]
    burs = [jnp.where(lower_eq, p[C:, :128], 0.0) for p in pair]

    def values_read(p, a):
        ab = split(
            jnp.concatenate(
                [jnp.where(lower, p[:C, 128:], 0.0), jnp.where(lower_eq, p[C:, 128:], 0.0)], axis=0
            )
        )
        vs = stacked((v[a].astype(BF),), masks)[0]
        return dot(ab[0], vs) + dot(ab[1], vs)

    abvs = each(values_read, pair, at)
    invs = [unit_packed - jnp.where(levels[0], arp, 0.0) for arp in arps]
    for n in range(1, 6):
        ss = each(split, invs)
        ts = each(
            lambda arp, s: mm(split(jnp.where(levels[n], arp, 0.0)), stacked(s, masks)), arps, ss
        )
        invs = each(lambda inv, s, t: inv - mm(s, stacked(split(t), masks)), invs, ss, ts)
    to_mids = each(jnp.exp, mids)
    wys = each(
        lambda inv, pc, to_mid, abv: split(
            mm(
                split(inv),
                stacked(split(jnp.concatenate([pc * to_mid, abv[:C]], axis=1)), masks2),
            )
        ),
        invs,
        pcs,
        to_mids,
        abvs,
    )
    bwys = each(lambda bur, wy: mm(split(bur), stacked(wy, masks2)), burs, wys)
    ueffs = each(lambda uc, to_mid, bwy: split(uc * to_mid - bwy[:, :128]), ucs, to_mids, bwys)
    own = each(lambda abv, bwy: abv[C:] - bwy[:, 128:], abvs, bwys)

    def change(rc, gc, mid, end, wy, a):
        rest = jnp.exp(end - mid)
        rwy = mm(split((rc * rest).T), wy)
        gs = split((gc * rest).T)
        vb = v[a].astype(BF)
        gv = dot(gs[0], vb) + dot(gs[1], vb)
        return split(eye * jnp.exp(end) - same_f * rwy[:, :128]), same_f * (gv - rwy[:, 128:])

    changes = each(change, rcs, gcs, mids, ends, wys, at)
    reads, owns = [], []
    both = jnp.concatenate([eye, jnp.zeros((128, 128), F32)], axis=1)
    for c in chunks:
        bs = split(both)
        out = mm(ueffs[c], bs)
        reads.append(out[:, :128])
        owns.append(own[c] + out[:, 128:])
        trans, state = changes[c]
        both = mm(trans, bs)
        both = jnp.concatenate([both[:, :128], both[:, 128:] + state], axis=1)
    total = jnp.concatenate(
        [both[:HEAD, :128] + both[HEAD:, :128], both[:HEAD, 128:] + both[HEAD:, 128:]], axis=0
    )
    return jnp.concatenate(reads, axis=0), jnp.concatenate(owns, axis=0), total


def local_kernel(resid, core_rows, q, k, v, dx, lx, dco, lro, extra, *refs):
    reads_out, owns_out, rows, total, reads, owns, sems = refs
    rows[0] = resid[...]
    rows[1] = core_rows[...]
    f = lambda r: r[...].astype(F32)
    a, b, t = local_scan(f(q), f(k), f(v), f(dx), f(lx), dco[...], lro[...], extra[...].T)
    reads[...] = a
    owns[...] = b
    stores = [
        pltpu.make_async_copy(reads, reads_out, sems.at[0]),
        pltpu.make_async_copy(owns, owns_out, sems.at[1]),
    ]
    for copy in stores:
        copy.start()
    out = sent(t[:HEAD], t[HEAD:])
    for d in range(total.shape[0]):
        total[d] = out
    for copy in stores:
        copy.wait()


def finish(reads, owns, state, gain):
    masks = head_masks()
    out = owns + mm(split(reads), stacked(split(state), masks))
    same = (iota((128, 128), 0) < HEAD) == (iota((128, 128), 1) < HEAD)
    mean = jnp.where(same, 1.0 / HEAD, 0.0).astype(BF)
    s = split(out)
    center = out - (dot(s[0], mean) + dot(s[1], mean))
    s = split(center * center)
    spread = dot(s[0], mean) + dot(s[1], mean)
    return (center * lax.rsqrt(spread + 1e-05) * gain).astype(BF)


def fold(level, masks2):
    while len(level) > 1:
        nxt = []
        for i in range(0, len(level) - 1, 2):
            (t1, x1), (t2, x2) = level[i], level[i + 1]
            both = jnp.concatenate([t1, x1], axis=1)
            out = mm(split(t2), stacked(split(both), masks2))
            nxt.append((out[:, :128], out[:, 128:] + x2))
        if len(level) % 2:
            nxt.append(level[-1])
        level = nxt
    return level[0]


def eye_packed():
    return jnp.where(iota((HEAD, 128), 0) == (iota((HEAD, 128), 1) & (HEAD - 1)), 1.0, 0.0)


def piece(pieces, d):
    p = pieces[d].astype(F32)
    return p[:HEAD], p[HEAD:]


def sent(trans, state):
    return jnp.concatenate([trans - eye_packed(), state], axis=0).astype(BF)


def earlier(pieces, count, index, masks2):
    level = []
    for d in range(count - 1):
        used = jnp.where(d < index, 1.0, 0.0)
        trans, state = piece(pieces, d)
        level.append((trans * used + eye_packed(), state * used))
    return fold(level, masks2)


def group_kernel(index, pieces, total, inside):
    masks2 = head_masks(256)
    level = [piece(pieces, d) for d in range(4)]
    t, x = fold([(t + eye_packed(), x) for t, x in level], masks2)
    out = sent(t, x)
    for d in range(total.shape[0]):
        total[d] = out
    t, x = earlier(pieces, 4, index[0], masks2)
    inside[...] = jnp.concatenate([t, x], axis=0)


def pack_kernel(gate, up, down, a, b):
    cols = gate.shape[1]
    cut = a.shape[2] - cols
    for n in range(a.shape[0]):
        a[n, :, :cols] = gate[...]
        a[n, :, cols:] = up[:, :cut]
    b[:, : cols - cut] = up[:, cut:]
    b[:, cols - cut :] = down[...]


def stackb_kernel(index, *refs):
    out = refs[8]
    for r in range(8):
        out[(index[2] + r) % 8] = refs[r][...]


def finish_kernel(place, core_place, pieces, inside, reads, owns, gain, mixed):
    _, x = earlier(pieces, pieces.shape[0], place[0], head_masks(256))
    t = inside[...]
    state = mm(split(t[:HEAD]), stacked(split(x), head_masks())) + t[HEAD:]
    out = finish(reads[...], owns[...], state, gain[...])
    rows = out.shape[0] // 8
    core = core_place[0]
    parts = [[out[(2 * y + c) * rows : (2 * y + c + 1) * rows] for y in range(4)] for c in range(2)]
    for d in range(4):
        for y in range(4):
            for c in range(2):
                at = y * rows + (c ^ core) * (4 * rows)
                mixed[d, pl.ds(pl.multiple_of(at, 16), rows)] = parts[c][y]


def proj_kernel(index, own, sib, r0, r1, r2, r3, weight, gain, mid, normed, resid, w, sems):
    core = index[1]
    loads = [
        pltpu.make_async_copy(
            weight.at[pl.ds(pl.multiple_of((2 * y + (c ^ core)) * 128, 128), 128)],
            w.at[pl.ds((4 * c + y) * 128, 128)],
            sems.at[4 * c + y],
        )
        for c in range(2)
        for y in range(4)
    ]
    for copy in loads:
        copy.start()
    for s, r in enumerate((r0, r1, r2, r3)):
        for n in range(2):
            resid[n, (index[4] + 4 - s) % 4] = r[n]
    half = own.shape[1] // 2
    sums = []
    for copy in loads[:4]:
        copy.wait()
    for n in range(2):
        left = jnp.concatenate([own[y, n * half : (n + 1) * half] for y in range(4)], axis=1)
        sums.append(dot(left, w[:512]))
    for copy in loads[4:]:
        copy.wait()
    for n in range(2):
        left = jnp.concatenate([sib[y, (1 - n) * half : (2 - n) * half] for y in range(4)], axis=1)
        rows = resid.shape[2]
        m = jnp.concatenate([resid[n, y] for y in range(4)], axis=0).astype(F32)
        m = m + (sums[n] + dot(left, w[512:]))
        m = m.astype(BF)
        if n == 0:
            for y in range(4):
                mid[y] = m[y * rows : (y + 1) * rows]
        m = m.astype(F32)
        scale = lax.rsqrt(jnp.mean(m * m, axis=-1, keepdims=True) + 1e-06)
        m = (m * scale * gain[...]).astype(BF)
        for k in range(8):
            normed[k, n * half : (n + 1) * half] = m[:, k * 256 : (k + 1) * 256]


def ffn_kernel(index, normed, *refs):
    a, b, (keep, send, wa, wb, sems) = refs[:8], refs[8:12], refs[12:]
    z, x = index[2], index[3]
    na, nb = wa.shape[3], wb.shape[3]
    cols = (na + nb) // 3
    tail = 2 * cols - na
    order = (0, 1, 7, 2, 6, 3, 5, 4)
    loads = [pltpu.make_async_copy(a[r], wa.at[n], sems.at[n]) for n, r in enumerate(order)]
    later = [
        pltpu.make_async_copy(b[s], wb.at[:, (x + 4 - s) % 4], sems.at[8 + s]) for s in range(4)
    ]
    for copy in loads + later:
        copy.start()
    both = None
    for first, last in ((0, 3), (3, 6), (6, 8)):
        for copy in loads[first:last]:
            copy.wait()
        left = jnp.concatenate([normed[(z + r) % 8] for r in order[first:last]], axis=1)
        part = dot(left, wa[first:last].reshape(-1, na))
        both = part if both is None else both + part
    for copy in later:
        copy.wait()
    left = jnp.concatenate([normed[k] for k in range(8)], axis=1)
    rest = dot(left, wb[:, :, :, :tail].reshape(-1, tail))
    both = jnp.concatenate([both, rest], axis=1)
    gate = both[:, :cols]
    hidden = (gate * (1.0 / (1.0 + jnp.exp(-gate))) * both[:, cols:]).astype(BF)
    half, rows = hidden.shape[0] // 2, hidden.shape[0] // 8
    for k in range(8):
        out = dot_t(hidden, wb[k, :, :, tail:].reshape(-1, cols)).astype(BF)
        for y in range(4):
            keep[y, k] = out[y * rows : (y + 1) * rows]
            send[y, k] = out[half + y * rows : half + (y + 1) * rows]


def pair_kernel(index, keep, other, out0, out1, out2, out3):
    for d, out in enumerate((out0, out1, out2, out3)):
        at = (index[4] + d) % 4
        out[...] = (keep[at].astype(F32) + other[at].astype(F32)).astype(out.dtype)


def final_kernel(index, own, near1, near2, near3, mid, result):
    m = mid[index[4]].astype(F32)
    for k in range(8):
        total = own[k] + (near1[k].astype(F32) + near2[k].astype(F32)) + near3[k].astype(F32)
        at = slice(k * 256, (k + 1) * 256)
        result[:, at] = (m[:, at] + 0.5 * total).astype(BF)


def vmem(n):
    return [pl.BlockSpec(memory_space=pltpu.VMEM)] * n


SMEM = pl.BlockSpec(memory_space=pltpu.SMEM)
ANY = pl.BlockSpec(memory_space=pl.ANY)
HBM = pl.BlockSpec(memory_space=pltpu.MemorySpace.HBM)
shape = jax.ShapeDtypeStruct


def call(kernel, name, out, in_specs, us, mib=16, scratch=(), space=None):
    def run(*args):
        return pl.pallas_call(
            kernel,
            out_shape=out,
            in_specs=in_specs,
            out_specs=space
            if isinstance(space, tuple)
            else jax.tree.map(lambda _: space or vmem(1)[0], out),
            scratch_shapes=scratch,
            compiler_params=pltpu.CompilerParams(vmem_limit_bytes=LIMIT.get(name, mib << 20)),
            cost_estimate=pl.CostEstimate(
                flops=int(us * FLOPS_US), bytes_accessed=0, transcendentals=0
            ),
        )(*args)

    return run


FLOPS_US = 1e8
LIMIT = {"pack": None, "local": None, "finish": 56 << 20, "group": 16 << 20}
NA = 1152


def per_device(
    resid,
    queries,
    keys,
    values,
    decay_input_part,
    decay_channel_offset,
    decay_head_extra,
    correction_rate_input,
    correction_rate_offset,
    head_norm_gain,
    mixer_output_weight,
    feedforward_norm_gain,
    gate_weight,
    up_weight,
    down_weight,
):
    tok, cols = queries.shape[0], gate_weight.shape[1]
    z, x, y, c = (lax.axis_index(a).astype(jnp.int32) for a in ("z", "x", "y", "c"))
    index = jnp.stack([z, c, z, x, y])

    def exchanged(array, axis):
        return lax.all_to_all(array, axis, split_axis=0, concat_axis=0, tiled=True)

    def shifted(array, axis, by):
        n = lax.axis_size(axis)
        return lax.ppermute(array, axis, [(i, (i + by) % n) for i in range(n)])

    part_a, part_b = call(
        pack_kernel,
        "pack",
        (shape((4, 64, NA), BF), shape((64, 3 * cols - NA), BF)),
        vmem(3),
        1,
        8,
    )(gate_weight, up_weight, down_weight.T)
    down_up = down_dn = part_b
    found_b = {0: part_b}
    for s in range(1, 5):
        found_b[8 - s] = down_up = shifted(down_up, "z", 1)
        if s < 4:
            found_b[s] = down_dn = shifted(down_dn, "z", -1)
    first = exchanged(part_a, "x")
    core_rows = shifted(resid, "c", 1)
    stack = call(
        stackb_kernel,
        "stackb",
        shape((8, *part_b.shape), BF),
        [SMEM] + vmem(8),
        1,
        8,
    )(index, *[found_b[r] for r in range(8)])
    found = {0: first}
    up = down = first
    for s in range(1, 5):
        found[8 - s] = up = shifted(up, "z", 1)
        if s < 4:
            found[s] = down = shifted(down, "z", -1)
    pieces_b = [stack] + [shifted(stack, "x", s) for s in range(1, 4)]

    reads, owns, rows, total = call(
        local_kernel,
        "local",
        (
            shape((tok, 128), F32),
            shape((tok, 128), F32),
            shape((2, *resid.shape), BF),
            shape((4, 128, 128), BF),
        ),
        vmem(10),
        6,
        24,
        [
            pltpu.VMEM((tok, 128), F32),
            pltpu.VMEM((tok, 128), F32),
            pltpu.SemaphoreType.DMA((2,)),
        ],
        (HBM, HBM, vmem(1)[0], vmem(1)[0]),
    )(
        resid,
        core_rows,
        queries,
        keys,
        values,
        decay_input_part,
        correction_rate_input,
        decay_channel_offset[None],
        correction_rate_offset[None],
        decay_head_extra.T,
    )
    rows = [rows] + [shifted(rows, "y", s) for s in range(1, 4)]
    near = exchanged(total, "x")
    total, inside = call(
        group_kernel,
        "group",
        (shape((8, 128, 128), BF), shape((128, 128), F32)),
        [SMEM] + vmem(1),
        1,
    )(x[None], near)
    far = exchanged(total, "z")
    mixed = call(finish_kernel, "finish", shape((4, tok, 128), BF), [SMEM] * 2 + vmem(5), 3)(
        z[None], c[None], far, inside, reads, owns, head_norm_gain[None]
    )
    mixed_own = exchanged(mixed, "y")
    mixed_sib = shifted(mixed_own, "c", 1)
    mid, normed = call(
        proj_kernel,
        "proj",
        (shape((4, tok // 8, 2048), BF), shape((8, tok, 256), BF)),
        [SMEM] + vmem(6) + [ANY] + vmem(1),
        3,
        48,
        [
            pltpu.VMEM((2, 4, tok // 8, 2048), BF),
            pltpu.VMEM((1024, 2048), BF),
            pltpu.SemaphoreType.DMA((8,)),
        ],
    )(
        index,
        mixed_own,
        mixed_sib,
        *rows,
        mixer_output_weight,
        feedforward_norm_gain[None],
    )
    part = shape((4, 8, tok // 8, 256), BF)
    keep, send = call(
        ffn_kernel,
        "ffn",
        (part, part),
        [SMEM] + vmem(1) + [ANY] * 12,
        7,
        32,
        [
            pltpu.VMEM((8, 4, 64, NA), BF),
            pltpu.VMEM((8, 4, 64, 3 * cols - NA), BF),
            pltpu.SemaphoreType.DMA((12,)),
        ],
    )(index, normed, *[found[r] for r in range(8)], *pieces_b)
    block = (8, tok // 8, 256)
    pairs = call(
        pair_kernel,
        "pair",
        (shape(block, F32), shape(block, BF), shape(block, BF), shape(block, BF)),
        [SMEM] + vmem(2),
        1,
    )(index, keep, shifted(send, "c", 1))
    near = [shifted(pairs[d], "y", d) for d in (1, 2, 3)]
    return call(final_kernel, "final", shape((tok // 8, 2048), BF), [SMEM] + vmem(5), 1)(
        index, pairs[0], *near, mid
    )


def solution(mesh):
    torus = Mesh(mesh.devices.reshape(8, 4, 4, 2), ("z", "x", "y", "c"))
    sp, tp = ("z", "x"), ("y", "c")
    in_specs = (
        P(sp + tp, None),
        P(sp, tp),
        P(sp, tp),
        P(sp, tp),
        P(sp, tp),
        P(tp),
        P(sp, tp),
        P(sp, tp),
        P(tp),
        P(tp),
        P(),
        P(),
        P(sp, tp),
        P(sp, tp),
        P(tp, sp),
    )

    return jax.shard_map(
        per_device, mesh=torus, in_specs=in_specs, out_specs=P(sp + tp, None), check_vma=False
    )
```

```python
import jax
import jax.numpy as jnp
from jax import lax
from jax.experimental import pallas as pl
from jax.experimental.pallas import tpu as pltpu
from jax.sharding import Mesh
from jax.sharding import PartitionSpec as P

HEAD = 64
C = 64
BF = jnp.bfloat16
F32 = jnp.float32


def split(x):
    hi = x.astype(BF)
    return hi, (x - hi.astype(F32)).astype(BF)


def dot(a, b):
    return lax.dot_general(a, b, (((1,), (0,)), ((), ())), preferred_element_type=F32)


def dot_t(a, b):
    return lax.dot_general(a, b, (((1,), (1,)), ((), ())), preferred_element_type=F32)


def mm(x, y, f=dot):
    return f(x[0], y[0]) + (f(x[0], y[1]) + f(x[1], y[0]))


def iota(shape, dim):
    return lax.broadcasted_iota(jnp.int32, shape, dim)


def head_masks(width=128):
    first = (iota((1, width), 1) & 127) < HEAD
    m0 = jnp.where(first, 1.0, 0.0)
    return m0.astype(BF), (1.0 - m0).astype(BF)


def stacked(y, masks):
    return tuple(jnp.concatenate([p * masks[0], p * masks[1]], axis=0) for p in y)


def local_scan(q, k, v, dx, lx, dco, lro, extra):
    chunks = range(q.shape[0] // C)
    first = iota((1, 128), 1) < HEAD
    masks, masks2 = head_masks(), head_masks(256)
    ext = jnp.where(first, extra[:, 0:1], extra[:, 1:2])
    log_decay = -0.6065306597126334 * (1.0 / (1.0 + jnp.exp(-(dco + dx)))) - ext
    lrate = 1.0 / (1.0 + jnp.exp(-(lro + lx)))
    same_f = jnp.where((iota((128, 128), 0) < HEAD) == (iota((128, 128), 1) < HEAD), 1.0, 0.0)
    ones = same_f.astype(BF)
    kk = split(k * k)
    unit = k * lax.rsqrt(dot(kk[0], ones) + dot(kk[1], ones) + 1e-06)
    rate = lrate * unit
    row, col = iota((C, 128), 0), iota((C, 128), 1) & (C - 1)
    lower = row > col
    lower_eq = row >= col
    unit_packed = jnp.where(row == col, 1.0, 0.0)
    tri = jnp.where(iota((C, C), 0) >= iota((C, C), 1), 1.0, 0.0).astype(BF)
    eye = jnp.where(iota((128, 128), 0) == iota((128, 128), 1), 1.0, 0.0)
    levels = [((row >> n) == (col >> n) + 1) & (((row >> n) & 1) == 1) for n in range(6)]
    at = [slice(c * C, (c + 1) * C) for c in chunks]

    def each(f, *lists):
        return [f(*args) for args in zip(*lists)]

    def summed(lw):
        w0 = lw.astype(BF)
        w1, w2 = split(lw - w0.astype(F32))
        return dot(tri, w0) + (dot(tri, w1) + dot(tri, w2))

    lws = [log_decay[a] for a in at]
    cums = each(summed, lws)
    mids = [cum[C // 2 - 1 : C // 2] for cum in cums]
    ends = [cum[C - 1 : C] for cum in cums]
    falls = each(lambda cum, mid: jnp.exp(mid - cum), cums, mids)
    pcs = each(lambda cum, lw, mid, a: jnp.exp(cum - lw - mid) * unit[a], cums, lws, mids, at)
    ucs = each(lambda cum, mid, a: jnp.exp(cum - mid) * q[a], cums, mids, at)
    rcs = each(lambda fall, a: fall * rate[a], falls, at)
    gcs = each(lambda fall, a: fall * k[a], falls, at)

    def pairs(pc, uc, rc, gc):
        left = split(jnp.concatenate([pc, uc], axis=0))
        rs, gs = stacked(split(rc), masks), stacked(split(gc), masks)
        right = tuple(jnp.concatenate([a, b], axis=0) for a, b in zip(rs, gs))
        return mm(left, right, dot_t)

    pair = each(pairs, pcs, ucs, rcs, gcs)
    arps = [jnp.where(lower, p[:C, :128], 0.0) for p in pair]
    burs = [jnp.where(lower_eq, p[C:, :128], 0.0) for p in pair]

    def values_read(p, a):
        ab = split(
            jnp.concatenate(
                [jnp.where(lower, p[:C, 128:], 0.0), jnp.where(lower_eq, p[C:, 128:], 0.0)], axis=0
            )
        )
        vs = stacked((v[a].astype(BF),), masks)[0]
        return dot(ab[0], vs) + dot(ab[1], vs)

    abvs = each(values_read, pair, at)
    invs = [unit_packed - jnp.where(levels[0], arp, 0.0) for arp in arps]
    for n in range(1, 6):
        ss = each(split, invs)
        ts = each(
            lambda arp, s: mm(split(jnp.where(levels[n], arp, 0.0)), stacked(s, masks)), arps, ss
        )
        invs = each(lambda inv, s, t: inv - mm(s, stacked(split(t), masks)), invs, ss, ts)
    to_mids = each(jnp.exp, mids)
    wys = each(
        lambda inv, pc, to_mid, abv: split(
            mm(
                split(inv),
                stacked(split(jnp.concatenate([pc * to_mid, abv[:C]], axis=1)), masks2),
            )
        ),
        invs,
        pcs,
        to_mids,
        abvs,
    )
    bwys = each(lambda bur, wy: mm(split(bur), stacked(wy, masks2)), burs, wys)
    ueffs = each(lambda uc, to_mid, bwy: split(uc * to_mid - bwy[:, :128]), ucs, to_mids, bwys)
    own = each(lambda abv, bwy: abv[C:] - bwy[:, 128:], abvs, bwys)

    def change(rc, gc, mid, end, wy, a):
        rest = jnp.exp(end - mid)
        rwy = mm(split((rc * rest).T), wy)
        gs = split((gc * rest).T)
        vb = v[a].astype(BF)
        gv = dot(gs[0], vb) + dot(gs[1], vb)
        return split(eye * jnp.exp(end) - same_f * rwy[:, :128]), same_f * (gv - rwy[:, 128:])

    changes = each(change, rcs, gcs, mids, ends, wys, at)
    reads, owns = [], []
    both = jnp.concatenate([eye, jnp.zeros((128, 128), F32)], axis=1)
    for c in chunks:
        bs = split(both)
        out = mm(ueffs[c], bs)
        reads.append(out[:, :128])
        owns.append(own[c] + out[:, 128:])
        trans, state = changes[c]
        both = mm(trans, bs)
        both = jnp.concatenate([both[:, :128], both[:, 128:] + state], axis=1)
    total = jnp.concatenate(
        [both[:HEAD, :128] + both[HEAD:, :128], both[:HEAD, 128:] + both[HEAD:, 128:]], axis=0
    )
    return jnp.concatenate(reads, axis=0), jnp.concatenate(owns, axis=0), total


def local_kernel(resid, core_rows, q, k, v, dx, lx, dco, lro, extra, *refs):
    reads_out, owns_out, rows, total, reads, owns, sems = refs
    rows[0] = resid[...]
    rows[1] = core_rows[...]
    f = lambda r: r[...].astype(F32)
    a, b, t = local_scan(f(q), f(k), f(v), f(dx), f(lx), dco[...], lro[...], extra[...].T)
    reads[...] = a
    owns[...] = b
    stores = [
        pltpu.make_async_copy(reads, reads_out, sems.at[0]),
        pltpu.make_async_copy(owns, owns_out, sems.at[1]),
    ]
    for copy in stores:
        copy.start()
    out = sent(t[:HEAD], t[HEAD:])
    for d in range(total.shape[0]):
        total[d] = out
    for copy in stores:
        copy.wait()


def finish(reads, owns, state, gain):
    masks = head_masks()
    out = owns + mm(split(reads), stacked(split(state), masks))
    same = (iota((128, 128), 0) < HEAD) == (iota((128, 128), 1) < HEAD)
    mean = jnp.where(same, 1.0 / HEAD, 0.0).astype(BF)
    s = split(out)
    center = out - (dot(s[0], mean) + dot(s[1], mean))
    s = split(center * center)
    spread = dot(s[0], mean) + dot(s[1], mean)
    return (center * lax.rsqrt(spread + 1e-05) * gain).astype(BF)


def fold(level, masks2):
    while len(level) > 1:
        nxt = []
        for i in range(0, len(level) - 1, 2):
            (t1, x1), (t2, x2) = level[i], level[i + 1]
            both = jnp.concatenate([t1, x1], axis=1)
            out = mm(split(t2), stacked(split(both), masks2))
            nxt.append((out[:, :128], out[:, 128:] + x2))
        if len(level) % 2:
            nxt.append(level[-1])
        level = nxt
    return level[0]


def eye_packed():
    return jnp.where(iota((HEAD, 128), 0) == (iota((HEAD, 128), 1) & (HEAD - 1)), 1.0, 0.0)


def piece(pieces, d):
    p = pieces[d].astype(F32)
    return p[:HEAD], p[HEAD:]


def sent(trans, state):
    return jnp.concatenate([trans - eye_packed(), state], axis=0).astype(BF)


def earlier(pieces, count, index, masks2):
    level = []
    for d in range(count - 1):
        used = jnp.where(d < index, 1.0, 0.0)
        trans, state = piece(pieces, d)
        level.append((trans * used + eye_packed(), state * used))
    return fold(level, masks2)


def group_kernel(index, pieces, total, inside):
    masks2 = head_masks(256)
    level = [piece(pieces, d) for d in range(4)]
    t, x = fold([(t + eye_packed(), x) for t, x in level], masks2)
    out = sent(t, x)
    for d in range(total.shape[0]):
        total[d] = out
    t, x = earlier(pieces, 4, index[0], masks2)
    inside[...] = jnp.concatenate([t, x], axis=0)


def pack_kernel(gate, up, down, a, b):
    cols = gate.shape[1]
    cut = a.shape[2] - cols
    for n in range(a.shape[0]):
        a[n, :, :cols] = gate[...]
        a[n, :, cols:] = up[:, :cut]
    b[:, : cols - cut] = up[:, cut:]
    b[:, cols - cut :] = down[...]


def stackb_kernel(index, *refs):
    out = refs[8]
    for r in range(8):
        out[(index[2] + r) % 8] = refs[r][...]


def finish_kernel(place, core_place, pieces, inside, reads, owns, gain, mixed):
    _, x = earlier(pieces, pieces.shape[0], place[0], head_masks(256))
    t = inside[...]
    state = mm(split(t[:HEAD]), stacked(split(x), head_masks())) + t[HEAD:]
    out = finish(reads[...], owns[...], state, gain[...])
    rows = out.shape[0] // 8
    core = core_place[0]
    parts = [[out[(2 * y + c) * rows : (2 * y + c + 1) * rows] for y in range(4)] for c in range(2)]
    for d in range(4):
        for y in range(4):
            for c in range(2):
                at = y * rows + (c ^ core) * (4 * rows)
                mixed[d, pl.ds(pl.multiple_of(at, 16), rows)] = parts[c][y]


def proj_kernel(index, own, sib, r0, r1, r2, r3, weight, gain, mid, normed, resid, w, sems):
    core = index[1]
    loads = [
        pltpu.make_async_copy(
            weight.at[pl.ds(pl.multiple_of((2 * y + (c ^ core)) * 128, 128), 128)],
            w.at[pl.ds((4 * c + y) * 128, 128)],
            sems.at[4 * c + y],
        )
        for c in range(2)
        for y in range(4)
    ]
    for copy in loads:
        copy.start()
    for s, r in enumerate((r0, r1, r2, r3)):
        for n in range(2):
            resid[n, (index[4] + 4 - s) % 4] = r[n]
    half = own.shape[1] // 2
    sums = []
    for copy in loads[:4]:
        copy.wait()
    for n in range(2):
        left = jnp.concatenate([own[y, n * half : (n + 1) * half] for y in range(4)], axis=1)
        sums.append(dot(left, w[:512]))
    for copy in loads[4:]:
        copy.wait()
    for n in range(2):
        left = jnp.concatenate([sib[y, (1 - n) * half : (2 - n) * half] for y in range(4)], axis=1)
        rows = resid.shape[2]
        m = jnp.concatenate([resid[n, y] for y in range(4)], axis=0).astype(F32)
        m = m + (sums[n] + dot(left, w[512:]))
        m = m.astype(BF)
        if n == 0:
            for y in range(4):
                mid[y] = m[y * rows : (y + 1) * rows]
        m = m.astype(F32)
        scale = lax.rsqrt(jnp.mean(m * m, axis=-1, keepdims=True) + 1e-06)
        m = (m * scale * gain[...]).astype(BF)
        for k in range(8):
            normed[k, n * half : (n + 1) * half] = m[:, k * 256 : (k + 1) * 256]


def ffn_kernel(index, normed, *refs):
    a, b, (keep, send, wa, wb, sems) = refs[:8], refs[8:12], refs[12:]
    z, x = index[2], index[3]
    na, nb = wa.shape[3], wb.shape[3]
    cols = (na + nb) // 3
    tail = 2 * cols - na
    order = (0, 1, 7, 2, 6, 3, 5, 4)
    loads = [pltpu.make_async_copy(a[r], wa.at[n], sems.at[n]) for n, r in enumerate(order)]
    later = [
        pltpu.make_async_copy(b[s], wb.at[:, (x + 4 - s) % 4], sems.at[8 + s]) for s in range(4)
    ]
    for copy in loads:
        copy.start()
    both = None
    for first, last in ((0, 2), (2, 5), (5, 8)):
        for copy in loads[first:last]:
            copy.wait()
        if not first:
            for copy in later:
                copy.start()
        left = jnp.concatenate([normed[(z + r) % 8] for r in order[first:last]], axis=1)
        part = dot(left, wa[first:last].reshape(-1, na))
        both = part if both is None else both + part
    for copy in later:
        copy.wait()
    left = jnp.concatenate([normed[k] for k in range(8)], axis=1)
    rest = dot(left, wb[:, :, :, :tail].reshape(-1, tail))
    both = jnp.concatenate([both, rest], axis=1)
    gate = both[:, :cols]
    hidden = (gate * (1.0 / (1.0 + jnp.exp(-gate))) * both[:, cols:]).astype(BF)
    half, rows = hidden.shape[0] // 2, hidden.shape[0] // 8
    for k in range(8):
        out = dot_t(hidden, wb[k, :, :, tail:].reshape(-1, cols)).astype(BF)
        for y in range(4):
            keep[y, k] = out[y * rows : (y + 1) * rows]
            send[y, k] = out[half + y * rows : half + (y + 1) * rows]


def pair_kernel(index, keep, other, out0, out1, out2, out3):
    for d, out in enumerate((out0, out1, out2, out3)):
        at = (index[4] + d) % 4
        out[...] = (keep[at].astype(F32) + other[at].astype(F32)).astype(out.dtype)


def final_kernel(index, own, near1, near2, near3, mid, result):
    m = mid[index[4]].astype(F32)
    for k in range(8):
        total = own[k] + (near1[k].astype(F32) + near2[k].astype(F32)) + near3[k].astype(F32)
        at = slice(k * 256, (k + 1) * 256)
        result[:, at] = (m[:, at] + 0.5 * total).astype(BF)


def vmem(n):
    return [pl.BlockSpec(memory_space=pltpu.VMEM)] * n


SMEM = pl.BlockSpec(memory_space=pltpu.SMEM)
ANY = pl.BlockSpec(memory_space=pl.ANY)
HBM = pl.BlockSpec(memory_space=pltpu.MemorySpace.HBM)
shape = jax.ShapeDtypeStruct


def call(kernel, name, out, in_specs, us, mib=16, scratch=(), space=None):
    def run(*args):
        return pl.pallas_call(
            kernel,
            out_shape=out,
            in_specs=in_specs,
            out_specs=space
            if isinstance(space, tuple)
            else jax.tree.map(lambda _: space or vmem(1)[0], out),
            scratch_shapes=scratch,
            compiler_params=pltpu.CompilerParams(vmem_limit_bytes=LIMIT.get(name, mib << 20)),
            cost_estimate=pl.CostEstimate(
                flops=int(us * FLOPS_US), bytes_accessed=0, transcendentals=0
            ),
        )(*args)

    return run


FLOPS_US = 1e8
LIMIT = {"pack": None, "local": None, "finish": 56 << 20, "group": 16 << 20}
NA = 1280


def per_device(
    resid,
    queries,
    keys,
    values,
    decay_input_part,
    decay_channel_offset,
    decay_head_extra,
    correction_rate_input,
    correction_rate_offset,
    head_norm_gain,
    mixer_output_weight,
    feedforward_norm_gain,
    gate_weight,
    up_weight,
    down_weight,
):
    tok, cols = queries.shape[0], gate_weight.shape[1]
    z, x, y, c = (lax.axis_index(a).astype(jnp.int32) for a in ("z", "x", "y", "c"))
    index = jnp.stack([z, c, z, x, y])

    def exchanged(array, axis):
        return lax.all_to_all(array, axis, split_axis=0, concat_axis=0, tiled=True)

    def shifted(array, axis, by):
        n = lax.axis_size(axis)
        return lax.ppermute(array, axis, [(i, (i + by) % n) for i in range(n)])

    part_a, part_b = call(
        pack_kernel,
        "pack",
        (shape((4, 64, NA), BF), shape((64, 3 * cols - NA), BF)),
        vmem(3),
        1,
        8,
    )(gate_weight, up_weight, down_weight.T)
    down_up = down_dn = part_b
    found_b = {0: part_b}
    for s in range(1, 5):
        found_b[8 - s] = down_up = shifted(down_up, "z", 1)
        if s < 4:
            found_b[s] = down_dn = shifted(down_dn, "z", -1)
    first = exchanged(part_a, "x")
    core_rows = shifted(resid, "c", 1)
    stack = call(
        stackb_kernel,
        "stackb",
        shape((8, *part_b.shape), BF),
        [SMEM] + vmem(8),
        1,
        8,
    )(index, *[found_b[r] for r in range(8)])
    found = {0: first}
    up = down = first
    for s in range(1, 5):
        found[8 - s] = up = shifted(up, "z", 1)
        if s < 4:
            found[s] = down = shifted(down, "z", -1)
    pieces_b = [stack] + [shifted(stack, "x", s) for s in range(1, 4)]

    reads, owns, rows, total = call(
        local_kernel,
        "local",
        (
            shape((tok, 128), F32),
            shape((tok, 128), F32),
            shape((2, *resid.shape), BF),
            shape((4, 128, 128), BF),
        ),
        vmem(10),
        6,
        24,
        [
            pltpu.VMEM((tok, 128), F32),
            pltpu.VMEM((tok, 128), F32),
            pltpu.SemaphoreType.DMA((2,)),
        ],
        (HBM, HBM, vmem(1)[0], vmem(1)[0]),
    )(
        resid,
        core_rows,
        queries,
        keys,
        values,
        decay_input_part,
        correction_rate_input,
        decay_channel_offset[None],
        correction_rate_offset[None],
        decay_head_extra.T,
    )
    rows = [rows] + [shifted(rows, "y", s) for s in range(1, 4)]
    near = exchanged(total, "x")
    total, inside = call(
        group_kernel,
        "group",
        (shape((8, 128, 128), BF), shape((128, 128), F32)),
        [SMEM] + vmem(1),
        1,
    )(x[None], near)
    far = exchanged(total, "z")
    mixed = call(finish_kernel, "finish", shape((4, tok, 128), BF), [SMEM] * 2 + vmem(5), 3)(
        z[None], c[None], far, inside, reads, owns, head_norm_gain[None]
    )
    mixed_own = exchanged(mixed, "y")
    mixed_sib = shifted(mixed_own, "c", 1)
    mid, normed = call(
        proj_kernel,
        "proj",
        (shape((4, tok // 8, 2048), BF), shape((8, tok, 256), BF)),
        [SMEM] + vmem(6) + [ANY] + vmem(1),
        3,
        48,
        [
            pltpu.VMEM((2, 4, tok // 8, 2048), BF),
            pltpu.VMEM((1024, 2048), BF),
            pltpu.SemaphoreType.DMA((8,)),
        ],
    )(
        index,
        mixed_own,
        mixed_sib,
        *rows,
        mixer_output_weight,
        feedforward_norm_gain[None],
    )
    part = shape((4, 8, tok // 8, 256), BF)
    keep, send = call(
        ffn_kernel,
        "ffn",
        (part, part),
        [SMEM] + vmem(1) + [ANY] * 12,
        7,
        32,
        [
            pltpu.VMEM((8, 4, 64, NA), BF),
            pltpu.VMEM((8, 4, 64, 3 * cols - NA), BF),
            pltpu.SemaphoreType.DMA((12,)),
        ],
    )(index, normed, *[found[r] for r in range(8)], *pieces_b)
    block = (8, tok // 8, 256)
    pairs = call(
        pair_kernel,
        "pair",
        (shape(block, F32), shape(block, BF), shape(block, BF), shape(block, BF)),
        [SMEM] + vmem(2),
        1,
    )(index, keep, shifted(send, "c", 1))
    near = [shifted(pairs[d], "y", d) for d in (1, 2, 3)]
    return call(final_kernel, "final", shape((tok // 8, 2048), BF), [SMEM] + vmem(5), 1)(
        index, pairs[0], *near, mid
    )


def solution(mesh):
    torus = Mesh(mesh.devices.reshape(8, 4, 4, 2), ("z", "x", "y", "c"))
    sp, tp = ("z", "x"), ("y", "c")
    in_specs = (
        P(sp + tp, None),
        P(sp, tp),
        P(sp, tp),
        P(sp, tp),
        P(sp, tp),
        P(tp),
        P(sp, tp),
        P(sp, tp),
        P(tp),
        P(tp),
        P(),
        P(),
        P(sp, tp),
        P(sp, tp),
        P(tp, sp),
    )

    return jax.shard_map(
        per_device, mesh=torus, in_specs=in_specs, out_specs=P(sp + tp, None), check_vma=False
    )
```
